256 devices in a mesh: sp: 128 (over z, y, x), tp: 2 (over core).
Axes of the slice: x: 4, y: 4, z: 8, core: 2. Of those that a mesh axis runs over, the one named last changes fastest.
Arguments:
- queries: bfloat16 [3, 32768, 2048], P(None, 'sp', 'tp'), may hold values from -6 to 6
- keys: bfloat16 [3, 32768, 2048], P(None, 'sp', 'tp'), may hold values from -6 to 6
- values: bfloat16 [3, 32768, 2048], P(None, 'sp', 'tp'), may hold values from -6 to 6
- w_out: bfloat16 [2048, 2048], P(None, 'tp'), may hold values from -1 to 1
Outputs:
- mixed: bfloat16 [32768, 2048], P('sp', 'tp')
The draws below stay inside these ranges and needn't reach their ends.
All inputs are finite; a program needn't handle non-finite values.
Results may differ from the reference program's by a relative error of at most 0.01.
Values may be sent and summed in bfloat16 or wider, within the bound.
A program may use at most 128 MiB of HBM per device.

```python
from functools import partial
import jax
import jax.numpy as jnp
from jax import lax

D = 2048
HEADS = 16
HEAD = 128
GROUPS = 3
KEYS_PER_QUERY = 128
FIRST_STRIDE = 1
SECOND_STRIDE = 4
THIRD_STRIDE = 16
TOKENS = 32768


def planted_pair(key):
    base = jax.random.fold_in(key, 11)
    first_key, second_key, pick_key, sign_key = jax.random.split(base, 4)
    shape = (GROUPS, TOKENS, HEADS * HEAD)
    query_part = jnp.clip(jax.random.normal(first_key, shape, jnp.float32), -6.0, 6.0)
    key_part = jnp.clip(jax.random.normal(second_key, shape, jnp.float32), -6.0, 6.0)
    return (query_part, key_part)


def draw_queries(key, part):
    return planted_pair(key)[0].astype(jnp.bfloat16)


def draw_keys(key, part):
    return planted_pair(key)[1].astype(jnp.bfloat16)


def block_levels(stream_key, extent, cuts, least, top_value):
    gain = 1.0
    for axis_at, parts in cuts:
        steps = jax.random.uniform(jax.random.fold_in(jax.random.fold_in(stream_key, 6), axis_at), (parts,), jnp.float32, least / len(cuts), top_value / len(cuts))
        gain = gain * jnp.repeat(jnp.exp(steps), extent[axis_at] // parts).reshape((-1,) + (1,) * (len(extent) - 1 - axis_at))
    return gain


def bell_draw(key, extent, scale, bound, shards=(), held_as=jnp.bfloat16):
    values = jax.random.normal(key, extent, jnp.float32) * scale
    if len(shards) > 0:
        values = block_levels(key, extent, shards, -0.22, 0.18) * values
    return jnp.clip(values, min=-bound, max=bound).astype(held_as)


def setup_inputs(seed: int = 0) -> dict:
    splits = jax.random.split(jax.random.key(seed), 5)
    queries = draw_queries(jax.random.fold_in(splits[4], 71), 0)
    keys = draw_keys(jax.random.fold_in(splits[4], 71), 0)
    values = bell_draw(splits[2], (GROUPS, TOKENS, HEADS * HEAD), 1.0, 6.0, ((1, 128), (2, 2)))
    w_out = bell_draw(splits[3], (HEADS * HEAD, D), (HEADS * HEAD // 64) ** -0.5, 1.0, ((1, 2),))
    return {"queries": queries, "keys": keys, "values": values, "w_out": w_out}


ROPE_BASE = 10000.0
MASKED = -1e30


def turn_halves(matrix, cosine, sine_part):
    first_half, second_half = jnp.split(matrix, 2, axis=-1)
    return jnp.concatenate([first_half * cosine - second_half * sine_part,
                            second_half * cosine + first_half * sine_part], axis=-1)


def strided_head(triple, dilation):
    query_head, key_head, value_head = triple
    length = query_head.shape[0]
    block_count = length // (KEYS_PER_QUERY * dilation)

    def blocked(matrix):
        shaped = jnp.transpose(matrix.reshape(length // dilation, dilation, HEAD), (1, 0, 2))
        return shaped.reshape(dilation, block_count, KEYS_PER_QUERY, HEAD).astype(jnp.float32)

    def with_previous(matrix):
        shaped = blocked(matrix)
        earlier = jnp.concatenate([jnp.zeros_like(shaped[:, :1]), shaped[:, :-1]], axis=1)
        return jnp.concatenate([earlier, shaped], axis=2)

    q_blocks = blocked(query_head)
    key_blocks = with_previous(key_head)
    value_blocks = with_previous(value_head)
    scores = jnp.einsum("dnqe,dnke->dnqk", q_blocks, key_blocks, precision=lax.Precision.HIGHEST)
    q_index = jnp.arange(KEYS_PER_QUERY)[:, None]
    k_index = jnp.arange(2 * KEYS_PER_QUERY)[None, :]
    distance = q_index + KEYS_PER_QUERY - k_index
    band = (distance >= 0) & (distance <= KEYS_PER_QUERY)
    opening = (jnp.arange(block_count)[:, None, None] == 0) & (k_index[None] < KEYS_PER_QUERY)
    allowed = band[None] & jnp.logical_not(opening)
    scores = jnp.where(allowed[None], scores, MASKED)
    row_max = jnp.max(scores, axis=-1, keepdims=True)
    weights = jnp.exp(scores - row_max)
    row_sum = jnp.sum(weights, axis=-1, keepdims=True)
    rounded = lax.optimization_barrier(weights.astype(jnp.bfloat16)).astype(jnp.float32)
    weighted = jnp.einsum("dnqk,dnke->dnqe", rounded, value_blocks, precision=lax.Precision.HIGHEST)
    result = weighted / row_sum
    log_sum = (row_max + jnp.log(row_sum))[..., 0]
    result = jnp.transpose(result.reshape(dilation, length // dilation, HEAD), (1, 0, 2)).reshape(length, HEAD)
    log_sum = jnp.transpose(log_sum.reshape(dilation, length // dilation)).reshape(length)
    return result, log_sum


def reference(queries, keys, values, w_out):
    length = queries.shape[1]
    positions = jnp.arange(length, dtype=jnp.int32).astype(jnp.float32)
    inverse = ROPE_BASE ** (-jnp.arange(0, HEAD, 2, dtype=jnp.float32) / HEAD)
    angles = positions[:, None] * inverse[None, :]
    cosine = jnp.cos(angles)[:, None, :]
    sine_part = jnp.sin(angles)[:, None, :]
    group_strides = (FIRST_STRIDE, SECOND_STRIDE, THIRD_STRIDE)
    results = []
    log_sums = []
    for group_id in range(len(group_strides)):
        query_f = queries[group_id].astype(jnp.float32).reshape(length, HEADS, HEAD)
        key_f = keys[group_id].astype(jnp.float32).reshape(length, HEADS, HEAD)
        turned_q = (turn_halves(query_f, cosine, sine_part) * HEAD ** -0.5).astype(jnp.bfloat16)
        turned_k = turn_halves(key_f, cosine, sine_part).astype(jnp.bfloat16)
        value_h = values[group_id].reshape(length, HEADS, HEAD)
        result, log_sum = lax.map(partial(strided_head, dilation=group_strides[group_id]),
                                  (jnp.transpose(turned_q, (1, 0, 2)),
                                   jnp.transpose(turned_k, (1, 0, 2)),
                                   jnp.transpose(value_h, (1, 0, 2))))
        results.append(jnp.transpose(result, (1, 0, 2)))
        log_sums.append(jnp.transpose(log_sum))
    shares = jax.nn.softmax(jnp.stack(log_sums), axis=0)
    attended = jnp.sum(shares[..., None] * jnp.stack(results), axis=0)
    attended = attended.astype(jnp.bfloat16).reshape(length, HEADS * HEAD)
    return jnp.dot(attended, w_out, preferred_element_type=jnp.float32).astype(jnp.bfloat16)
```

```python
import functools

import jax
import jax.numpy as jnp
from jax import lax
from jax.experimental import pallas as pl
from jax.experimental.pallas import tpu as pltpu
from jax.sharding import PartitionSpec as P

HEAD = 128
ROPE_BASE = 10000.0
MASKED = -1e30
ROWS = 256
COLS = 1024
HEADS = COLS // HEAD
BACK = 128
PLANE = 16
LINE = 4
CHUNKS = 4
WIDE = COLS // CHUNKS
CHUNK_HEADS = WIDE // HEAD
MESH = pl.DeviceIdType.MESH
BF16 = jnp.bfloat16
F32 = jnp.float32


def one_hot(condition):
    return jnp.where(condition, 1.0, 0.0).astype(BF16)


def dot(a, b):
    return jnp.dot(a, b, preferred_element_type=F32)


def dot_nt(a, b):
    return lax.dot_general(a, b, (((1,), (1,)), ((), ())), preferred_element_type=F32)


def kernel(
    sp_size,
    cos_ref, sin_ref, q_hbm, k_hbm, v_hbm, w_hbm, out_ref,
    qv, kv, vv, wv, s2, r2, s1, r1, kv0, q0, o2, b2, o1, b1, l2, lb2, l1, lb1,
    o0, lse0, own, other, band,
    in_sem, w_sem, s2_send, s2_recv, s1_send, s1_recv, h2_send, h2_recv, h1_send, h1_recv,
    h0_send, h0_recv, o2_send, o2_recv, o1_send, o1_recv, l2_send, l2_recv, l1_send, l1_recv,
    a_send, a_recv,
):
    sp = lax.axis_index("sp")
    tp = lax.axis_index("tp")
    x = lax.rem(sp, LINE)
    y = lax.rem(sp // LINE, LINE)
    j = lax.rem(sp, PLANE)
    plane = sp - j

    def block(distance):
        return lax.rem(sp + distance + sp_size, sp_size)

    def peer(d):
        px = lax.rem(x + d // LINE, LINE)
        py = lax.rem(y + lax.rem(d, LINE), LINE)
        return py * LINE + px

    def mate(d):
        return lax.rem(x + d, LINE)

    def columns(c):
        return pl.ds(pl.multiple_of(c * WIDE, WIDE), WIDE)

    loads = []
    for g in (2, 1, 0):
        for i, (src, dst) in enumerate(((q_hbm, qv), (k_hbm, kv), (v_hbm, vv))):
            target = dst.at[g]
            if g == 0 and i == 2:
                target = kv0.at[1, pl.ds(BACK, ROWS)]
            loads.append(pltpu.make_async_copy(src.at[g], target, in_sem.at[g, i]))
    for copy in loads:
        copy.start()
    w_copies = [
        pltpu.make_async_copy(w_hbm.at[pl.ds(pl.multiple_of(half * COLS, COLS), COLS)], wv.at[n], w_sem.at[n])
        for n, half in enumerate((tp, 1 - tp))
    ]
    for copy in w_copies:
        copy.start()

    barrier = pltpu.get_barrier_semaphore()

    def greet(d, _):
        pl.semaphore_signal(barrier, inc=1, device_id=(plane + peer(d), tp), device_id_type=MESH)
        return 0

    lax.fori_loop(1, PLANE, greet, 0)
    for distance in (1, LINE, PLANE):
        for sign in (1, -1):
            pl.semaphore_signal(barrier, inc=1, device_id=(block(sign * distance), tp), device_id_type=MESH)
    pl.semaphore_signal(barrier, inc=1, device_id=(sp, 1 - tp), device_id_type=MESH)

    q_index = lax.broadcasted_iota(jnp.int32, (BACK, 2 * BACK), 0)
    k_index = lax.broadcasted_iota(jnp.int32, (BACK, 2 * BACK), 1)
    inside = (k_index >= q_index) & (k_index <= q_index + BACK)
    base = jnp.where(inside, 0.0, MASKED)
    band[3] = base
    for g, reach in enumerate((1, LINE, PLANE)):
        opening = jnp.where(sp >= reach, 0.0, MASKED)
        band[g] = jnp.where(k_index < BACK, base + opening, base)

    row = lax.broadcasted_iota(jnp.int32, (ROWS, ROWS), 0)
    col = lax.broadcasted_iota(jnp.int32, (ROWS, ROWS), 1)
    n2 = ROWS // PLANE
    n1 = ROWS // LINE

    def perm2():
        return one_hot(col == PLANE * (row % n2) + row // n2)

    def perm1():
        return one_hot(col == LINE * (row % n1) + row // n1)

    def perm1_back():
        return one_hot(row == LINE * (col % n1) + col // n1)

    def turned(piece):
        parts = []
        for h in range(piece.shape[1] // HEAD):
            m = piece[:, h * HEAD : (h + 1) * HEAD].astype(F32)
            parts.append(m * cos_ref[...] + pltpu.roll(m, HEAD // 2, 1) * sin_ref[...])
        return jnp.concatenate(parts, axis=1)

    def prepared(g, c):
        cs = columns(c)
        q = (turned(qv[g, :, cs]) * HEAD**-0.5).astype(BF16)
        k = turned(kv[g, :, cs]).astype(BF16)
        return q, k

    for i in range(3):
        loads[i].wait()
    pl.semaphore_wait(barrier, PLANE - 1 + 7)

    def g2_copy(c, d):
        return pltpu.make_async_remote_copy(
            src_ref=s2.at[peer(d), :, :, columns(c)],
            dst_ref=r2.at[8 + j, :, :, columns(c)],
            send_sem=s2_send.at[c, d],
            recv_sem=s2_recv.at[c, d],
            device_id=(plane + peer(d), tp),
            device_id_type=MESH,
        )

    def g2_out(c, _):
        cs = columns(c)
        q, k = prepared(2, c)
        order = perm2()
        for i, m in enumerate((q, k, vv[2, :, cs])):
            s2[:, i, :, cs] = dot(order, m).astype(BF16).reshape(PLANE, n2, WIDE)
        r2[8 + j, :, :, cs] = s2[j, :, :, cs]
        lax.fori_loop(1, PLANE, lambda d, _: (g2_copy(c, d).start(), 0)[1], 0)
        return 0

    lax.fori_loop(0, CHUNKS, g2_out, 0)

    for i in range(3, 6):
        loads[i].wait()

    def g1_copy(c, d):
        return pltpu.make_async_remote_copy(
            src_ref=s1.at[mate(d), :, :, columns(c)],
            dst_ref=r1.at[2 + x, :, :, columns(c)],
            send_sem=s1_send.at[c, d],
            recv_sem=s1_recv.at[c, d],
            device_id=(sp - x + mate(d), tp),
            device_id_type=MESH,
        )

    def g1_out(c, _):
        cs = columns(c)
        q, k = prepared(1, c)
        order = perm1()
        for i, m in enumerate((q, k, vv[1, :, cs])):
            s1[:, i, :, cs] = dot(order, m).astype(BF16).reshape(LINE, n1, WIDE)
        r1[2 + x, :, :, cs] = s1[x, :, :, cs]
        lax.fori_loop(1, LINE, lambda d, _: (g1_copy(c, d).start(), 0)[1], 0)
        return 0

    lax.fori_loop(0, CHUNKS, g1_out, 0)

    for i in range(6, 9):
        loads[i].wait()

    def g0_out(c, _):
        cs = columns(c)
        q, k = prepared(0, c)
        q0[:, cs] = q
        kv0[0, pl.ds(BACK, ROWS), cs] = k
        return 0

    lax.fori_loop(0, CHUNKS, g0_out, 0)
    h0_copy = pltpu.make_async_remote_copy(
        src_ref=kv0.at[:, pl.ds(ROWS, BACK)],
        dst_ref=kv0.at[:, pl.ds(0, BACK)],
        send_sem=h0_send,
        recv_sem=h0_recv,
        device_id=(block(1), tp),
        device_id_type=MESH,
    )
    h0_copy.start()

    def h2_copy(c):
        return pltpu.make_async_remote_copy(
            src_ref=r2.at[pl.ds(16, 8), pl.ds(1, 2), :, columns(c)],
            dst_ref=r2.at[pl.ds(0, 8), pl.ds(1, 2), :, columns(c)],
            send_sem=h2_send.at[c],
            recv_sem=h2_recv.at[c],
            device_id=(block(PLANE), tp),
            device_id_type=MESH,
        )

    def h1_copy(c):
        return pltpu.make_async_remote_copy(
            src_ref=r1.at[pl.ds(4, 2), pl.ds(1, 2), :, columns(c)],
            dst_ref=r1.at[pl.ds(0, 2), pl.ds(1, 2), :, columns(c)],
            send_sem=h1_send.at[c],
            recv_sem=h1_recv.at[c],
            device_id=(block(LINE), tp),
            device_id_type=MESH,
        )

    def attend(q, k, v, bias):
        scores = dot_nt(q, k) + bias
        row_max = jnp.max(scores, axis=1, keepdims=True)
        probs = jnp.exp(scores - row_max)
        row_sum = jnp.sum(probs, axis=1, keepdims=True)
        result = dot(probs.astype(BF16), v) / row_sum
        return result, row_max + jnp.log(row_sum)

    lane = lax.broadcasted_iota(jnp.int32, (BACK, HEAD), 1)

    def g2_halo(c, _):
        lax.fori_loop(1, PLANE, lambda d, _: (g2_copy(c, d).wait_recv(), 0)[1], 0)
        h2_copy(c).start()
        return 0

    def g1_halo(c, _):
        lax.fori_loop(1, LINE, lambda d, _: (g1_copy(c, d).wait_recv(), 0)[1], 0)
        h1_copy(c).start()
        return 0

    def o2_copy(c, d):
        return pltpu.make_async_remote_copy(
            src_ref=o2.at[peer(d), :, columns(c)],
            dst_ref=b2.at[j, :, columns(c)],
            send_sem=o2_send.at[c, d],
            recv_sem=o2_recv.at[c, d],
            device_id=(plane + peer(d), tp),
            device_id_type=MESH,
        )

    def l2_copy(d):
        return pltpu.make_async_remote_copy(
            src_ref=l2.at[peer(d)],
            dst_ref=lb2.at[j],
            send_sem=l2_send.at[d],
            recv_sem=l2_recv.at[d],
            device_id=(plane + peer(d), tp),
            device_id_type=MESH,
        )

    def o1_copy(c, d):
        return pltpu.make_async_remote_copy(
            src_ref=o1.at[mate(d), :, columns(c)],
            dst_ref=b1.at[x, :, columns(c)],
            send_sem=o1_send.at[c, d],
            recv_sem=o1_recv.at[c, d],
            device_id=(sp - x + mate(d), tp),
            device_id_type=MESH,
        )

    def l1_copy(d):
        return pltpu.make_async_remote_copy(
            src_ref=l1.at[mate(d)],
            dst_ref=lb1.at[x],
            send_sem=l1_send.at[d],
            recv_sem=l1_recv.at[d],
            device_id=(sp - x + mate(d), tp),
            device_id_type=MESH,
        )

    def split_terms(lse):
        high = lse.astype(BF16).astype(F32)
        rest = lse - high
        middle = rest.astype(BF16).astype(F32)
        low = rest - middle
        return (high + pltpu.roll(middle, HEADS, 1) + pltpu.roll(low, 2 * HEADS, 1)).astype(BF16)

    def g2_attend(c, carry):
        h2_copy(c).wait_recv()
        lses = list(carry)
        for h in range(CHUNK_HEADS):
            cs = pl.ds(pl.multiple_of(c * WIDE + h * HEAD, HEAD), HEAD)
            for b in range(2):
                q = r2[pl.ds(8 + 8 * b, 8), 0, :, cs].reshape(BACK, HEAD)
                k = r2[pl.ds(8 * b, 16), 1, :, cs].reshape(2 * BACK, HEAD)
                v = r2[pl.ds(8 * b, 16), 2, :, cs].reshape(2 * BACK, HEAD)
                result, lse = attend(q, k, v, band[2 if b == 0 else 3])
                o2[pl.ds(8 * b, 8), :, cs] = result.astype(BF16).reshape(8, n2, HEAD)
                lses[b] = jnp.where(lane == c * CHUNK_HEADS + h, lse, lses[b])
        b2[j, :, columns(c)] = o2[j, :, columns(c)]
        lax.fori_loop(1, PLANE, lambda d, _: (o2_copy(c, d).start(), 0)[1], 0)
        return tuple(lses)

    def g1_attend(c, carry):
        h1_copy(c).wait_recv()
        lses = list(carry)
        for h in range(CHUNK_HEADS):
            cs = pl.ds(pl.multiple_of(c * WIDE + h * HEAD, HEAD), HEAD)
            for b in range(2):
                q = r1[pl.ds(2 + 2 * b, 2), 0, :, cs].reshape(BACK, HEAD)
                k = r1[pl.ds(2 * b, 4), 1, :, cs].reshape(2 * BACK, HEAD)
                v = r1[pl.ds(2 * b, 4), 2, :, cs].reshape(2 * BACK, HEAD)
                result, lse = attend(q, k, v, band[1 if b == 0 else 3])
                o1[pl.ds(2 * b, 2), :, cs] = result.astype(BF16).reshape(2, n1, HEAD)
                lses[b] = jnp.where(lane == c * CHUNK_HEADS + h, lse, lses[b])
        b1[x, :, columns(c)] = o1[x, :, columns(c)]
        lax.fori_loop(1, LINE, lambda d, _: (o1_copy(c, d).start(), 0)[1], 0)
        return tuple(lses)

    empty = (jnp.zeros((BACK, HEAD), F32), jnp.zeros((BACK, HEAD), F32))
    lax.fori_loop(0, CHUNKS, g2_halo, 0)
    lses = lax.fori_loop(0, CHUNKS, g2_attend, empty)
    for b in range(2):
        l2[pl.ds(8 * b, 8)] = split_terms(lses[b]).reshape(8, n2, HEAD)
    lb2[j] = l2[j]
    lax.fori_loop(1, PLANE, lambda d, _: (l2_copy(d).start(), 0)[1], 0)

    lax.fori_loop(0, CHUNKS, g1_halo, 0)
    lses = lax.fori_loop(0, CHUNKS, g1_attend, empty)
    for b in range(2):
        l1[pl.ds(2 * b, 2)] = split_terms(lses[b]).reshape(2, n1, HEAD)
    lb1[x] = l1[x]
    lax.fori_loop(1, LINE, lambda d, _: (l1_copy(d).start(), 0)[1], 0)

    h0_copy.wait_recv()

    def g0_attend(c, _):
        for h in range(CHUNK_HEADS):
            cs = pl.ds(pl.multiple_of(c * WIDE + h * HEAD, HEAD), HEAD)
            for b in range(2):
                q = q0[pl.ds(BACK * b, BACK), cs]
                k = kv0[0, pl.ds(BACK * b, 2 * BACK), cs]
                v = kv0[1, pl.ds(BACK * b, 2 * BACK), cs]
                result, lse = attend(q, k, v, band[0 if b == 0 else 3])
                o0[pl.ds(BACK * b, BACK), cs] = result
                lse0[pl.ds(BACK * b, BACK), cs] = jnp.broadcast_to(lse, (BACK, HEAD))
        return 0

    lax.fori_loop(0, CHUNKS, g0_attend, 0)

    lax.fori_loop(1, PLANE, lambda d, _: (l2_copy(d).wait_recv(), 0)[1], 0)
    lax.fori_loop(1, LINE, lambda d, _: (l1_copy(d).wait_recv(), 0)[1], 0)

    def a_copy(c):
        return pltpu.make_async_remote_copy(
            src_ref=own.at[:, columns(c)],
            dst_ref=other.at[:, columns(c)],
            send_sem=a_send.at[c],
            recv_sem=a_recv.at[c],
            device_id=(sp, 1 - tp),
            device_id_type=MESH,
        )

    def merge(c, _):
        lax.fori_loop(1, PLANE, lambda d, _: (o2_copy(c, d).wait_recv(), 0)[1], 0)
        lax.fori_loop(1, LINE, lambda d, _: (o1_copy(c, d).wait_recv(), 0)[1], 0)
        cs = columns(c)
        term = lax.broadcasted_iota(jnp.int32, (HEAD, WIDE), 0)
        feature = lax.broadcasted_iota(jnp.int32, (HEAD, WIDE), 1)
        spread = one_hot((term < 3 * HEADS) & (term % HEADS == c * CHUNK_HEADS + feature // HEAD))
        back2, back1 = perm2(), perm1_back()
        out2 = dot(back2, b2[:, :, cs].reshape(ROWS, WIDE))
        out1 = dot(back1, b1[:, :, cs].reshape(ROWS, WIDE))
        log2 = dot(dot(back2, lb2[...].reshape(ROWS, HEAD)).astype(BF16), spread)
        log1 = dot(dot(back1, lb1[...].reshape(ROWS, HEAD)).astype(BF16), spread)
        log0 = lse0[:, cs]
        top = jnp.maximum(jnp.maximum(log0, log1), log2)
        e0, e1, e2 = jnp.exp(log0 - top), jnp.exp(log1 - top), jnp.exp(log2 - top)
        merged = (e0 * o0[:, cs] + e1 * out1 + e2 * out2) / (e0 + e1 + e2)
        own[:, cs] = merged.astype(BF16)
        a_copy(c).start()
        return 0

    lax.fori_loop(0, CHUNKS, merge, 0)

    for copy in w_copies:
        copy.wait()
    lax.fori_loop(0, CHUNKS, lambda c, _: (a_copy(c).wait_recv(), 0)[1], 0)

    def project(c, _):
        cs = columns(c)
        out_ref[:, cs] = (dot(own[...], wv[0, :, cs]) + dot(other[...], wv[1, :, cs])).astype(BF16)
        return 0

    lax.fori_loop(0, CHUNKS, project, 0)

    def drain(c, _):
        lax.fori_loop(1, PLANE, lambda d, _: (g2_copy(c, d).wait_send(), o2_copy(c, d).wait_send(), 0)[2], 0)
        lax.fori_loop(1, LINE, lambda d, _: (g1_copy(c, d).wait_send(), o1_copy(c, d).wait_send(), 0)[2], 0)
        h2_copy(c).wait_send()
        h1_copy(c).wait_send()
        a_copy(c).wait_send()
        return 0

    lax.fori_loop(0, CHUNKS, drain, 0)
    lax.fori_loop(1, PLANE, lambda d, _: (l2_copy(d).wait_send(), 0)[1], 0)
    lax.fori_loop(1, LINE, lambda d, _: (l1_copy(d).wait_send(), 0)[1], 0)
    h0_copy.wait_send()


def shards(queries, keys, values, w_out):
    sp_size = lax.axis_size("sp")
    positions = (lax.iota(jnp.int32, ROWS) + lax.axis_index("sp") * ROWS).astype(F32)
    inverse = ROPE_BASE ** (-jnp.arange(0, HEAD, 2, dtype=F32) / HEAD)
    angles = positions[:, None] * inverse[None, :]
    cosine, sine = jnp.cos(angles), jnp.sin(angles)
    cos_table = jnp.concatenate([cosine, cosine], axis=1)
    sin_table = jnp.concatenate([-sine, sine], axis=1)
    n2, n1 = ROWS // PLANE, ROWS // LINE
    dma = pltpu.SemaphoreType.DMA
    vmem = pl.BlockSpec(memory_space=pltpu.VMEM)
    hbm = pl.BlockSpec(memory_space=pl.ANY)
    return pl.pallas_call(
        functools.partial(kernel, sp_size),
        out_shape=jax.ShapeDtypeStruct((ROWS, COLS), BF16),
        in_specs=[vmem, vmem, hbm, hbm, hbm, hbm],
        out_specs=vmem,
        scratch_shapes=[
            pltpu.VMEM((3, ROWS, COLS), BF16),
            pltpu.VMEM((3, ROWS, COLS), BF16),
            pltpu.VMEM((3, ROWS, COLS), BF16),
            pltpu.VMEM((2, COLS, COLS), BF16),
            pltpu.VMEM((PLANE, 3, n2, COLS), BF16),
            pltpu.VMEM((PLANE + 8, 3, n2, COLS), BF16),
            pltpu.VMEM((LINE, 3, n1, COLS), BF16),
            pltpu.VMEM((LINE + 2, 3, n1, COLS), BF16),
            pltpu.VMEM((2, ROWS + BACK, COLS), BF16),
            pltpu.VMEM((ROWS, COLS), BF16),
            pltpu.VMEM((PLANE, n2, COLS), BF16),
            pltpu.VMEM((PLANE, n2, COLS), BF16),
            pltpu.VMEM((LINE, n1, COLS), BF16),
            pltpu.VMEM((LINE, n1, COLS), BF16),
            pltpu.VMEM((PLANE, n2, HEAD), BF16),
            pltpu.VMEM((PLANE, n2, HEAD), BF16),
            pltpu.VMEM((LINE, n1, HEAD), BF16),
            pltpu.VMEM((LINE, n1, HEAD), BF16),
            pltpu.VMEM((ROWS, COLS), F32),
            pltpu.VMEM((ROWS, COLS), F32),
            pltpu.VMEM((ROWS, COLS), BF16),
            pltpu.VMEM((ROWS, COLS), BF16),
            pltpu.VMEM((4, BACK, 2 * BACK), F32),
            dma((3, 3)), dma((2,)),
            dma((CHUNKS, PLANE)), dma((CHUNKS, PLANE)), dma((CHUNKS, LINE)), dma((CHUNKS, LINE)),
            dma((CHUNKS,)), dma((CHUNKS,)), dma((CHUNKS,)), dma((CHUNKS,)),
            dma, dma,
            dma((CHUNKS, PLANE)), dma((CHUNKS, PLANE)), dma((CHUNKS, LINE)), dma((CHUNKS, LINE)),
            dma((PLANE,)), dma((PLANE,)), dma((LINE,)), dma((LINE,)),
            dma((CHUNKS,)), dma((CHUNKS,)),
        ],
        name="attention",
        compiler_params=pltpu.CompilerParams(collective_id=0, has_side_effects=True),
    )(cos_table, sin_table, queries, keys, values, w_out)


def solution(mesh):
    return jax.shard_map(
        shards,
        mesh=mesh,
        in_specs=(P(None, "sp", "tp"), P(None, "sp", "tp"), P(None, "sp", "tp"), P(None, "tp")),
        out_specs=P("sp", "tp"),
        check_vma=False,
    )
```

```python
import functools

import jax
import jax.numpy as jnp
from jax import lax
from jax.experimental import pallas as pl
from jax.experimental.pallas import tpu as pltpu
from jax.sharding import PartitionSpec as P

HEAD = 128
ROPE_BASE = 10000.0
MASKED = -1e30
ROWS = 256
COLS = 1024
HEADS = COLS // HEAD
BACK = 128
PLANE = 16
LINE = 4
CHUNKS = 4
WIDE = COLS // CHUNKS
CHUNK_HEADS = WIDE // HEAD
MESH = pl.DeviceIdType.MESH
BF16 = jnp.bfloat16
F32 = jnp.float32


def one_hot(condition):
    return jnp.where(condition, 1.0, 0.0).astype(BF16)


def scoped(name, body, carry, first=0, last=CHUNKS):
    def named(c, carry):
        with jax.named_scope(name):
            return body(c, carry)

    return lax.fori_loop(first, last, named, carry)


def dot(a, b):
    return jnp.dot(a, b, preferred_element_type=F32)


def dot_nt(a, b):
    return lax.dot_general(a, b, (((1,), (1,)), ((), ())), preferred_element_type=F32)


def kernel(
    sp_size,
    cos_ref, sin_ref, q_hbm, k_hbm, v_hbm, w_hbm, out_ref,
    qv, kv, vv, wv, s2, r2, s1, r1, k0, q0, qn, on, ob, ln, lb, o2, b2, o1, b1, l2, lb2, l1, lb1,
    o0, lse0, sum0, lse2, own, other, total, band, perms, wanted,
    in_sem, w_sem, s2_send, s2_recv, s1_send, s1_recv, h2_send, h2_recv, h1_send, h1_recv,
    n0_send, n0_recv, o2_send, o2_recv, o1_send, o1_recv, l2_send, l2_recv, l1_send, l1_recv,
    a_send, a_recv,
):
    sp = lax.axis_index("sp")
    tp = lax.axis_index("tp")
    x = lax.rem(sp, LINE)
    y = lax.rem(sp // LINE, LINE)
    j = lax.rem(sp, PLANE)
    plane = sp - j

    def block(distance):
        return lax.rem(sp + distance + sp_size, sp_size)

    def peer(d):
        px = lax.rem(x + d // LINE, LINE)
        py = lax.rem(y + lax.rem(d, LINE), LINE)
        return py * LINE + px

    def mate(d):
        return lax.rem(x + d, LINE)

    def columns(c):
        return pl.ds(pl.multiple_of(c * WIDE, WIDE), WIDE)

    loads = []
    for g in (0, 1, 2):
        for i, (src, dst) in enumerate(((q_hbm, qv), (k_hbm, kv), (v_hbm, vv))):
            loads.append(pltpu.make_async_copy(src.at[g], dst.at[g], in_sem.at[g, i]))
    for copy in loads:
        copy.start()
    w_copies = [
        pltpu.make_async_copy(w_hbm.at[pl.ds(pl.multiple_of(half * COLS, COLS), COLS)], wv.at[n], w_sem.at[n])
        for n, half in enumerate((tp, 1 - tp))
    ]
    for copy in w_copies:
        copy.start()

    barrier = pltpu.get_barrier_semaphore()

    def greet(d, _):
        pl.semaphore_signal(barrier, inc=1, device_id=(plane + peer(d), tp), device_id_type=MESH)
        return 0

    lax.fori_loop(1, PLANE, greet, 0)
    for distance in (LINE, PLANE):
        for sign in (1, -1):
            pl.semaphore_signal(barrier, inc=1, device_id=(block(sign * distance), tp), device_id_type=MESH)
    pl.semaphore_signal(barrier, inc=1, device_id=(sp, 1 - tp), device_id_type=MESH)

    q_index = lax.broadcasted_iota(jnp.int32, (BACK, 2 * BACK), 0)
    k_index = lax.broadcasted_iota(jnp.int32, (BACK, 2 * BACK), 1)
    inside = (k_index >= q_index) & (k_index <= q_index + BACK)
    base = jnp.where(inside, 0.0, MASKED)
    band[0] = base
    for g, reach in ((1, LINE), (2, PLANE)):
        opening = jnp.where(sp >= reach, 0.0, MASKED)
        band[g] = jnp.where(k_index < BACK, base + opening, base)

    row = lax.broadcasted_iota(jnp.int32, (ROWS, ROWS), 0)
    col = lax.broadcasted_iota(jnp.int32, (ROWS, ROWS), 1)
    n2 = ROWS // PLANE
    n1 = ROWS // LINE

    perms[0] = one_hot(col == PLANE * (row % n2) + row // n2)
    perms[1] = one_hot(col == LINE * (row % n1) + row // n1)
    perms[2] = one_hot(row == LINE * (col % n1) + col // n1)
    token = lax.broadcasted_iota(jnp.int32, (ROWS, LINE * HEAD), 0)
    lane1 = lax.broadcasted_iota(jnp.int32, (ROWS, LINE * HEAD), 1)
    wanted[...] = one_hot(lane1 == (token % LINE) * HEAD + (x % 2) * n1 + token // LINE)

    def turned(piece):
        parts = []
        for h in range(piece.shape[1] // HEAD):
            m = piece[:, h * HEAD : (h + 1) * HEAD].astype(F32)
            parts.append(m * cos_ref[...] + pltpu.roll(m, HEAD // 2, 1) * sin_ref[...])
        return jnp.concatenate(parts, axis=1)

    def prepared(g, c):
        cs = columns(c)
        q = (turned(qv[g, :, cs]) * HEAD**-0.5).astype(BF16)
        k = turned(kv[g, :, cs]).astype(BF16)
        return q, k

    def remote(src, dst, i, device):
        return pltpu.make_async_remote_copy(
            src_ref=src,
            dst_ref=dst,
            send_sem=n0_send.at[i],
            recv_sem=n0_recv.at[i],
            device_id=(device, tp),
            device_id_type=MESH,
        )

    before, after = sp - x + mate(LINE - 1), sp - x + mate(1)

    def q0_copy():
        return remote(q0.at[pl.ds(0, BACK)], qn.at[0], 0, before)

    def q0_relay():
        return remote(qn.at[0], qn.at[1], 1, block(-LINE))

    def on_copy():
        return remote(on, ob.at[0], 2, after)

    def on_relay():
        return remote(ob.at[0], ob.at[1], 3, block(LINE))

    def ln_copy():
        return remote(ln, lb.at[0], 4, after)

    def ln_relay():
        return remote(lb.at[0], lb.at[1], 5, block(LINE))

    q_slot = jnp.where(x == LINE - 1, 1, 0)
    o_slot = jnp.where(x == 0, 1, 0)

    with jax.named_scope("load0"):
        for i in range(3):
            loads[i].wait()

    def g0_out(c, _):
        cs = columns(c)
        q, k = prepared(0, c)
        q0[:, cs] = q
        k0[:, cs] = k
        return 0

    scoped("g0_out", g0_out, 0)
    with jax.named_scope("barrier"):
        pl.semaphore_wait(barrier, PLANE - 1 + 5)
    q0_copy().start()

    for i in range(3, 6):
        loads[i].wait()

    def g1_copy(c, d):
        return pltpu.make_async_remote_copy(
            src_ref=s1.at[mate(d), :, :, columns(c)],
            dst_ref=r1.at[2 + x, :, :, columns(c)],
            send_sem=s1_send.at[c, d],
            recv_sem=s1_recv.at[c, d],
            device_id=(sp - x + mate(d), tp),
            device_id_type=MESH,
        )

    def g1_out(c, _):
        cs = columns(c)
        q, k = prepared(1, c)
        order = perms[1]
        for i, m in enumerate((q, k, vv[1, :, cs])):
            s1[:, i, :, cs] = dot(order, m).astype(BF16).reshape(LINE, n1, WIDE)
        r1[2 + x, :, :, cs] = s1[x, :, :, cs]
        lax.fori_loop(1, LINE, lambda d, _: (g1_copy(c, d).start(), 0)[1], 0)
        return 0

    scoped("g1_out", g1_out, 0)

    for i in range(6, 9):
        loads[i].wait()

    def g2_copy(c, d):
        return pltpu.make_async_remote_copy(
            src_ref=s2.at[peer(d), :, :, columns(c)],
            dst_ref=r2.at[8 + j, :, :, columns(c)],
            send_sem=s2_send.at[c, d],
            recv_sem=s2_recv.at[c, d],
            device_id=(plane + peer(d), tp),
            device_id_type=MESH,
        )

    def g2_out(c, _):
        cs = columns(c)
        q, k = prepared(2, c)
        order = perms[0]
        for i, m in enumerate((q, k, vv[2, :, cs])):
            s2[:, i, :, cs] = dot(order, m).astype(BF16).reshape(PLANE, n2, WIDE)
        r2[8 + j, :, :, cs] = s2[j, :, :, cs]
        lax.fori_loop(1, PLANE, lambda d, _: (g2_copy(c, d).start(), 0)[1], 0)
        return 0

    scoped("g2_out", g2_out, 0, 0, CHUNKS // 2)

    def h2_copy(c):
        return pltpu.make_async_remote_copy(
            src_ref=r2.at[pl.ds(16, 8), pl.ds(1, 2), :, columns(c)],
            dst_ref=r2.at[pl.ds(0, 8), pl.ds(1, 2), :, columns(c)],
            send_sem=h2_send.at[c],
            recv_sem=h2_recv.at[c],
            device_id=(block(PLANE), tp),
            device_id_type=MESH,
        )

    def h1_copy(c):
        return pltpu.make_async_remote_copy(
            src_ref=r1.at[pl.ds(4, 2), pl.ds(1, 2), :, columns(c)],
            dst_ref=r1.at[pl.ds(0, 2), pl.ds(1, 2), :, columns(c)],
            send_sem=h1_send.at[c],
            recv_sem=h1_recv.at[c],
            device_id=(block(LINE), tp),
            device_id_type=MESH,
        )

    def attend(q, k, v, bias):
        scores = dot_nt(q, k) + bias
        row_max = jnp.max(scores, axis=1, keepdims=True)
        probs = jnp.exp(scores - row_max)
        row_sum = jnp.sum(probs, axis=1, keepdims=True)
        result = dot(probs.astype(BF16), v) / row_sum
        return result, row_max + jnp.log(row_sum)

    lane = lax.broadcasted_iota(jnp.int32, (BACK, HEAD), 1)

    def g2_halo(c, _):
        lax.fori_loop(1, PLANE, lambda d, _: (g2_copy(c, d).wait_recv(), 0)[1], 0)
        h2_copy(c).start()
        return 0

    def g1_halo(c, _):
        lax.fori_loop(1, LINE, lambda d, _: (g1_copy(c, d).wait_recv(), 0)[1], 0)
        h1_copy(c).start()
        return 0

    def o2_copy(c, d):
        return pltpu.make_async_remote_copy(
            src_ref=o2.at[peer(d), :, columns(c)],
            dst_ref=b2.at[j, :, columns(c)],
            send_sem=o2_send.at[c, d],
            recv_sem=o2_recv.at[c, d],
            device_id=(plane + peer(d), tp),
            device_id_type=MESH,
        )

    def l2_copy(part, d):
        return pltpu.make_async_remote_copy(
            src_ref=l2.at[part, peer(d)],
            dst_ref=lb2.at[part, j],
            send_sem=l2_send.at[part, d],
            recv_sem=l2_recv.at[part, d],
            device_id=(plane + peer(d), tp),
            device_id_type=MESH,
        )

    def o1_copy(c, d):
        return pltpu.make_async_remote_copy(
            src_ref=o1.at[mate(d), :, columns(c)],
            dst_ref=b1.at[x, :, columns(c)],
            send_sem=o1_send.at[c, d],
            recv_sem=o1_recv.at[c, d],
            device_id=(sp - x + mate(d), tp),
            device_id_type=MESH,
        )

    def l1_copy(c, d):
        return pltpu.make_async_remote_copy(
            src_ref=l1.at[c, mate(d)],
            dst_ref=lb1.at[c, x],
            send_sem=l1_send.at[c, d],
            recv_sem=l1_recv.at[c, d],
            device_id=(sp - x + mate(d), tp),
            device_id_type=MESH,
        )

    def split_terms(lse, heads):
        high = lse.astype(BF16).astype(F32)
        rest = lse - high
        middle = rest.astype(BF16).astype(F32)
        low = rest - middle
        return (high + pltpu.roll(middle, heads, 1) + pltpu.roll(low, 2 * heads, 1)).astype(BF16)

    def place(lses, b, head, lse):
        lses[b] = jnp.where(lane == head, lse, lses[b])

    def g2_attend(c, _):
        with jax.named_scope("wait_h2"):
            h2_copy(c).wait_recv()
        lses = [lse2[0], lse2[1]]
        for h in range(CHUNK_HEADS):
            cs = pl.ds(pl.multiple_of(c * WIDE + h * HEAD, HEAD), HEAD)
            for b in range(2):
                q = r2[pl.ds(8 + 8 * b, 8), 0, :, cs].reshape(BACK, HEAD)
                k = r2[pl.ds(8 * b, 16), 1, :, cs].reshape(2 * BACK, HEAD)
                v = r2[pl.ds(8 * b, 16), 2, :, cs].reshape(2 * BACK, HEAD)
                result, lse = attend(q, k, v, band[2 if b == 0 else 0])
                o2[pl.ds(8 * b, 8), :, cs] = result.astype(BF16).reshape(8, n2, HEAD)
                place(lses, b, lax.rem(c, CHUNKS // 2) * CHUNK_HEADS + h, lse)
        lse2[0], lse2[1] = lses
        b2[j, :, columns(c)] = o2[j, :, columns(c)]
        lax.fori_loop(1, PLANE, lambda d, _: (o2_copy(c, d).start(), 0)[1], 0)

        @pl.when(lax.rem(c, CHUNKS // 2) == CHUNKS // 2 - 1)
        def _():
            part = c // (CHUNKS // 2)
            for b in range(2):
                l2[part, pl.ds(8 * b, 8)] = split_terms(lse2[b], HEADS // 2).reshape(8, n2, HEAD)
            lb2[part, j] = l2[part, j]
            lax.fori_loop(1, PLANE, lambda d, _: (l2_copy(part, d).start(), 0)[1], 0)

        return 0

    def g1_attend(c, _):
        with jax.named_scope("wait_h1"):
            h1_copy(c).wait_recv()
        lses = list(empty)
        for h in range(CHUNK_HEADS):
            cs = pl.ds(pl.multiple_of(c * WIDE + h * HEAD, HEAD), HEAD)
            for b in range(2):
                q = r1[pl.ds(2 + 2 * b, 2), 0, :, cs].reshape(BACK, HEAD)
                k = r1[pl.ds(2 * b, 4), 1, :, cs].reshape(2 * BACK, HEAD)
                v = r1[pl.ds(2 * b, 4), 2, :, cs].reshape(2 * BACK, HEAD)
                result, lse = attend(q, k, v, band[1 if b == 0 else 0])
                o1[pl.ds(2 * b, 2), :, cs] = result.astype(BF16).reshape(2, n1, HEAD)
                place(lses, b, h, lse)
        slot = lax.broadcasted_iota(jnp.int32, (n2, HEAD), 0)
        chosen = one_hot(slot == lax.broadcasted_iota(jnp.int32, (n2, HEAD), 1))
        for b in range(2):
            turned_terms = dot_nt(chosen, split_terms(lses[b], CHUNK_HEADS)).astype(BF16)
            l1[c, 2 * b] = turned_terms
            l1[c, 2 * b + 1] = turned_terms
        b1[x, :, columns(c)] = o1[x, :, columns(c)]
        lb1[c, x] = l1[c, x]
        lax.fori_loop(1, LINE, lambda d, _: (o1_copy(c, d).start(), l1_copy(c, d).start(), 0)[2], 0)
        return 0

    def g0_attend(c, _):
        for h in range(CHUNK_HEADS):
            cs = pl.ds(pl.multiple_of(c * WIDE + h * HEAD, HEAD), HEAD)
            for b in range(2):
                q = q0[pl.ds(BACK * b, BACK), cs]
                k = k0[pl.ds(0, BACK * (b + 1)), cs]
                v = vv[0, pl.ds(0, BACK * (b + 1)), cs]
                result, lse = attend(q, k, v, band[0] if b else band[0, :, BACK:])
                o0[pl.ds(BACK * b, BACK), cs] = result
                lse0[pl.ds(BACK * b, BACK), cs] = jnp.broadcast_to(lse, (BACK, HEAD))
        return 0

    def n0_attend(c, carry):
        lses = list(carry)
        for h in range(CHUNK_HEADS):
            cs = pl.ds(pl.multiple_of(c * WIDE + h * HEAD, HEAD), HEAD)
            k = k0[pl.ds(BACK, BACK), cs]
            v = vv[0, pl.ds(BACK, BACK), cs]
            result, lse = attend(qn[q_slot, :, cs], k, v, band[0, :, :BACK])
            on[:, cs] = result.astype(BF16)
            place(lses, 0, c * CHUNK_HEADS + h, lse)
        return tuple(lses)

    empty = (jnp.zeros((BACK, HEAD), F32), jnp.zeros((BACK, HEAD), F32))

    def g1_both(c, _):
        g1_halo(c, 0)

        @pl.when(c > 0)
        def _():
            g1_attend(c - 1, 0)

        return 0

    scoped("g0_attend", g0_attend, 0)
    scoped("g1_both", g1_both, 0, 0, 1)
    with jax.named_scope("wait_q0"):
        q0_copy().wait_recv()

    @pl.when(x == LINE - 1)
    def _():
        q0_relay().start()

    scoped("g1_both", g1_both, 0, 1, 2)
    with jax.named_scope("wait_q0r"):

        @pl.when(x == LINE - 1)
        def _():
            q0_relay().wait_recv()

    lses = scoped("n0_attend", n0_attend, empty[:1])
    ln[...] = split_terms(lses[0], HEADS)
    on_copy().start()
    ln_copy().start()
    scoped("g2_out", g2_out, 0, CHUNKS // 2, CHUNKS)
    scoped("g1_both", g1_both, 0, 2, CHUNKS)
    with jax.named_scope("g1_last"):
        g1_attend(CHUNKS - 1, 0)

    lse2[...] = jnp.zeros_like(lse2)

    def g2_both(c, _):
        g2_halo(c, 0)

        @pl.when(c > 0)
        def _():
            g2_attend(c - 1, 0)

        return 0

    scoped("g2_both", g2_both, 0, 0, 2)
    with jax.named_scope("wait_on"):
        on_copy().wait_recv()
        ln_copy().wait_recv()

        @pl.when(x == 0)
        def _():
            on_relay().start()
            ln_relay().start()

    scoped("g2_both", g2_both, 0, 2, CHUNKS)
    with jax.named_scope("g2_last"):
        g2_attend(CHUNKS - 1, 0)

    def drain(c, _):
        lax.fori_loop(1, PLANE, lambda d, _: (g2_copy(c, d).wait_send(), 0)[1], 0)
        lax.fori_loop(1, LINE, lambda d, _: (g1_copy(c, d).wait_send(), 0)[1], 0)
        h2_copy(c).wait_send()
        h1_copy(c).wait_send()
        return 0

    scoped("drain", drain, 0)
    for copy in w_copies:
        copy.wait()
    for copy in (q0_copy(), on_copy(), ln_copy()):
        copy.wait_send()

    @pl.when(x == LINE - 1)
    def _():
        q0_relay().wait_send()


    with jax.named_scope("wait_l"):

        @pl.when(x == 0)
        def _():
            on_relay().wait()
            ln_relay().wait()

    def a_copy(c):
        return pltpu.make_async_remote_copy(
            src_ref=own.at[:, columns(c)],
            dst_ref=other.at[:, columns(c)],
            send_sem=a_send.at[c],
            recv_sem=a_recv.at[c],
            device_id=(sp, 1 - tp),
            device_id_type=MESH,
        )

    def spread(terms, heads, first):
        term = lax.broadcasted_iota(jnp.int32, (terms, WIDE), 0)
        feature = lax.broadcasted_iota(jnp.int32, (terms, WIDE), 1)
        return one_hot((term < 3 * heads) & (term % heads == first + feature // HEAD))

    def project(c):
        cs = columns(c)
        return dot(own[:, cs], wv[0, cs, :]) + dot(other[:, cs], wv[1, cs, :])

    def premerge(c, _):
        with jax.named_scope("wait_o1"):
            lax.fori_loop(1, LINE, lambda d, _: (o1_copy(c, d).wait_recv(), l1_copy(c, d).wait_recv(), 0)[2], 0)
        cs = columns(c)
        out1 = dot(perms[2], b1[:, :, cs].reshape(ROWS, WIDE))
        lanes1 = jnp.concatenate([lb1[c, r] for r in range(LINE)], axis=1)
        log1 = dot(dot_nt(wanted[...], lanes1).astype(BF16), spread(n2, CHUNK_HEADS, 0))
        log3 = dot(lb[o_slot], spread(HEAD, HEADS, c * CHUNK_HEADS)) + jnp.where(sp >= 1, 0.0, MASKED)
        for half in range(2):
            rows = slice(half * BACK, (half + 1) * BACK)
            logs = [lse0[rows, cs], log1[rows]]
            outs = [o0[rows, cs], out1[rows]]
            if half == 0:
                logs.append(log3)
                outs.append(ob[o_slot, :, cs].astype(F32))
            top = functools.reduce(jnp.maximum, logs)
            weights = [jnp.exp(log - top) for log in logs]
            o0[rows, cs] = sum(weight * out for weight, out in zip(weights, outs))
            sum0[rows, cs] = sum(weights)
            lse0[rows, cs] = top
        return 0

    scoped("premerge", premerge, 0)

    def merge(c, _):
        part = c // (CHUNKS // 2)
        with jax.named_scope("wait_o2"):
            lax.fori_loop(1, PLANE, lambda d, _: (o2_copy(c, d).wait_recv(), 0)[1], 0)

            @pl.when(lax.rem(c, CHUNKS // 2) == 0)
            def _():
                lax.fori_loop(1, PLANE, lambda d, _: (l2_copy(part, d).wait_recv(), 0)[1], 0)

        cs = columns(c)
        out2 = dot(perms[0], b2[:, :, cs].reshape(ROWS, WIDE))
        terms = dot(perms[0], lb2[part].reshape(ROWS, HEAD)).astype(BF16)
        log2 = dot(terms, spread(HEAD, HEADS // 2, lax.rem(c, CHUNKS // 2) * CHUNK_HEADS))
        top = jnp.maximum(lse0[:, cs], log2)
        old, new = jnp.exp(lse0[:, cs] - top), jnp.exp(log2 - top)
        own[:, cs] = ((o0[:, cs] * old + out2 * new) / (sum0[:, cs] * old + new)).astype(BF16)
        a_copy(c).start()

        @pl.when(c == 1)
        def _():
            a_copy(0).wait_recv()
            total[...] = project(0)

        @pl.when(c > 1)
        def _():
            a_copy(c - 1).wait_recv()
            total[...] += project(c - 1)

        return 0

    scoped("merge", merge, 0)

    with jax.named_scope("wait_a"):
        a_copy(CHUNKS - 1).wait_recv()
    with jax.named_scope("project"):
        out_ref[...] = (total[...] + project(CHUNKS - 1)).astype(BF16)

    def finish(c, _):
        lax.fori_loop(1, PLANE, lambda d, _: (o2_copy(c, d).wait_send(), 0)[1], 0)
        lax.fori_loop(1, LINE, lambda d, _: (o1_copy(c, d).wait_send(), l1_copy(c, d).wait_send(), 0)[2], 0)
        a_copy(c).wait_send()
        return 0

    with jax.named_scope("finish"):
        lax.fori_loop(0, CHUNKS, finish, 0)
        for part in range(2):
            lax.fori_loop(1, PLANE, lambda d, _: (l2_copy(part, d).wait_send(), 0)[1], 0)


def shards(queries, keys, values, w_out):
    sp_size = lax.axis_size("sp")
    positions = (lax.iota(jnp.int32, ROWS) + lax.axis_index("sp") * ROWS).astype(F32)
    inverse = ROPE_BASE ** (-jnp.arange(0, HEAD, 2, dtype=F32) / HEAD)
    angles = positions[:, None] * inverse[None, :]
    cosine, sine = jnp.cos(angles), jnp.sin(angles)
    cos_table = jnp.concatenate([cosine, cosine], axis=1)
    sin_table = jnp.concatenate([-sine, sine], axis=1)
    n2, n1 = ROWS // PLANE, ROWS // LINE
    dma = pltpu.SemaphoreType.DMA
    vmem = pl.BlockSpec(memory_space=pltpu.VMEM)
    hbm = pl.BlockSpec(memory_space=pl.ANY)
    return pl.pallas_call(
        functools.partial(kernel, sp_size),
        out_shape=jax.ShapeDtypeStruct((ROWS, COLS), BF16),
        in_specs=[vmem, vmem, hbm, hbm, hbm, hbm],
        out_specs=vmem,
        scratch_shapes=[
            pltpu.VMEM((3, ROWS, COLS), BF16),
            pltpu.VMEM((3, ROWS, COLS), BF16),
            pltpu.VMEM((3, ROWS, COLS), BF16),
            pltpu.VMEM((2, COLS, COLS), BF16),
            pltpu.VMEM((PLANE, 3, n2, COLS), BF16),
            pltpu.VMEM((PLANE + 8, 3, n2, COLS), BF16),
            pltpu.VMEM((LINE, 3, n1, COLS), BF16),
            pltpu.VMEM((LINE + 2, 3, n1, COLS), BF16),
            pltpu.VMEM((ROWS, COLS), BF16),
            pltpu.VMEM((ROWS, COLS), BF16),
            pltpu.VMEM((2, BACK, COLS), BF16),
            pltpu.VMEM((BACK, COLS), BF16),
            pltpu.VMEM((2, BACK, COLS), BF16),
            pltpu.VMEM((BACK, HEAD), BF16),
            pltpu.VMEM((2, BACK, HEAD), BF16),
            pltpu.VMEM((PLANE, n2, COLS), BF16),
            pltpu.VMEM((PLANE, n2, COLS), BF16),
            pltpu.VMEM((LINE, n1, COLS), BF16),
            pltpu.VMEM((LINE, n1, COLS), BF16),
            pltpu.VMEM((2, PLANE, n2, HEAD), BF16),
            pltpu.VMEM((2, PLANE, n2, HEAD), BF16),
            pltpu.VMEM((CHUNKS, LINE, n2, HEAD), BF16),
            pltpu.VMEM((CHUNKS, LINE, n2, HEAD), BF16),
            pltpu.VMEM((ROWS, COLS), F32),
            pltpu.VMEM((ROWS, COLS), F32),
            pltpu.VMEM((ROWS, COLS), F32),
            pltpu.VMEM((2, BACK, HEAD), F32),
            pltpu.VMEM((ROWS, COLS), BF16),
            pltpu.VMEM((ROWS, COLS), BF16),
            pltpu.VMEM((ROWS, COLS), F32),
            pltpu.VMEM((3, BACK, 2 * BACK), F32),
            pltpu.VMEM((3, ROWS, ROWS), BF16),
            pltpu.VMEM((ROWS, LINE * HEAD), BF16),
            dma((3, 3)), dma((2,)),
            dma((CHUNKS, PLANE)), dma((CHUNKS, PLANE)), dma((CHUNKS, LINE)), dma((CHUNKS, LINE)),
            dma((CHUNKS,)), dma((CHUNKS,)), dma((CHUNKS,)), dma((CHUNKS,)),
            dma((6,)), dma((6,)),
            dma((CHUNKS, PLANE)), dma((CHUNKS, PLANE)), dma((CHUNKS, LINE)), dma((CHUNKS, LINE)),
            dma((2, PLANE)), dma((2, PLANE)), dma((CHUNKS, LINE)), dma((CHUNKS, LINE)),
            dma((CHUNKS,)), dma((CHUNKS,)),
        ],
        name="attention",
        compiler_params=pltpu.CompilerParams(collective_id=0, has_side_effects=True),
    )(cos_table, sin_table, queries, keys, values, w_out)


def solution(mesh):
    return jax.shard_map(
        shards,
        mesh=mesh,
        in_specs=(P(None, "sp", "tp"), P(None, "sp", "tp"), P(None, "sp", "tp"), P(None, "tp")),
        out_specs=P("sp", "tp"),
        check_vma=False,
    )
```

```python
import functools

import jax
import jax.numpy as jnp
from jax import lax
from jax.experimental import pallas as pl
from jax.experimental.pallas import tpu as pltpu
from jax.sharding import PartitionSpec as P

HEAD = 128
ROPE_BASE = 10000.0
MASKED = -1e30
ROWS = 256
COLS = 1024
HEADS = COLS // HEAD
BACK = 128
PLANE = 16
LINE = 4
CHUNKS = 4
WIDE = COLS // CHUNKS
CHUNK_HEADS = WIDE // HEAD
MESH = pl.DeviceIdType.MESH
BF16 = jnp.bfloat16
F32 = jnp.float32


def arrived(ref, sem):
    pltpu.make_async_copy(ref, ref, sem).wait()


def one_hot(condition):
    return jnp.where(condition, 1.0, 0.0).astype(BF16)


def scoped(name, body, carry, first=0, last=CHUNKS):
    def named(c, carry):
        with jax.named_scope(name):
            return body(c, carry)

    return lax.fori_loop(first, last, named, carry)


def dot(a, b):
    return jnp.dot(a, b, preferred_element_type=F32)


def dot_nt(a, b):
    return lax.dot_general(a, b, (((1,), (1,)), ((), ())), preferred_element_type=F32)


def kernel(
    sp_size,
    cos_ref, sin_ref, q_hbm, k_hbm, v_hbm, w_hbm, out_ref,
    qv, kv, vv, wv, s2, r2, s1, r1, k0, q0, qn, on, ob, ln, lb, o2, b2, o1, b1, l2, lb2, l1, lb1,
    g1, log1, o0, lse0, sum0, own, other, total, band, perms, wanted,
    in_sem, w_sem, s2_send, s2_recv, s1_send, s1_recv, h2_send, h2_recv, h1_send, h1_recv,
    n0_send, n0_recv, o2_send, o2_recv, o1_send, o1_recv, l2_send, l2_recv, l1_send, l1_recv,
    a_send, a_recv,
):
    sp = lax.axis_index("sp")
    tp = lax.axis_index("tp")
    x = lax.rem(sp, LINE)
    y = lax.rem(sp // LINE, LINE)
    j = lax.rem(sp, PLANE)
    plane = sp - j

    def block(distance):
        return lax.rem(sp + distance + sp_size, sp_size)

    def peer(d):
        px = lax.rem(x + d // LINE, LINE)
        py = lax.rem(y + lax.rem(d, LINE), LINE)
        return py * LINE + px

    def mate(d):
        return lax.rem(x + d, LINE)

    def columns(c):
        return pl.ds(pl.multiple_of(c * WIDE, WIDE), WIDE)

    loads = []
    for g in (0, 2, 1):
        for i, (src, dst) in enumerate(((q_hbm, qv), (k_hbm, kv), (v_hbm, vv))):
            loads.append(pltpu.make_async_copy(src.at[g], dst.at[g], in_sem.at[g, i]))
    for copy in loads:
        copy.start()
    w_copies = [
        pltpu.make_async_copy(w_hbm.at[pl.ds(pl.multiple_of(half * COLS, COLS), COLS)], wv.at[n], w_sem.at[n])
        for n, half in enumerate((tp, 1 - tp))
    ]
    for copy in w_copies:
        copy.start()

    barrier = pltpu.get_barrier_semaphore()

    def greet(d, _):
        pl.semaphore_signal(barrier, inc=1, device_id=(plane + peer(d), tp), device_id_type=MESH)
        return 0

    lax.fori_loop(1, PLANE, greet, 0)
    for distance in (LINE, PLANE):
        for sign in (1, -1):
            pl.semaphore_signal(barrier, inc=1, device_id=(block(sign * distance), tp), device_id_type=MESH)
    pl.semaphore_signal(barrier, inc=1, device_id=(sp, 1 - tp), device_id_type=MESH)

    q_index = lax.broadcasted_iota(jnp.int32, (BACK, 2 * BACK), 0)
    k_index = lax.broadcasted_iota(jnp.int32, (BACK, 2 * BACK), 1)
    inside = (k_index >= q_index) & (k_index <= q_index + BACK)
    base = jnp.where(inside, 0.0, MASKED)
    band[0] = base
    for g, reach in ((1, LINE), (2, PLANE)):
        opening = jnp.where(sp >= reach, 0.0, MASKED)
        band[g] = jnp.where(k_index < BACK, base + opening, base)

    row = lax.broadcasted_iota(jnp.int32, (ROWS, ROWS), 0)
    col = lax.broadcasted_iota(jnp.int32, (ROWS, ROWS), 1)
    n2 = ROWS // PLANE
    n1 = ROWS // LINE

    perms[0] = one_hot(col == PLANE * (row % n2) + row // n2)
    perms[1] = one_hot(col == LINE * (row % n1) + row // n1)
    perms[2] = one_hot(row == LINE * (col % n1) + col // n1)
    token = lax.broadcasted_iota(jnp.int32, (ROWS, LINE * HEAD), 0)
    lane1 = lax.broadcasted_iota(jnp.int32, (ROWS, LINE * HEAD), 1)
    wanted[...] = one_hot(lane1 == (token % LINE) * HEAD + (x % 2) * n1 + token // LINE)

    def turned(piece):
        parts = []
        for h in range(piece.shape[1] // HEAD):
            m = piece[:, h * HEAD : (h + 1) * HEAD].astype(F32)
            parts.append(m * cos_ref[...] + pltpu.roll(m, HEAD // 2, 1) * sin_ref[...])
        return jnp.concatenate(parts, axis=1)

    def prepared(g, c):
        cs = columns(c)
        q = (turned(qv[g, :, cs]) * HEAD**-0.5).astype(BF16)
        k = turned(kv[g, :, cs]).astype(BF16)
        return q, k

    def remote(src, dst, i, device):
        return pltpu.make_async_remote_copy(
            src_ref=src,
            dst_ref=dst,
            send_sem=n0_send.at[i],
            recv_sem=n0_recv.at[i],
            device_id=(device, tp),
            device_id_type=MESH,
        )

    before, after = sp - x + mate(LINE - 1), sp - x + mate(1)

    def q0_copy():
        return remote(q0.at[pl.ds(0, BACK)], qn.at[0], 0, before)

    def q0_relay():
        return remote(qn.at[0], qn.at[1], 1, block(-LINE))

    def on_copy():
        return remote(on, ob.at[0], 2, after)

    def on_relay():
        return remote(ob.at[0], ob.at[1], 3, block(LINE))

    def ln_copy():
        return remote(ln, lb.at[0], 4, after)

    def ln_relay():
        return remote(lb.at[0], lb.at[1], 5, block(LINE))

    q_slot = jnp.where(x == LINE - 1, 1, 0)
    o_slot = jnp.where(x == 0, 1, 0)

    with jax.named_scope("load0"):
        for i in range(3):
            loads[i].wait()

    def g0_out(c, _):
        cs = columns(c)
        q, k = prepared(0, c)
        q0[:, cs] = q
        k0[:, cs] = k
        return 0

    scoped("g0_out", g0_out, 0)
    with jax.named_scope("barrier"):
        pl.semaphore_wait(barrier, PLANE - 1 + 5)
    q0_copy().start()

    def g2_copy(c, d, part):
        what = pl.ds(part, part + 1)
        return pltpu.make_async_remote_copy(
            src_ref=s2.at[peer(d), what, :, columns(c)],
            dst_ref=r2.at[8 + j, what, :, columns(c)],
            send_sem=s2_send.at[part],
            recv_sem=s2_recv.at[part, c],
            device_id=(plane + peer(d), tp),
            device_id_type=MESH,
        )

    def g2_out(c, _):
        cs = columns(c)
        q, k = prepared(2, c)
        order = perms[0]
        for i, m in enumerate((q, k, vv[2, :, cs])):
            s2[:, i, :, cs] = dot(order, m).astype(BF16).reshape(PLANE, n2, WIDE)
        r2[8 + j, :, :, cs] = s2[j, :, :, cs]
        lax.fori_loop(1, PLANE, lambda d, _: (g2_copy(c, d, 1).start(), 0)[1], 0)
        return 0

    def g2_queries(c, _):
        lax.fori_loop(1, PLANE, lambda d, _: (g2_copy(c, d, 0).start(), 0)[1], 0)
        return 0


    def g1_copy(c, d, part):
        what = pl.ds(part, part + 1)
        return pltpu.make_async_remote_copy(
            src_ref=s1.at[mate(d), what, :, columns(c)],
            dst_ref=r1.at[2 + x, what, :, columns(c)],
            send_sem=s1_send.at[part],
            recv_sem=s1_recv.at[part, c],
            device_id=(sp - x + mate(d), tp),
            device_id_type=MESH,
        )

    def g1_out(c, _):
        cs = columns(c)
        q, k = prepared(1, c)
        order = perms[1]
        for i, m in enumerate((q, k, vv[1, :, cs])):
            s1[:, i, :, cs] = dot(order, m).astype(BF16).reshape(LINE, n1, WIDE)
        r1[2 + x, :, :, cs] = s1[x, :, :, cs]
        lax.fori_loop(1, LINE, lambda d, _: (g1_copy(c, d, 1).start(), 0)[1], 0)
        return 0

    def g1_queries(c, _):
        lax.fori_loop(1, LINE, lambda d, _: (g1_copy(c, d, 0).start(), 0)[1], 0)
        return 0

    def send_out(c, _):
        g2_out(c, 0)
        g1_out(c, 0)
        return 0

    for i in range(3, 9):
        loads[i].wait()
    scoped("send_out", send_out, 0, 0, CHUNKS - 1)


    def h2_copy(c):
        return pltpu.make_async_remote_copy(
            src_ref=r2.at[pl.ds(16, 8), pl.ds(1, 2), :, columns(c)],
            dst_ref=r2.at[pl.ds(0, 8), pl.ds(1, 2), :, columns(c)],
            send_sem=h2_send,
            recv_sem=h2_recv.at[c],
            device_id=(block(PLANE), tp),
            device_id_type=MESH,
        )

    def h1_copy(c):
        return pltpu.make_async_remote_copy(
            src_ref=r1.at[pl.ds(4, 2), pl.ds(1, 2), :, columns(c)],
            dst_ref=r1.at[pl.ds(0, 2), pl.ds(1, 2), :, columns(c)],
            send_sem=h1_send,
            recv_sem=h1_recv.at[c],
            device_id=(block(LINE), tp),
            device_id_type=MESH,
        )

    def attend(q, k, v, bias):
        scores = dot_nt(q, k) + bias
        row_max = jnp.max(scores, axis=1, keepdims=True)
        probs = jnp.exp(scores - row_max)
        row_sum = jnp.sum(probs, axis=1, keepdims=True)
        result = dot(probs.astype(BF16), v) / row_sum
        return result, row_max + jnp.log(row_sum)

    lane = lax.broadcasted_iota(jnp.int32, (BACK, HEAD), 1)

    def g2_halo(c, _):
        arrived(r2.at[pl.ds(8, PLANE - 1), pl.ds(1, 2), :, columns(c)], s2_recv.at[1, c])
        h2_copy(c).start()
        return 0

    def g1_halo(c, _):
        arrived(r1.at[pl.ds(2, LINE - 1), pl.ds(1, 2), :, columns(c)], s1_recv.at[1, c])
        h1_copy(c).start()
        return 0

    def rung(d):
        return lax.rem(y + d, LINE)

    def o2_copy(c, d):
        return pltpu.make_async_remote_copy(
            src_ref=o2.at[pl.ds(LINE * rung(d), LINE), :, columns(c)],
            dst_ref=b2.at[pl.ds(LINE * y, LINE), :, columns(c)],
            send_sem=o2_send,
            recv_sem=o2_recv.at[c],
            device_id=(plane + rung(d) * LINE + x, tp),
            device_id_type=MESH,
        )

    def l2_copy(c, d):
        return pltpu.make_async_remote_copy(
            src_ref=l2.at[c, pl.ds(LINE * rung(d), LINE)],
            dst_ref=lb2.at[c, pl.ds(LINE * y, LINE)],
            send_sem=l2_send,
            recv_sem=l2_recv.at[c],
            device_id=(plane + rung(d) * LINE + x, tp),
            device_id_type=MESH,
        )

    def o1_copy(c, d):
        return pltpu.make_async_remote_copy(
            src_ref=o1.at[mate(d), :, columns(c)],
            dst_ref=b1.at[x, :, columns(c)],
            send_sem=o1_send,
            recv_sem=o1_recv.at[c],
            device_id=(sp - x + mate(d), tp),
            device_id_type=MESH,
        )

    def l1_copy(c, d):
        return pltpu.make_async_remote_copy(
            src_ref=l1.at[c, mate(d)],
            dst_ref=lb1.at[c, x],
            send_sem=l1_send,
            recv_sem=l1_recv.at[c],
            device_id=(sp - x + mate(d), tp),
            device_id_type=MESH,
        )

    def split_terms(lse, heads):
        high = lse.astype(BF16).astype(F32)
        rest = lse - high
        middle = rest.astype(BF16).astype(F32)
        low = rest - middle
        return (high + pltpu.roll(middle, heads, 1) + pltpu.roll(low, 2 * heads, 1)).astype(BF16)

    def place(lses, b, head, lse):
        lses[b] = jnp.where(lane == head, lse, lses[b])

    def g2_attend(c, _):
        with jax.named_scope("wait_h2"):
            h2_copy(c).wait_recv()
        with jax.named_scope("wait_q2"):
            arrived(r2.at[pl.ds(8, PLANE - 1), pl.ds(0, 1), :, columns(c)], s2_recv.at[0, c])
        lses = list(empty)
        for h in range(CHUNK_HEADS):
            cs = pl.ds(pl.multiple_of(c * WIDE + h * HEAD, HEAD), HEAD)
            for b in range(2):
                q = r2[pl.ds(8 + 8 * b, 8), 0, :, cs].reshape(BACK, HEAD)
                k = r2[pl.ds(8 * b, 16), 1, :, cs].reshape(2 * BACK, HEAD)
                v = r2[pl.ds(8 * b, 16), 2, :, cs].reshape(2 * BACK, HEAD)
                result, lse = attend(q, k, v, band[2 if b == 0 else 0])
                o2[pl.ds(8 * b, 8), :, cs] = result.astype(BF16).reshape(8, n2, HEAD)
                place(lses, b, h, lse)
        for b in range(2):
            l2[c, pl.ds(8 * b, 8)] = split_terms(lses[b], CHUNK_HEADS).reshape(8, n2, HEAD)
        mine = pl.ds(LINE * y, LINE)
        b2[mine, :, columns(c)] = o2[mine, :, columns(c)]
        lb2[c, mine] = l2[c, mine]
        lax.fori_loop(1, LINE, lambda d, _: (o2_copy(c, d).start(), l2_copy(c, d).start(), 0)[2], 0)
        return 0

    def g1_attend(c, _):
        with jax.named_scope("wait_h1"):
            h1_copy(c).wait_recv()
        with jax.named_scope("wait_q1"):
            arrived(r1.at[pl.ds(2, LINE - 1), pl.ds(0, 1), :, columns(c)], s1_recv.at[0, c])
        for h in range(CHUNK_HEADS):
            cs = pl.ds(pl.multiple_of(c * WIDE + h * HEAD, HEAD), HEAD)
            for b in range(2):
                q = r1[pl.ds(2 + 2 * b, 2), 0, :, cs].reshape(BACK, HEAD)
                k = r1[pl.ds(2 * b, 4), 1, :, cs].reshape(2 * BACK, HEAD)
                v = r1[pl.ds(2 * b, 4), 2, :, cs].reshape(2 * BACK, HEAD)
                result, lse = attend(q, k, v, band[1 if b == 0 else 0])
                rows, lanes = pl.ds(BACK * b, BACK), pl.ds(HEAD * h, HEAD)
                g1[rows, lanes] = result
                log1[rows, lanes] = jnp.broadcast_to(lse, (BACK, HEAD))
        return 0

    def join(c, _):
        with jax.named_scope("wait_o2"):
            arrived(b2.at[pl.ds(0, PLANE - LINE), :, columns(c)], o2_recv.at[c])
            arrived(lb2.at[c, pl.ds(0, PLANE - LINE)], l2_recv.at[c])
        cs = columns(c)
        out2 = dot(perms[2], b2[:, :, cs].reshape(ROWS, WIDE))
        terms = dot(perms[2], lb2[c].reshape(ROWS, HEAD)).astype(BF16)
        log2 = dot(terms, spread(HEAD, CHUNK_HEADS, 0))
        top = jnp.maximum(log1[...], log2)
        w1, w2 = jnp.exp(log1[...] - top), jnp.exp(log2 - top)
        weight = w1 + w2
        o1[:, :, cs] = ((w1 * g1[...] + w2 * out2) / weight).astype(BF16).reshape(LINE, n1, WIDE)
        log12 = top + jnp.log(weight)
        slot = lax.broadcasted_iota(jnp.int32, (n2, HEAD), 0)
        chosen = one_hot(slot == lax.broadcasted_iota(jnp.int32, (n2, HEAD), 1))
        for b in range(2):
            lses = list(empty[:1])
            for h in range(CHUNK_HEADS):
                place(lses, 0, h, log12[BACK * b : BACK * (b + 1), HEAD * h : HEAD * (h + 1)])
            turned_terms = dot_nt(chosen, split_terms(lses[0], CHUNK_HEADS)).astype(BF16)
            l1[c, 2 * b] = turned_terms
            l1[c, 2 * b + 1] = turned_terms
        b1[x, :, cs] = o1[x, :, cs]
        lb1[c, x] = l1[c, x]
        lax.fori_loop(1, LINE, lambda d, _: (o1_copy(c, d).start(), l1_copy(c, d).start(), 0)[2], 0)
        return 0

    def spread(terms, heads, first):
        term = lax.broadcasted_iota(jnp.int32, (terms, WIDE), 0)
        feature = lax.broadcasted_iota(jnp.int32, (terms, WIDE), 1)
        return one_hot((term < 3 * heads) & (term % heads == first + feature // HEAD))

    def g0_attend(c, _):
        for h in range(CHUNK_HEADS):
            cs = pl.ds(pl.multiple_of(c * WIDE + h * HEAD, HEAD), HEAD)
            for b in range(2):
                q = q0[pl.ds(BACK * b, BACK), cs]
                k = k0[pl.ds(0, BACK * (b + 1)), cs]
                v = vv[0, pl.ds(0, BACK * (b + 1)), cs]
                result, lse = attend(q, k, v, band[0] if b else band[0, :, BACK:])
                o0[pl.ds(BACK * b, BACK), cs] = result
                lse0[pl.ds(BACK * b, BACK), cs] = jnp.broadcast_to(lse, (BACK, HEAD))
        return 0

    def n0_attend(c, carry):
        lses = list(carry)
        for h in range(CHUNK_HEADS):
            cs = pl.ds(pl.multiple_of(c * WIDE + h * HEAD, HEAD), HEAD)
            k = k0[pl.ds(BACK, BACK), cs]
            v = vv[0, pl.ds(BACK, BACK), cs]
            result, lse = attend(qn[q_slot, :, cs], k, v, band[0, :, :BACK])
            on[:, cs] = result.astype(BF16)
            place(lses, 0, c * CHUNK_HEADS + h, lse)
        return tuple(lses)

    empty = (jnp.zeros((BACK, HEAD), F32), jnp.zeros((BACK, HEAD), F32))

    scoped("g0_attend", g0_attend, 0)
    with jax.named_scope("wait_q0"):
        q0_copy().wait_recv()

    @pl.when(x == LINE - 1)
    def _():
        q0_relay().start()

    def step(c, _):
        with jax.named_scope("g2_halo"):
            g2_halo(c, 0)
        with jax.named_scope("g1_halo"):
            g1_halo(c, 0)

        @pl.when(c == 0)
        def _():
            with jax.named_scope("wait_q0r"):

                @pl.when(x == LINE - 1)
                def _():
                    q0_relay().wait_recv()

            lses = scoped("n0_attend", n0_attend, empty[:1])
            ln[...] = split_terms(lses[0], HEADS)
            on_copy().start()
            ln_copy().start()
            scoped("send_out", send_out, 0, CHUNKS - 1, CHUNKS)
            scoped("g2_queries", g2_queries, 0)
            scoped("g1_queries", g1_queries, 0)

        return 0

    lax.fori_loop(0, CHUNKS, step, 0)
    with jax.named_scope("wait_on"):
        on_copy().wait_recv()
        ln_copy().wait_recv()

        @pl.when(x == 0)
        def _():
            on_relay().start()
            ln_relay().start()

    scoped("g2_attend", g2_attend, 0)

    def last(c, _):
        with jax.named_scope("g1_attend"):
            g1_attend(c, 0)
        with jax.named_scope("join"):
            join(c, 0)
        return 0

    lax.fori_loop(0, CHUNKS, last, 0)

    with jax.named_scope("drain"):
        for part in range(2):
            what = pl.ds(part, part + 1)
            arrived(s2.at[pl.ds(0, PLANE - 1), what], s2_send.at[part])
            arrived(s1.at[pl.ds(0, LINE - 1), what], s1_send.at[part])
        arrived(r2.at[pl.ds(16, 8), pl.ds(1, 2)], h2_send)
        arrived(r1.at[pl.ds(4, 2), pl.ds(1, 2)], h1_send)
    for copy in w_copies:
        copy.wait()
    for copy in (q0_copy(), on_copy(), ln_copy()):
        copy.wait_send()

    @pl.when(x == LINE - 1)
    def _():
        q0_relay().wait_send()


    with jax.named_scope("wait_l"):

        @pl.when(x == 0)
        def _():
            on_relay().wait()
            ln_relay().wait()

    def a_copy(c):
        return pltpu.make_async_remote_copy(
            src_ref=own.at[:, columns(c)],
            dst_ref=other.at[:, columns(c)],
            send_sem=a_send,
            recv_sem=a_recv.at[c],
            device_id=(sp, 1 - tp),
            device_id_type=MESH,
        )

    def project(c):
        cs = columns(c)
        return dot(own[:, cs], wv[0, cs, :]) + dot(other[:, cs], wv[1, cs, :])

    def premerge(c, _):
        cs = columns(c)
        rows = slice(0, BACK)
        log3 = dot(lb[o_slot], spread(HEAD, HEADS, c * CHUNK_HEADS)) + jnp.where(sp >= 1, 0.0, MASKED)
        top = jnp.maximum(lse0[rows, cs], log3)
        w0, w3 = jnp.exp(lse0[rows, cs] - top), jnp.exp(log3 - top)
        o0[rows, cs] = w0 * o0[rows, cs] + w3 * ob[o_slot, :, cs].astype(F32)
        sum0[:, cs] = w0 + w3
        lse0[rows, cs] = top
        return 0

    scoped("premerge", premerge, 0)

    def merge(c, _):
        with jax.named_scope("wait_o1"):
            arrived(b1.at[pl.ds(0, LINE - 1), :, columns(c)], o1_recv.at[c])
            arrived(lb1.at[c, pl.ds(0, LINE - 1)], l1_recv.at[c])
        cs = columns(c)
        out12 = dot(perms[2], b1[:, :, cs].reshape(ROWS, WIDE))
        lanes1 = jnp.concatenate([lb1[c, r] for r in range(LINE)], axis=1)
        log12 = dot(dot_nt(wanted[...], lanes1).astype(BF16), spread(n2, CHUNK_HEADS, 0))
        for half in range(2):
            rows = slice(half * BACK, (half + 1) * BACK)
            top = jnp.maximum(lse0[rows, cs], log12[rows])
            old, new = jnp.exp(lse0[rows, cs] - top), jnp.exp(log12[rows] - top)
            weight = sum0[:, cs] * old + new if half == 0 else old + new
            own[rows, cs] = ((o0[rows, cs] * old + out12[rows] * new) / weight).astype(BF16)
        a_copy(c).start()

        @pl.when(c == 1)
        def _():
            a_copy(0).wait_recv()
            total[...] = project(0)

        @pl.when(c > 1)
        def _():
            a_copy(c - 1).wait_recv()
            total[...] += project(c - 1)

        return 0

    scoped("merge", merge, 0)

    with jax.named_scope("wait_a"):
        a_copy(CHUNKS - 1).wait_recv()
    with jax.named_scope("project"):
        out_ref[...] = (total[...] + project(CHUNKS - 1)).astype(BF16)

    with jax.named_scope("finish"):
        arrived(o2.at[pl.ds(0, PLANE - LINE)], o2_send)
        arrived(l2.at[:, pl.ds(0, PLANE - LINE)], l2_send)
        arrived(o1.at[pl.ds(0, LINE - 1)], o1_send)
        arrived(l1.at[:, pl.ds(0, LINE - 1)], l1_send)
        arrived(own, a_send)


def shards(queries, keys, values, w_out):
    sp_size = lax.axis_size("sp")
    positions = (lax.iota(jnp.int32, ROWS) + lax.axis_index("sp") * ROWS).astype(F32)
    inverse = ROPE_BASE ** (-jnp.arange(0, HEAD, 2, dtype=F32) / HEAD)
    angles = positions[:, None] * inverse[None, :]
    cosine, sine = jnp.cos(angles), jnp.sin(angles)
    cos_table = jnp.concatenate([cosine, cosine], axis=1)
    sin_table = jnp.concatenate([-sine, sine], axis=1)
    n2, n1 = ROWS // PLANE, ROWS // LINE
    dma = pltpu.SemaphoreType.DMA
    vmem = pl.BlockSpec(memory_space=pltpu.VMEM)
    hbm = pl.BlockSpec(memory_space=pl.ANY)
    return pl.pallas_call(
        functools.partial(kernel, sp_size),
        out_shape=jax.ShapeDtypeStruct((ROWS, COLS), BF16),
        in_specs=[vmem, vmem, hbm, hbm, hbm, hbm],
        out_specs=vmem,
        scratch_shapes=[
            pltpu.VMEM((3, ROWS, COLS), BF16),
            pltpu.VMEM((3, ROWS, COLS), BF16),
            pltpu.VMEM((3, ROWS, COLS), BF16),
            pltpu.VMEM((2, COLS, COLS), BF16),
            pltpu.VMEM((PLANE, 3, n2, COLS), BF16),
            pltpu.VMEM((PLANE + 8, 3, n2, COLS), BF16),
            pltpu.VMEM((LINE, 3, n1, COLS), BF16),
            pltpu.VMEM((LINE + 2, 3, n1, COLS), BF16),
            pltpu.VMEM((ROWS, COLS), BF16),
            pltpu.VMEM((ROWS, COLS), BF16),
            pltpu.VMEM((2, BACK, COLS), BF16),
            pltpu.VMEM((BACK, COLS), BF16),
            pltpu.VMEM((2, BACK, COLS), BF16),
            pltpu.VMEM((BACK, HEAD), BF16),
            pltpu.VMEM((2, BACK, HEAD), BF16),
            pltpu.VMEM((PLANE, n2, COLS), BF16),
            pltpu.VMEM((PLANE, n2, COLS), BF16),
            pltpu.VMEM((LINE, n1, COLS), BF16),
            pltpu.VMEM((LINE, n1, COLS), BF16),
            pltpu.VMEM((CHUNKS, PLANE, n2, HEAD), BF16),
            pltpu.VMEM((CHUNKS, PLANE, n2, HEAD), BF16),
            pltpu.VMEM((CHUNKS, LINE, n2, HEAD), BF16),
            pltpu.VMEM((CHUNKS, LINE, n2, HEAD), BF16),
            pltpu.VMEM((ROWS, WIDE), F32),
            pltpu.VMEM((ROWS, WIDE), F32),
            pltpu.VMEM((ROWS, COLS), F32),
            pltpu.VMEM((ROWS, COLS), F32),
            pltpu.VMEM((BACK, COLS), F32),
            pltpu.VMEM((ROWS, COLS), BF16),
            pltpu.VMEM((ROWS, COLS), BF16),
            pltpu.VMEM((ROWS, COLS), F32),
            pltpu.VMEM((3, BACK, 2 * BACK), F32),
            pltpu.VMEM((3, ROWS, ROWS), BF16),
            pltpu.VMEM((ROWS, LINE * HEAD), BF16),
            dma((3, 3)), dma((2,)),
            dma((2,)), dma((2, CHUNKS)), dma((2,)), dma((2, CHUNKS)),
            dma, dma((CHUNKS,)), dma, dma((CHUNKS,)),
            dma((6,)), dma((6,)),
            dma, dma((CHUNKS,)), dma, dma((CHUNKS,)), dma, dma((CHUNKS,)), dma, dma((CHUNKS,)),
            dma, dma((CHUNKS,)),
        ],
        name="attention",
        compiler_params=pltpu.CompilerParams(collective_id=0, has_side_effects=True),
    )(cos_table, sin_table, queries, keys, values, w_out)


def solution(mesh):
    return jax.shard_map(
        shards,
        mesh=mesh,
        in_specs=(P(None, "sp", "tp"), P(None, "sp", "tp"), P(None, "sp", "tp"), P(None, "tp")),
        out_specs=P("sp", "tp"),
        check_vma=False,
    )
```

```python
import functools

import jax
import jax.numpy as jnp
from jax import lax
from jax.experimental import pallas as pl
from jax.experimental.pallas import tpu as pltpu
from jax.sharding import PartitionSpec as P

HEAD = 128
ROPE_BASE = 10000.0
MASKED = -1e30
ROWS = 256
COLS = 1024
HEADS = COLS // HEAD
BACK = 128
PLANE = 16
LINE = 4
CHUNKS = 4
WIDE = COLS // CHUNKS
CHUNK_HEADS = WIDE // HEAD
MESH = pl.DeviceIdType.MESH
BF16 = jnp.bfloat16
F32 = jnp.float32


def arrived(ref, sem):
    pltpu.make_async_copy(ref, ref, sem).wait()


def one_hot(condition):
    return jnp.where(condition, 1.0, 0.0).astype(BF16)


def scoped(name, body, carry, first=0, last=CHUNKS):
    def named(c, carry):
        with jax.named_scope(name):
            return body(c, carry)

    return lax.fori_loop(first, last, named, carry)


def dot(a, b):
    return jnp.dot(a, b, preferred_element_type=F32)


def dot_nt(a, b):
    return lax.dot_general(a, b, (((1,), (1,)), ((), ())), preferred_element_type=F32)


def kernel(
    sp_size,
    inverse_ref, q_hbm, k_hbm, v_hbm, w_hbm, out_ref,
    qv, kv, vv, wv, s2, r2, s1, r1, k0, q0, qn, on, ob, ln, lb, o2, b2, o1, b1, l2, lb2, l1, lb1,
    g1, log1, o0, lse0, sum0, own, other, total, band, perms, wanted, cos_full, sin_full,
    in_sem, w_sem, s2_send, s2_recv, s1_send, s1_recv, h2_send, h2_recv, h1_send, h1_recv,
    n0_send, n0_recv, o2_send, o2_recv, o1_send, o1_recv, l2_send, l2_recv, l1_send, l1_recv,
    a_send, a_recv,
):
    sp = lax.axis_index("sp")
    tp = lax.axis_index("tp")
    x = lax.rem(sp, LINE)
    y = lax.rem(sp // LINE, LINE)
    j = lax.rem(sp, PLANE)
    plane = sp - j

    def block(distance):
        return lax.rem(sp + distance + sp_size, sp_size)

    def peer(d):
        px = lax.rem(x + d // LINE, LINE)
        py = lax.rem(y + lax.rem(d, LINE), LINE)
        return py * LINE + px

    def mate(d):
        return lax.rem(x + d, LINE)

    def columns(c):
        return pl.ds(pl.multiple_of(c * WIDE, WIDE), WIDE)

    loads = []
    for g in (0, 2, 1):
        for i, (src, dst) in enumerate(((q_hbm, qv), (k_hbm, kv), (v_hbm, vv))):
            loads.append(pltpu.make_async_copy(src.at[g], dst.at[g], in_sem.at[g, i]))
    for copy in loads:
        copy.start()
    w_copies = [
        pltpu.make_async_copy(w_hbm.at[pl.ds(pl.multiple_of(half * COLS, COLS), COLS)], wv.at[n], w_sem.at[n])
        for n, half in enumerate((tp, 1 - tp))
    ]
    for copy in w_copies:
        copy.start()

    barrier = pltpu.get_barrier_semaphore()

    def greet(d, _):
        pl.semaphore_signal(barrier, inc=1, device_id=(plane + peer(d), tp), device_id_type=MESH)
        return 0

    lax.fori_loop(1, PLANE, greet, 0)
    for distance in (LINE, PLANE):
        for sign in (1, -1):
            pl.semaphore_signal(barrier, inc=1, device_id=(block(sign * distance), tp), device_id_type=MESH)
    pl.semaphore_signal(barrier, inc=1, device_id=(sp, 1 - tp), device_id_type=MESH)

    q_index = lax.broadcasted_iota(jnp.int32, (BACK, 2 * BACK), 0)
    k_index = lax.broadcasted_iota(jnp.int32, (BACK, 2 * BACK), 1)
    inside = (k_index >= q_index) & (k_index <= q_index + BACK)
    base = jnp.where(inside, 0.0, MASKED)
    band[0] = base
    for g, reach in ((1, LINE), (2, PLANE)):
        opening = jnp.where(sp >= reach, 0.0, MASKED)
        band[g] = jnp.where(k_index < BACK, base + opening, base)

    row = lax.broadcasted_iota(jnp.int32, (ROWS, ROWS), 0)
    col = lax.broadcasted_iota(jnp.int32, (ROWS, ROWS), 1)
    n2 = ROWS // PLANE
    n1 = ROWS // LINE

    perms[0] = one_hot(col == PLANE * (row % n2) + row // n2)
    perms[1] = one_hot(col == LINE * (row % n1) + row // n1)
    perms[2] = one_hot(row == LINE * (col % n1) + col // n1)
    token = lax.broadcasted_iota(jnp.int32, (ROWS, LINE * HEAD), 0)
    lane1 = lax.broadcasted_iota(jnp.int32, (ROWS, LINE * HEAD), 1)
    for which, half in enumerate((x % 2, y % 2)):
        wanted[which] = one_hot(lane1 == (token % LINE) * HEAD + half * n1 + token // LINE)

    position = (lax.broadcasted_iota(jnp.int32, (ROWS, HEAD), 0) + sp * ROWS).astype(F32)
    feature = lax.broadcasted_iota(jnp.int32, (ROWS, HEAD), 1)
    inverse = inverse_ref[...]
    angles = position * jnp.concatenate([inverse, inverse], axis=1)
    sine = jnp.sin(angles)
    cos_full[...] = jnp.cos(angles)
    sin_full[...] = jnp.where(feature < HEAD // 2, -sine, sine)

    def turned(piece):
        parts = []
        for h in range(piece.shape[1] // HEAD):
            m = piece[:, h * HEAD : (h + 1) * HEAD].astype(F32)
            parts.append(m * cos_full[...] + pltpu.roll(m, HEAD // 2, 1) * sin_full[...])
        return jnp.concatenate(parts, axis=1)

    def prepared(g, c):
        cs = columns(c)
        q = (turned(qv[g, :, cs]) * HEAD**-0.5).astype(BF16)
        k = turned(kv[g, :, cs]).astype(BF16)
        return q, k

    def remote(src, dst, i, device):
        return pltpu.make_async_remote_copy(
            src_ref=src,
            dst_ref=dst,
            send_sem=n0_send.at[i],
            recv_sem=n0_recv.at[i],
            device_id=(device, tp),
            device_id_type=MESH,
        )

    before, after = sp - x + mate(LINE - 1), sp - x + mate(1)

    def q0_copy():
        return remote(q0.at[pl.ds(0, BACK)], qn.at[0], 0, before)

    def q0_relay():
        return remote(qn.at[0], qn.at[1], 1, block(-LINE))

    near, far = pl.ds(0, COLS // 2), pl.ds(COLS // 2, COLS // 2)

    def on_near():
        return remote(on.at[:, near], ob.at[0, :, near], 2, after)

    def on_near_relay():
        return remote(ob.at[0, :, near], ob.at[1, :, near], 3, block(LINE))

    def on_far():
        return remote(on.at[:, far], ob.at[0, :, far], 6, after)

    def on_far_turn():
        return remote(on.at[:, far], ob.at[1, :, far], 7, block(LINE))

    def on_far_relay():
        return remote(ob.at[1, :, far], ob.at[1, :, far], 8, after)

    def ln_copy():
        return remote(ln, lb.at[0], 4, after)

    def ln_relay():
        return remote(lb.at[0], lb.at[1], 5, block(LINE))

    q_slot = jnp.where(x == LINE - 1, 1, 0)
    o_slot = jnp.where(x == 0, 1, 0)

    with jax.named_scope("load0"):
        for i in range(3):
            loads[i].wait()

    def g0_out(c, _):
        cs = columns(c)
        q, k = prepared(0, c)
        q0[:, cs] = q
        k0[:, cs] = k
        return 0

    scoped("g0_out", g0_out, 0)
    with jax.named_scope("barrier"):
        pl.semaphore_wait(barrier, PLANE - 1 + 5)
    q0_copy().start()

    def g2_copy(c, d, part):
        what = pl.ds(part, part + 1)
        return pltpu.make_async_remote_copy(
            src_ref=s2.at[peer(d), what, :, columns(c)],
            dst_ref=r2.at[8 + j, what, :, columns(c)],
            send_sem=s2_send.at[part],
            recv_sem=s2_recv.at[part, c],
            device_id=(plane + peer(d), tp),
            device_id_type=MESH,
        )

    def g2_out(c, _):
        cs = columns(c)
        q, k = prepared(2, c)
        order = perms[0]
        for i, m in enumerate((q, k, vv[2, :, cs])):
            s2[:, i, :, cs] = dot(order, m).astype(BF16).reshape(PLANE, n2, WIDE)
        r2[8 + j, :, :, cs] = s2[j, :, :, cs]
        lax.fori_loop(1, PLANE, lambda d, _: (g2_copy(c, d, 1).start(), 0)[1], 0)
        return 0

    def g2_queries(c, _):
        lax.fori_loop(1, PLANE, lambda d, _: (g2_copy(c, d, 0).start(), 0)[1], 0)
        return 0


    def g1_copy(c, d, part):
        what = pl.ds(part, part + 1)
        return pltpu.make_async_remote_copy(
            src_ref=s1.at[mate(d), what, :, columns(c)],
            dst_ref=r1.at[2 + x, what, :, columns(c)],
            send_sem=s1_send.at[part],
            recv_sem=s1_recv.at[part, c],
            device_id=(sp - x + mate(d), tp),
            device_id_type=MESH,
        )

    def g1_out(c, _):
        cs = columns(c)
        q, k = prepared(1, c)
        order = perms[1]
        for i, m in enumerate((q, k, vv[1, :, cs])):
            s1[:, i, :, cs] = dot(order, m).astype(BF16).reshape(LINE, n1, WIDE)
        r1[2 + x, :, :, cs] = s1[x, :, :, cs]
        lax.fori_loop(1, LINE, lambda d, _: (g1_copy(c, d, 1).start(), 0)[1], 0)
        return 0

    def g1_queries(c, _):
        lax.fori_loop(1, LINE, lambda d, _: (g1_copy(c, d, 0).start(), 0)[1], 0)
        return 0

    def send_out(c, _):
        g2_out(c, 0)
        g1_out(c, 0)
        return 0

    for i in range(3, 9):
        loads[i].wait()
    scoped("send_out", send_out, 0)
    scoped("g2_queries", g2_queries, 0)


    def h2_copy(c):
        return pltpu.make_async_remote_copy(
            src_ref=r2.at[pl.ds(16, 8), pl.ds(1, 2), :, columns(c)],
            dst_ref=r2.at[pl.ds(0, 8), pl.ds(1, 2), :, columns(c)],
            send_sem=h2_send,
            recv_sem=h2_recv.at[c],
            device_id=(block(PLANE), tp),
            device_id_type=MESH,
        )

    def h1_copy(c):
        return pltpu.make_async_remote_copy(
            src_ref=r1.at[pl.ds(4, 2), pl.ds(1, 2), :, columns(c)],
            dst_ref=r1.at[pl.ds(0, 2), pl.ds(1, 2), :, columns(c)],
            send_sem=h1_send,
            recv_sem=h1_recv.at[c],
            device_id=(block(LINE), tp),
            device_id_type=MESH,
        )

    def attend(q, k, v, bias):
        scores = dot_nt(q, k) + bias
        row_max = jnp.max(scores, axis=1, keepdims=True)
        probs = jnp.exp(scores - row_max)
        row_sum = jnp.sum(probs, axis=1, keepdims=True)
        result = dot(probs.astype(BF16), v) / row_sum
        return result, row_max + jnp.log(row_sum)

    lane = lax.broadcasted_iota(jnp.int32, (BACK, HEAD), 1)

    def g2_halo(c, _):
        arrived(r2.at[pl.ds(8, PLANE - 1), pl.ds(1, 2), :, columns(c)], s2_recv.at[1, c])
        h2_copy(c).start()
        return 0

    def g1_halo(c, _):
        arrived(r1.at[pl.ds(2, LINE - 1), pl.ds(1, 2), :, columns(c)], s1_recv.at[1, c])
        h1_copy(c).start()
        return 0

    def rung(d):
        return lax.rem(y + d, LINE)

    def o2_copy(c, d):
        return pltpu.make_async_remote_copy(
            src_ref=o2.at[pl.ds(LINE * rung(d), LINE), :, columns(c)],
            dst_ref=b2.at[pl.ds(LINE * y, LINE), :, columns(c)],
            send_sem=o2_send,
            recv_sem=o2_recv.at[c],
            device_id=(plane + rung(d) * LINE + x, tp),
            device_id_type=MESH,
        )

    def l2_copy(c, d):
        return pltpu.make_async_remote_copy(
            src_ref=l2.at[c, rung(d)],
            dst_ref=lb2.at[c, y],
            send_sem=l2_send,
            recv_sem=l2_recv.at[c],
            device_id=(plane + rung(d) * LINE + x, tp),
            device_id_type=MESH,
        )

    def o1_copy(c, d):
        return pltpu.make_async_remote_copy(
            src_ref=o1.at[mate(d), :, columns(c)],
            dst_ref=b1.at[x, :, columns(c)],
            send_sem=o1_send,
            recv_sem=o1_recv.at[c],
            device_id=(sp - x + mate(d), tp),
            device_id_type=MESH,
        )

    def l1_copy(c, d):
        return pltpu.make_async_remote_copy(
            src_ref=l1.at[c, mate(d)],
            dst_ref=lb1.at[c, x],
            send_sem=l1_send,
            recv_sem=l1_recv.at[c],
            device_id=(sp - x + mate(d), tp),
            device_id_type=MESH,
        )

    def split_terms(lse, heads):
        high = lse.astype(BF16).astype(F32)
        rest = lse - high
        middle = rest.astype(BF16).astype(F32)
        low = rest - middle
        return (high + pltpu.roll(middle, heads, 1) + pltpu.roll(low, 2 * heads, 1)).astype(BF16)

    def place(lses, b, head, lse):
        lses[b] = jnp.where(lane == head, lse, lses[b])

    def pack(target, c, lses):
        slot = lax.broadcasted_iota(jnp.int32, (n2, HEAD), 0)
        chosen = one_hot(slot == lax.broadcasted_iota(jnp.int32, (n2, HEAD), 1))
        for b in range(2):
            tile = dot_nt(chosen, split_terms(lses[b], CHUNK_HEADS)).astype(BF16)
            target[c, 2 * b] = tile
            target[c, 2 * b + 1] = tile

    def unpack(tiles, c, which):
        lanes = jnp.concatenate([tiles[c, r] for r in range(LINE)], axis=1)
        return dot(dot_nt(wanted[which], lanes).astype(BF16), spread(n2, CHUNK_HEADS, 0))

    def g2_attend(c, _):
        with jax.named_scope("wait_h2"):
            h2_copy(c).wait_recv()
        with jax.named_scope("wait_q2"):
            arrived(r2.at[pl.ds(8, PLANE - 1), pl.ds(0, 1), :, columns(c)], s2_recv.at[0, c])
        lses = list(empty)
        for h in range(CHUNK_HEADS):
            cs = pl.ds(pl.multiple_of(c * WIDE + h * HEAD, HEAD), HEAD)
            for b in range(2):
                q = r2[pl.ds(8 + 8 * b, 8), 0, :, cs].reshape(BACK, HEAD)
                k = r2[pl.ds(8 * b, 16), 1, :, cs].reshape(2 * BACK, HEAD)
                v = r2[pl.ds(8 * b, 16), 2, :, cs].reshape(2 * BACK, HEAD)
                result, lse = attend(q, k, v, band[2 if b == 0 else 0])
                o2[pl.ds(8 * b, 8), :, cs] = result.astype(BF16).reshape(8, n2, HEAD)
                place(lses, b, h, lse)
        pack(l2, c, lses)
        mine = pl.ds(LINE * y, LINE)
        b2[mine, :, columns(c)] = o2[mine, :, columns(c)]
        lb2[c, y] = l2[c, y]
        lax.fori_loop(1, LINE, lambda d, _: (o2_copy(c, d).start(), l2_copy(c, d).start(), 0)[2], 0)
        return 0

    def g1_attend(c, _):
        with jax.named_scope("wait_h1"):
            h1_copy(c).wait_recv()
        with jax.named_scope("wait_q1"):
            arrived(r1.at[pl.ds(2, LINE - 1), pl.ds(0, 1), :, columns(c)], s1_recv.at[0, c])
        for h in range(CHUNK_HEADS):
            cs = pl.ds(pl.multiple_of(c * WIDE + h * HEAD, HEAD), HEAD)
            for b in range(2):
                q = r1[pl.ds(2 + 2 * b, 2), 0, :, cs].reshape(BACK, HEAD)
                k = r1[pl.ds(2 * b, 4), 1, :, cs].reshape(2 * BACK, HEAD)
                v = r1[pl.ds(2 * b, 4), 2, :, cs].reshape(2 * BACK, HEAD)
                result, lse = attend(q, k, v, band[1 if b == 0 else 0])
                rows, lanes = pl.ds(BACK * b, BACK), pl.ds(HEAD * h, HEAD)
                g1[lax.rem(c, 2), rows, lanes] = result
                log1[lax.rem(c, 2), rows, lanes] = jnp.broadcast_to(lse, (BACK, HEAD))
        return 0

    def join(c, _):
        with jax.named_scope("wait_o2"):
            arrived(b2.at[pl.ds(0, PLANE - LINE), :, columns(c)], o2_recv.at[c])
            arrived(lb2.at[c, pl.ds(0, LINE - 1)], l2_recv.at[c])
        cs = columns(c)
        out2 = dot(perms[2], b2[:, :, cs].reshape(ROWS, WIDE))
        log2 = unpack(lb2, c, 1)
        here = lax.rem(c, 2)
        top = jnp.maximum(log1[here], log2)
        w1, w2 = jnp.exp(log1[here] - top), jnp.exp(log2 - top)
        weight = w1 + w2
        o1[:, :, cs] = ((w1 * g1[here] + w2 * out2) / weight).astype(BF16).reshape(LINE, n1, WIDE)
        log12 = top + jnp.log(weight)
        lses = list(empty)
        for b in range(2):
            for h in range(CHUNK_HEADS):
                place(lses, b, h, log12[BACK * b : BACK * (b + 1), HEAD * h : HEAD * (h + 1)])
        pack(l1, c, lses)
        b1[x, :, cs] = o1[x, :, cs]
        lb1[c, x] = l1[c, x]
        lax.fori_loop(1, LINE, lambda d, _: (o1_copy(c, d).start(), l1_copy(c, d).start(), 0)[2], 0)
        return 0

    def spread(terms, heads, first):
        term = lax.broadcasted_iota(jnp.int32, (terms, WIDE), 0)
        feature = lax.broadcasted_iota(jnp.int32, (terms, WIDE), 1)
        return one_hot((term < 3 * heads) & (term % heads == first + feature // HEAD))

    def g0_attend(c, _):
        for h in range(CHUNK_HEADS):
            cs = pl.ds(pl.multiple_of(c * WIDE + h * HEAD, HEAD), HEAD)
            for b in range(2):
                q = q0[pl.ds(BACK * b, BACK), cs]
                k = k0[pl.ds(0, BACK * (b + 1)), cs]
                v = vv[0, pl.ds(0, BACK * (b + 1)), cs]
                result, lse = attend(q, k, v, band[0] if b else band[0, :, BACK:])
                o0[pl.ds(BACK * b, BACK), cs] = result
                lse0[pl.ds(BACK * b, BACK), cs] = jnp.broadcast_to(lse, (BACK, HEAD))
        return 0

    def n0_attend(c, carry):
        lses = list(carry)
        for h in range(CHUNK_HEADS):
            cs = pl.ds(pl.multiple_of(c * WIDE + h * HEAD, HEAD), HEAD)
            k = k0[pl.ds(BACK, BACK), cs]
            v = vv[0, pl.ds(BACK, BACK), cs]
            result, lse = attend(qn[q_slot, :, cs], k, v, band[0, :, :BACK])
            on[:, cs] = result.astype(BF16)
            place(lses, 0, c * CHUNK_HEADS + h, lse)
        return tuple(lses)

    empty = (jnp.zeros((BACK, HEAD), F32), jnp.zeros((BACK, HEAD), F32))

    scoped("g0_attend", g0_attend, 0)
    with jax.named_scope("wait_q0"):
        q0_copy().wait_recv()

    @pl.when(x == LINE - 1)
    def _():
        q0_relay().start()

    def step(c, _):
        with jax.named_scope("g2_halo"):
            g2_halo(c, 0)
        with jax.named_scope("g1_halo"):
            g1_halo(c, 0)

        @pl.when(c == 1)
        def _():
            with jax.named_scope("wait_q0r"):

                @pl.when(x == LINE - 1)
                def _():
                    q0_relay().wait_recv()

            lses = scoped("n0_attend", n0_attend, empty[:1])
            ln[...] = split_terms(lses[0], HEADS)
            on_near().start()
            ln_copy().start()

            @pl.when(x < LINE - 1)
            def _():
                on_far().start()

            @pl.when(x == LINE - 1)
            def _():
                on_far_turn().start()


        return 0

    lax.fori_loop(0, CHUNKS, step, 0)
    with jax.named_scope("wait_far"):

        @pl.when(x == LINE - 1)
        def _():
            on_far_turn().wait_recv()
            on_far_relay().start()

    scoped("g1_queries", g1_queries, 0)

    def g2_step(c, _):
        @pl.when((c == 2) & (x == 0))
        def _():
            with jax.named_scope("wait_on"):
                on_near().wait_recv()
                ln_copy().wait_recv()
                on_near_relay().start()
                ln_relay().start()

        with jax.named_scope("g2_attend"):
            g2_attend(c, 0)
        return 0

    lax.fori_loop(0, CHUNKS, g2_step, 0)

    def last(c, _):
        @pl.when(c < CHUNKS)
        def _():
            with jax.named_scope("g1_attend"):
                g1_attend(c, 0)

        @pl.when(c > 0)
        def _():
            with jax.named_scope("join"):
                join(c - 1, 0)

        return 0

    lax.fori_loop(0, CHUNKS + 1, last, 0)

    with jax.named_scope("drain"):
        for part in range(2):
            what = pl.ds(part, part + 1)
            arrived(s2.at[pl.ds(0, PLANE - 1), what], s2_send.at[part])
            arrived(s1.at[pl.ds(0, LINE - 1), what], s1_send.at[part])
        arrived(r2.at[pl.ds(16, 8), pl.ds(1, 2)], h2_send)
        arrived(r1.at[pl.ds(4, 2), pl.ds(1, 2)], h1_send)
    for copy in w_copies:
        copy.wait()
    for copy in (q0_copy(), on_near(), ln_copy()):
        copy.wait_send()

    @pl.when(x == LINE - 1)
    def _():
        q0_relay().wait_send()
        on_far_turn().wait_send()
        on_far_relay().wait_send()

    @pl.when(x < LINE - 1)
    def _():
        on_far().wait_send()


    with jax.named_scope("wait_l"):

        @pl.when(x == 0)
        def _():
            on_near_relay().wait()
            on_far_relay().wait_recv()
            ln_relay().wait()

        @pl.when(x > 0)
        def _():
            on_near().wait_recv()
            on_far().wait_recv()
            ln_copy().wait_recv()

    def a_copy(c):
        return pltpu.make_async_remote_copy(
            src_ref=own.at[:, columns(c)],
            dst_ref=other.at[:, columns(c)],
            send_sem=a_send,
            recv_sem=a_recv.at[c],
            device_id=(sp, 1 - tp),
            device_id_type=MESH,
        )

    def project(c):
        cs = columns(c)
        return dot(own[:, cs], wv[0, cs, :]) + dot(other[:, cs], wv[1, cs, :])

    def premerge(c, _):
        cs = columns(c)
        rows = slice(0, BACK)
        log3 = dot(lb[o_slot], spread(HEAD, HEADS, c * CHUNK_HEADS)) + jnp.where(sp >= 1, 0.0, MASKED)
        top = jnp.maximum(lse0[rows, cs], log3)
        w0, w3 = jnp.exp(lse0[rows, cs] - top), jnp.exp(log3 - top)
        o0[rows, cs] = w0 * o0[rows, cs] + w3 * ob[o_slot, :, cs].astype(F32)
        sum0[:, cs] = w0 + w3
        lse0[rows, cs] = top
        return 0

    scoped("premerge", premerge, 0)

    def merge(c, _):
        with jax.named_scope("wait_o1"):
            arrived(b1.at[pl.ds(0, LINE - 1), :, columns(c)], o1_recv.at[c])
            arrived(lb1.at[c, pl.ds(0, LINE - 1)], l1_recv.at[c])
        cs = columns(c)
        out12 = dot(perms[2], b1[:, :, cs].reshape(ROWS, WIDE))
        log12 = unpack(lb1, c, 0)
        for half in range(2):
            rows = slice(half * BACK, (half + 1) * BACK)
            top = jnp.maximum(lse0[rows, cs], log12[rows])
            old, new = jnp.exp(lse0[rows, cs] - top), jnp.exp(log12[rows] - top)
            weight = sum0[:, cs] * old + new if half == 0 else old + new
            own[rows, cs] = ((o0[rows, cs] * old + out12[rows] * new) / weight).astype(BF16)
        a_copy(c).start()

        @pl.when(c == 1)
        def _():
            a_copy(0).wait_recv()
            total[...] = project(0)

        @pl.when(c > 1)
        def _():
            a_copy(c - 1).wait_recv()
            total[...] += project(c - 1)

        return 0

    scoped("merge", merge, 0)

    with jax.named_scope("wait_a"):
        a_copy(CHUNKS - 1).wait_recv()
    with jax.named_scope("project"):
        out_ref[...] = (total[...] + project(CHUNKS - 1)).astype(BF16)

    with jax.named_scope("finish"):
        arrived(o2.at[pl.ds(0, PLANE - LINE)], o2_send)
        arrived(l2.at[:, pl.ds(0, LINE - 1)], l2_send)
        arrived(o1.at[pl.ds(0, LINE - 1)], o1_send)
        arrived(l1.at[:, pl.ds(0, LINE - 1)], l1_send)
        arrived(own, a_send)


def shards(queries, keys, values, w_out):
    sp_size = lax.axis_size("sp")
    inverse = ROPE_BASE ** (-jnp.arange(0, HEAD, 2, dtype=F32) / HEAD)
    n2, n1 = ROWS // PLANE, ROWS // LINE
    dma = pltpu.SemaphoreType.DMA
    vmem = pl.BlockSpec(memory_space=pltpu.VMEM)
    hbm = pl.BlockSpec(memory_space=pl.ANY)
    return pl.pallas_call(
        functools.partial(kernel, sp_size),
        out_shape=pltpu.VMEM((ROWS, COLS), BF16),
        in_specs=[vmem, hbm, hbm, hbm, hbm],
        out_specs=vmem,
        scratch_shapes=[
            pltpu.VMEM((3, ROWS, COLS), BF16),
            pltpu.VMEM((3, ROWS, COLS), BF16),
            pltpu.VMEM((3, ROWS, COLS), BF16),
            pltpu.VMEM((2, COLS, COLS), BF16),
            pltpu.VMEM((PLANE, 3, n2, COLS), BF16),
            pltpu.VMEM((PLANE + 8, 3, n2, COLS), BF16),
            pltpu.VMEM((LINE, 3, n1, COLS), BF16),
            pltpu.VMEM((LINE + 2, 3, n1, COLS), BF16),
            pltpu.VMEM((ROWS, COLS), BF16),
            pltpu.VMEM((ROWS, COLS), BF16),
            pltpu.VMEM((2, BACK, COLS), BF16),
            pltpu.VMEM((BACK, COLS), BF16),
            pltpu.VMEM((2, BACK, COLS), BF16),
            pltpu.VMEM((BACK, HEAD), BF16),
            pltpu.VMEM((2, BACK, HEAD), BF16),
            pltpu.VMEM((PLANE, n2, COLS), BF16),
            pltpu.VMEM((PLANE, n2, COLS), BF16),
            pltpu.VMEM((LINE, n1, COLS), BF16),
            pltpu.VMEM((LINE, n1, COLS), BF16),
            pltpu.VMEM((CHUNKS, LINE, n2, HEAD), BF16),
            pltpu.VMEM((CHUNKS, LINE, n2, HEAD), BF16),
            pltpu.VMEM((CHUNKS, LINE, n2, HEAD), BF16),
            pltpu.VMEM((CHUNKS, LINE, n2, HEAD), BF16),
            pltpu.VMEM((2, ROWS, WIDE), F32),
            pltpu.VMEM((2, ROWS, WIDE), F32),
            pltpu.VMEM((ROWS, COLS), F32),
            pltpu.VMEM((ROWS, COLS), F32),
            pltpu.VMEM((BACK, COLS), F32),
            pltpu.VMEM((ROWS, COLS), BF16),
            pltpu.VMEM((ROWS, COLS), BF16),
            pltpu.VMEM((ROWS, COLS), F32),
            pltpu.VMEM((3, BACK, 2 * BACK), F32),
            pltpu.VMEM((3, ROWS, ROWS), BF16),
            pltpu.VMEM((2, ROWS, LINE * HEAD), BF16),
            pltpu.VMEM((ROWS, HEAD), F32),
            pltpu.VMEM((ROWS, HEAD), F32),
            dma((3, 3)), dma((2,)),
            dma((2,)), dma((2, CHUNKS)), dma((2,)), dma((2, CHUNKS)),
            dma, dma((CHUNKS,)), dma, dma((CHUNKS,)),
            dma((9,)), dma((9,)),
            dma, dma((CHUNKS,)), dma, dma((CHUNKS,)), dma, dma((CHUNKS,)), dma, dma((CHUNKS,)),
            dma, dma((CHUNKS,)),
        ],
        name="attention",
        compiler_params=pltpu.CompilerParams(collective_id=0, has_side_effects=True),
    )(inverse[None, :], queries, keys, values, w_out)


def solution(mesh):
    return jax.shard_map(
        shards,
        mesh=mesh,
        in_specs=(P(None, "sp", "tp"), P(None, "sp", "tp"), P(None, "sp", "tp"), P(None, "tp")),
        out_specs=P("sp", "tp"),
        check_vma=False,
    )
```

```python
import functools

import jax
import jax.numpy as jnp
from jax import lax
from jax.experimental import pallas as pl
from jax.experimental.pallas import tpu as pltpu
from jax.sharding import PartitionSpec as P

HEAD = 128
ROPE_BASE = 10000.0
MASKED = -1e30
ROWS = 256
COLS = 1024
HEADS = COLS // HEAD
BACK = 128
PLANE = 16
LINE = 4
CHUNKS = 4
WIDE = COLS // CHUNKS
CHUNK_HEADS = WIDE // HEAD
MESH = pl.DeviceIdType.MESH
BF16 = jnp.bfloat16
F32 = jnp.float32


def arrived(ref, sem):
    pltpu.make_async_copy(ref, ref, sem).wait()


def one_hot(condition):
    return jnp.where(condition, 1.0, 0.0).astype(BF16)


def scoped(name, body, carry, first=0, last=CHUNKS):
    def named(c, carry):
        with jax.named_scope(name):
            return body(c, carry)

    return lax.fori_loop(first, last, named, carry)


def dot(a, b):
    return jnp.dot(a, b, preferred_element_type=F32)


def dot_nt(a, b):
    return lax.dot_general(a, b, (((1,), (1,)), ((), ())), preferred_element_type=F32)


def kernel(
    sp_size,
    inverse_ref, q_hbm, k_hbm, v_hbm, w_hbm, out_ref,
    qv, kv, vv, wv, s2, r2, s1, r1, k0, q0, qn, on, ob, ln, lb, o2, b2, o1, b1, l2, lb2, l1, lb1,
    g1, log1, o0, lse0, sum0, own, other, total, band, perms, wanted, cos_full, sin_full,
    in_sem, w_sem, s2_send, s2_recv, s1_send, s1_recv, h2_send, h2_recv, h1_send, h1_recv,
    n0_send, n0_recv, o2_send, o2_recv, o1_send, o1_recv, l2_send, l2_recv, l1_send, l1_recv,
    a_send, a_recv, next_ready, row_ready,
):
    sp = lax.axis_index("sp")
    tp = lax.axis_index("tp")
    x = lax.rem(sp, LINE)
    y = lax.rem(sp // LINE, LINE)
    j = lax.rem(sp, PLANE)
    plane = sp - j

    def block(distance):
        return lax.rem(sp + distance + sp_size, sp_size)

    def peer(d):
        px = lax.rem(x + d // LINE, LINE)
        py = lax.rem(y + lax.rem(d, LINE), LINE)
        return py * LINE + px

    def mate(d):
        return lax.rem(x + d, LINE)

    def columns(c):
        return pl.ds(pl.multiple_of(c * WIDE, WIDE), WIDE)

    loads = []
    for g in (0, 2, 1):
        for i, (src, dst) in enumerate(((q_hbm, qv), (k_hbm, kv), (v_hbm, vv))):
            loads.append(pltpu.make_async_copy(src.at[g], dst.at[g], in_sem.at[g, i]))
    for copy in loads:
        copy.start()
    w_copies = [
        pltpu.make_async_copy(w_hbm.at[pl.ds(pl.multiple_of(half * COLS, COLS), COLS)], wv.at[n], w_sem.at[n])
        for n, half in enumerate((tp, 1 - tp))
    ]
    for copy in w_copies:
        copy.start()

    barrier = pltpu.get_barrier_semaphore()

    def greet(d, _):
        pl.semaphore_signal(barrier, inc=1, device_id=(plane + peer(d), tp), device_id_type=MESH)
        return 0

    lax.fori_loop(1, PLANE, greet, 0)
    pl.semaphore_signal(barrier, inc=1, device_id=(sp, 1 - tp), device_id_type=MESH)

    has_next = sp + PLANE < sp_size
    has_last = sp >= PLANE
    row_next = sp + LINE < sp_size
    row_last = sp >= LINE
    edge_next = row_next & (y == LINE - 1)
    edge_last = row_last & (y == 0)

    @pl.when(has_next)
    def _():
        pl.semaphore_signal(barrier, inc=1, device_id=(block(PLANE), tp), device_id_type=MESH)

    @pl.when(edge_next)
    def _():
        pl.semaphore_signal(barrier, inc=1, device_id=(block(LINE), tp), device_id_type=MESH)

    @pl.when(jnp.logical_not(has_last))
    def _():
        r2[pl.ds(0, 8), pl.ds(1, 2)] = jnp.zeros((8, 2, ROWS // PLANE, COLS), BF16)

    @pl.when(jnp.logical_not(row_last))
    def _():
        r1[pl.ds(0, 2), pl.ds(1, 2)] = jnp.zeros((2, 2, ROWS // LINE, COLS), BF16)
        ob[1] = jnp.zeros((BACK, COLS), BF16)
        lb[1] = jnp.zeros((BACK, HEAD), BF16)

    @pl.when(jnp.logical_not(row_next))
    def _():
        qn[1] = jnp.zeros((BACK, COLS), BF16)

    q_index = lax.broadcasted_iota(jnp.int32, (BACK, 2 * BACK), 0)
    k_index = lax.broadcasted_iota(jnp.int32, (BACK, 2 * BACK), 1)
    inside = (k_index >= q_index) & (k_index <= q_index + BACK)
    base = jnp.where(inside, 0.0, MASKED)
    band[0] = base
    for g, reach in ((1, LINE), (2, PLANE)):
        opening = jnp.where(sp >= reach, 0.0, MASKED)
        band[g] = jnp.where(k_index < BACK, base + opening, base)

    row = lax.broadcasted_iota(jnp.int32, (ROWS, ROWS), 0)
    col = lax.broadcasted_iota(jnp.int32, (ROWS, ROWS), 1)
    n2 = ROWS // PLANE
    n1 = ROWS // LINE

    perms[0] = one_hot(col == PLANE * (row % n2) + row // n2)
    perms[1] = one_hot(col == LINE * (row % n1) + row // n1)
    perms[2] = one_hot(row == LINE * (col % n1) + col // n1)
    token = lax.broadcasted_iota(jnp.int32, (ROWS, LINE * HEAD), 0)
    lane1 = lax.broadcasted_iota(jnp.int32, (ROWS, LINE * HEAD), 1)
    for which, half in enumerate((x % 2, y % 2)):
        wanted[which] = one_hot(lane1 == (token % LINE) * HEAD + half * n1 + token // LINE)

    position = (lax.broadcasted_iota(jnp.int32, (ROWS, HEAD), 0) + sp * ROWS).astype(F32)
    feature = lax.broadcasted_iota(jnp.int32, (ROWS, HEAD), 1)
    inverse = inverse_ref[...]
    angles = position * jnp.concatenate([inverse, inverse], axis=1)
    sine = jnp.sin(angles)
    cos_full[...] = jnp.cos(angles)
    sin_full[...] = jnp.where(feature < HEAD // 2, -sine, sine)

    def turned(piece):
        parts = []
        for h in range(piece.shape[1] // HEAD):
            m = piece[:, h * HEAD : (h + 1) * HEAD].astype(F32)
            parts.append(m * cos_full[...] + pltpu.roll(m, HEAD // 2, 1) * sin_full[...])
        return jnp.concatenate(parts, axis=1)

    def prepared(g, c):
        cs = columns(c)
        q = (turned(qv[g, :, cs]) * HEAD**-0.5).astype(BF16)
        k = turned(kv[g, :, cs]).astype(BF16)
        return q, k

    def remote(src, dst, i, device):
        return pltpu.make_async_remote_copy(
            src_ref=src,
            dst_ref=dst,
            send_sem=n0_send.at[i],
            recv_sem=n0_recv.at[i],
            device_id=(device, tp),
            device_id_type=MESH,
        )

    before, after = sp - x + mate(LINE - 1), sp - x + mate(1)

    def q0_copy():
        return remote(q0.at[pl.ds(0, BACK)], qn.at[0], 0, before)

    def q0_relay():
        return remote(qn.at[0], qn.at[1], 1, block(-LINE))

    near, far = pl.ds(0, COLS // 2), pl.ds(COLS // 2, COLS // 2)

    def on_near():
        return remote(on.at[:, near], ob.at[0, :, near], 2, after)

    def on_near_relay():
        return remote(ob.at[0, :, near], ob.at[1, :, near], 3, block(LINE))

    def on_far():
        return remote(on.at[:, far], ob.at[0, :, far], 6, after)

    def on_far_turn():
        return remote(on.at[:, far], ob.at[1, :, far], 7, block(LINE))

    def on_far_relay():
        return remote(ob.at[1, :, far], ob.at[1, :, far], 8, after)

    def ln_copy():
        return remote(ln, lb.at[0], 4, after)

    def ln_relay():
        return remote(lb.at[0], lb.at[1], 5, block(LINE))

    q_slot = jnp.where(x == LINE - 1, 1, 0)
    o_slot = jnp.where(x == 0, 1, 0)

    with jax.named_scope("load0"):
        for i in range(3):
            loads[i].wait()

    def g0_out(c, _):
        cs = columns(c)
        q, k = prepared(0, c)
        q0[:, cs] = q
        k0[:, cs] = k
        return 0

    scoped("g0_out", g0_out, 0)
    with jax.named_scope("barrier"):
        expected = PLANE + jnp.where(has_last, 1, 0) + jnp.where(edge_last, 1, 0)
        pl.semaphore_wait(barrier, expected)

    @pl.when(has_last)
    def _():
        pl.semaphore_signal(next_ready, inc=1, device_id=(block(-PLANE), tp), device_id_type=MESH)

    @pl.when(edge_last)
    def _():
        pl.semaphore_signal(row_ready, inc=1, device_id=(block(-LINE), tp), device_id_type=MESH)

    q0_copy().start()

    def g2_copy(c, d, part):
        what = pl.ds(part, part + 1)
        return pltpu.make_async_remote_copy(
            src_ref=s2.at[peer(d), what, :, columns(c)],
            dst_ref=r2.at[8 + j, what, :, columns(c)],
            send_sem=s2_send.at[part],
            recv_sem=s2_recv.at[part, c],
            device_id=(plane + peer(d), tp),
            device_id_type=MESH,
        )

    def g2_out(c, _):
        cs = columns(c)
        q, k = prepared(2, c)
        order = perms[0]
        for i, m in enumerate((q, k, vv[2, :, cs])):
            s2[:, i, :, cs] = dot(order, m).astype(BF16).reshape(PLANE, n2, WIDE)
        r2[8 + j, :, :, cs] = s2[j, :, :, cs]
        lax.fori_loop(1, PLANE, lambda d, _: (g2_copy(c, d, 1).start(), 0)[1], 0)
        return 0

    def g2_queries(c, _):
        lax.fori_loop(1, PLANE, lambda d, _: (g2_copy(c, d, 0).start(), 0)[1], 0)
        return 0


    def g1_copy(c, d, part):
        what = pl.ds(part, part + 1)
        return pltpu.make_async_remote_copy(
            src_ref=s1.at[mate(d), what, :, columns(c)],
            dst_ref=r1.at[2 + x, what, :, columns(c)],
            send_sem=s1_send.at[part],
            recv_sem=s1_recv.at[part, c],
            device_id=(sp - x + mate(d), tp),
            device_id_type=MESH,
        )

    def g1_out(c, _):
        cs = columns(c)
        q, k = prepared(1, c)
        order = perms[1]
        for i, m in enumerate((q, k, vv[1, :, cs])):
            s1[:, i, :, cs] = dot(order, m).astype(BF16).reshape(LINE, n1, WIDE)
        r1[2 + x, :, :, cs] = s1[x, :, :, cs]
        lax.fori_loop(1, LINE, lambda d, _: (g1_copy(c, d, 1).start(), 0)[1], 0)
        return 0

    def g1_queries(c, _):
        lax.fori_loop(1, LINE, lambda d, _: (g1_copy(c, d, 0).start(), 0)[1], 0)
        return 0

    def send_out(c, _):
        g2_out(c, 0)
        g1_out(c, 0)
        return 0

    for i in range(3, 9):
        loads[i].wait()
    scoped("send_out", send_out, 0)
    scoped("g2_queries", g2_queries, 0)


    def h2_copy(c):
        return pltpu.make_async_remote_copy(
            src_ref=r2.at[pl.ds(16, 8), pl.ds(1, 2), :, columns(c)],
            dst_ref=r2.at[pl.ds(0, 8), pl.ds(1, 2), :, columns(c)],
            send_sem=h2_send,
            recv_sem=h2_recv.at[c],
            device_id=(block(PLANE), tp),
            device_id_type=MESH,
        )

    def h1_copy(c):
        return pltpu.make_async_remote_copy(
            src_ref=r1.at[pl.ds(4, 2), pl.ds(1, 2), :, columns(c)],
            dst_ref=r1.at[pl.ds(0, 2), pl.ds(1, 2), :, columns(c)],
            send_sem=h1_send,
            recv_sem=h1_recv.at[c],
            device_id=(block(LINE), tp),
            device_id_type=MESH,
        )

    def attend(q, k, v, bias):
        scores = dot_nt(q, k) + bias
        row_max = jnp.max(scores, axis=1, keepdims=True)
        probs = jnp.exp(scores - row_max)
        row_sum = jnp.sum(probs, axis=1, keepdims=True)
        result = dot(probs.astype(BF16), v) / row_sum
        return result, row_max + jnp.log(row_sum)

    lane = lax.broadcasted_iota(jnp.int32, (BACK, HEAD), 1)

    def g2_halo(c, _):
        arrived(r2.at[pl.ds(8, PLANE - 1), pl.ds(1, 2), :, columns(c)], s2_recv.at[1, c])

        @pl.when(has_next & (c == 0))
        def _():
            pl.semaphore_wait(next_ready, 1)

        @pl.when(has_next)
        def _():
            h2_copy(c).start()

        return 0

    def g1_halo(c, _):
        arrived(r1.at[pl.ds(2, LINE - 1), pl.ds(1, 2), :, columns(c)], s1_recv.at[1, c])

        @pl.when(edge_next & (c == 0))
        def _():
            pl.semaphore_wait(row_ready, 1)

        @pl.when(row_next)
        def _():
            h1_copy(c).start()

        return 0

    def rung(d):
        return lax.rem(y + d, LINE)

    def o2_copy(c, d):
        return pltpu.make_async_remote_copy(
            src_ref=o2.at[pl.ds(LINE * rung(d), LINE), :, columns(c)],
            dst_ref=b2.at[pl.ds(LINE * y, LINE), :, columns(c)],
            send_sem=o2_send,
            recv_sem=o2_recv.at[c],
            device_id=(plane + rung(d) * LINE + x, tp),
            device_id_type=MESH,
        )

    def l2_copy(c, d):
        return pltpu.make_async_remote_copy(
            src_ref=l2.at[c, rung(d)],
            dst_ref=lb2.at[c, y],
            send_sem=l2_send,
            recv_sem=l2_recv.at[c],
            device_id=(plane + rung(d) * LINE + x, tp),
            device_id_type=MESH,
        )

    def o1_copy(c, d):
        return pltpu.make_async_remote_copy(
            src_ref=o1.at[mate(d), :, columns(c)],
            dst_ref=b1.at[x, :, columns(c)],
            send_sem=o1_send,
            recv_sem=o1_recv.at[c],
            device_id=(sp - x + mate(d), tp),
            device_id_type=MESH,
        )

    def l1_copy(c, d):
        return pltpu.make_async_remote_copy(
            src_ref=l1.at[c, mate(d)],
            dst_ref=lb1.at[c, x],
            send_sem=l1_send,
            recv_sem=l1_recv.at[c],
            device_id=(sp - x + mate(d), tp),
            device_id_type=MESH,
        )

    def split_terms(lse, heads):
        high = lse.astype(BF16).astype(F32)
        rest = lse - high
        middle = rest.astype(BF16).astype(F32)
        low = rest - middle
        return (high + pltpu.roll(middle, heads, 1) + pltpu.roll(low, 2 * heads, 1)).astype(BF16)

    def place(lses, b, head, lse):
        lses[b] = jnp.where(lane == head, lse, lses[b])

    def pack(target, c, lses):
        slot = lax.broadcasted_iota(jnp.int32, (n2, HEAD), 0)
        chosen = one_hot(slot == lax.broadcasted_iota(jnp.int32, (n2, HEAD), 1))
        for b in range(2):
            tile = dot_nt(chosen, split_terms(lses[b], CHUNK_HEADS)).astype(BF16)
            target[c, 2 * b] = tile
            target[c, 2 * b + 1] = tile

    def unpack(tiles, c, which):
        lanes = jnp.concatenate([tiles[c, r] for r in range(LINE)], axis=1)
        return dot(dot_nt(wanted[which], lanes).astype(BF16), spread(n2, CHUNK_HEADS, 0))

    def g2_attend(c, _):
        with jax.named_scope("wait_h2"):

            @pl.when(has_last)
            def _():
                h2_copy(c).wait_recv()

        with jax.named_scope("wait_q2"):
            arrived(r2.at[pl.ds(8, PLANE - 1), pl.ds(0, 1), :, columns(c)], s2_recv.at[0, c])
        lses = list(empty)
        for h in range(CHUNK_HEADS):
            cs = pl.ds(pl.multiple_of(c * WIDE + h * HEAD, HEAD), HEAD)
            for b in range(2):
                q = r2[pl.ds(8 + 8 * b, 8), 0, :, cs].reshape(BACK, HEAD)
                k = r2[pl.ds(8 * b, 16), 1, :, cs].reshape(2 * BACK, HEAD)
                v = r2[pl.ds(8 * b, 16), 2, :, cs].reshape(2 * BACK, HEAD)
                result, lse = attend(q, k, v, band[2 if b == 0 else 0])
                o2[pl.ds(8 * b, 8), :, cs] = result.astype(BF16).reshape(8, n2, HEAD)
                place(lses, b, h, lse)
        pack(l2, c, lses)
        mine = pl.ds(LINE * y, LINE)
        b2[mine, :, columns(c)] = o2[mine, :, columns(c)]
        lb2[c, y] = l2[c, y]
        lax.fori_loop(1, LINE, lambda d, _: (o2_copy(c, d).start(), l2_copy(c, d).start(), 0)[2], 0)
        return 0

    def g1_attend(c, _):
        with jax.named_scope("wait_h1"):

            @pl.when(row_last)
            def _():
                h1_copy(c).wait_recv()

        with jax.named_scope("wait_q1"):
            arrived(r1.at[pl.ds(2, LINE - 1), pl.ds(0, 1), :, columns(c)], s1_recv.at[0, c])
        for h in range(CHUNK_HEADS):
            cs = pl.ds(pl.multiple_of(c * WIDE + h * HEAD, HEAD), HEAD)
            for b in range(2):
                q = r1[pl.ds(2 + 2 * b, 2), 0, :, cs].reshape(BACK, HEAD)
                k = r1[pl.ds(2 * b, 4), 1, :, cs].reshape(2 * BACK, HEAD)
                v = r1[pl.ds(2 * b, 4), 2, :, cs].reshape(2 * BACK, HEAD)
                result, lse = attend(q, k, v, band[1 if b == 0 else 0])
                rows, lanes = pl.ds(BACK * b, BACK), pl.ds(HEAD * h, HEAD)
                g1[lax.rem(c, 2), rows, lanes] = result
                log1[lax.rem(c, 2), rows, lanes] = jnp.broadcast_to(lse, (BACK, HEAD))
        return 0

    def join(c, _):
        with jax.named_scope("wait_o2"):
            arrived(b2.at[pl.ds(0, PLANE - LINE), :, columns(c)], o2_recv.at[c])
            arrived(lb2.at[c, pl.ds(0, LINE - 1)], l2_recv.at[c])
        cs = columns(c)
        out2 = dot(perms[2], b2[:, :, cs].reshape(ROWS, WIDE))
        log2 = unpack(lb2, c, 1)
        here = lax.rem(c, 2)
        top = jnp.maximum(log1[here], log2)
        w1, w2 = jnp.exp(log1[here] - top), jnp.exp(log2 - top)
        weight = w1 + w2
        o1[:, :, cs] = ((w1 * g1[here] + w2 * out2) / weight).astype(BF16).reshape(LINE, n1, WIDE)
        log12 = top + jnp.log(weight)
        lses = list(empty)
        for b in range(2):
            for h in range(CHUNK_HEADS):
                place(lses, b, h, log12[BACK * b : BACK * (b + 1), HEAD * h : HEAD * (h + 1)])
        pack(l1, c, lses)
        b1[x, :, cs] = o1[x, :, cs]
        lb1[c, x] = l1[c, x]
        lax.fori_loop(1, LINE, lambda d, _: (o1_copy(c, d).start(), l1_copy(c, d).start(), 0)[2], 0)
        return 0

    def spread(terms, heads, first):
        term = lax.broadcasted_iota(jnp.int32, (terms, WIDE), 0)
        feature = lax.broadcasted_iota(jnp.int32, (terms, WIDE), 1)
        return one_hot((term < 3 * heads) & (term % heads == first + feature // HEAD))

    def g0_attend(c, _):
        for h in range(CHUNK_HEADS):
            cs = pl.ds(pl.multiple_of(c * WIDE + h * HEAD, HEAD), HEAD)
            for b in range(2):
                q = q0[pl.ds(BACK * b, BACK), cs]
                k = k0[pl.ds(0, BACK * (b + 1)), cs]
                v = vv[0, pl.ds(0, BACK * (b + 1)), cs]
                result, lse = attend(q, k, v, band[0] if b else band[0, :, BACK:])
                o0[pl.ds(BACK * b, BACK), cs] = result
                lse0[pl.ds(BACK * b, BACK), cs] = jnp.broadcast_to(lse, (BACK, HEAD))
        return 0

    def n0_attend(c, carry):
        lses = list(carry)
        for h in range(CHUNK_HEADS):
            cs = pl.ds(pl.multiple_of(c * WIDE + h * HEAD, HEAD), HEAD)
            k = k0[pl.ds(BACK, BACK), cs]
            v = vv[0, pl.ds(BACK, BACK), cs]
            result, lse = attend(qn[q_slot, :, cs], k, v, band[0, :, :BACK])
            on[:, cs] = result.astype(BF16)
            place(lses, 0, c * CHUNK_HEADS + h, lse)
        return tuple(lses)

    empty = (jnp.zeros((BACK, HEAD), F32), jnp.zeros((BACK, HEAD), F32))

    scoped("g0_attend", g0_attend, 0)
    with jax.named_scope("wait_q0"):
        q0_copy().wait_recv()

    @pl.when((x == LINE - 1) & row_last)
    def _():
        q0_relay().start()

    def step(c, _):
        with jax.named_scope("g2_halo"):
            g2_halo(c, 0)
        with jax.named_scope("g1_halo"):
            g1_halo(c, 0)

        @pl.when(c == 1)
        def _():
            with jax.named_scope("wait_q0r"):

                @pl.when((x == LINE - 1) & row_next)
                def _():
                    q0_relay().wait_recv()

            lses = scoped("n0_attend", n0_attend, empty[:1])
            ln[...] = split_terms(lses[0], HEADS)
            on_near().start()
            ln_copy().start()

            @pl.when(x < LINE - 1)
            def _():
                on_far().start()

            @pl.when((x == LINE - 1) & row_next)
            def _():
                on_far_turn().start()


        return 0

    lax.fori_loop(0, CHUNKS, step, 0)
    with jax.named_scope("wait_far"):

        @pl.when((x == LINE - 1) & row_last)
        def _():
            on_far_turn().wait_recv()
            on_far_relay().start()

    scoped("g1_queries", g1_queries, 0)

    def g2_step(c, _):
        @pl.when((c == 2) & (x == 0))
        def _():
            with jax.named_scope("wait_on"):
                on_near().wait_recv()
                ln_copy().wait_recv()

                @pl.when(row_next)
                def _():
                    on_near_relay().start()
                    ln_relay().start()


        with jax.named_scope("g2_attend"):
            g2_attend(c, 0)
        return 0

    lax.fori_loop(0, CHUNKS, g2_step, 0)

    def last(c, _):
        @pl.when(c < CHUNKS)
        def _():
            with jax.named_scope("g1_attend"):
                g1_attend(c, 0)

        @pl.when(c > 0)
        def _():
            with jax.named_scope("join"):
                join(c - 1, 0)

        return 0

    lax.fori_loop(0, CHUNKS + 1, last, 0)

    with jax.named_scope("drain"):
        for part in range(2):
            what = pl.ds(part, part + 1)
            arrived(s2.at[pl.ds(0, PLANE - 1), what], s2_send.at[part])
            arrived(s1.at[pl.ds(0, LINE - 1), what], s1_send.at[part])

        @pl.when(has_next)
        def _():
            arrived(r2.at[pl.ds(16, 8), pl.ds(1, 2)], h2_send)

        @pl.when(row_next)
        def _():
            arrived(r1.at[pl.ds(4, 2), pl.ds(1, 2)], h1_send)

    for copy in w_copies:
        copy.wait()
    for copy in (q0_copy(), on_near(), ln_copy()):
        copy.wait_send()

    @pl.when((x == LINE - 1) & row_last)
    def _():
        q0_relay().wait_send()
        on_far_relay().wait_send()

    @pl.when((x == LINE - 1) & row_next)
    def _():
        on_far_turn().wait_send()

    @pl.when(x < LINE - 1)
    def _():
        on_far().wait_send()


    with jax.named_scope("wait_l"):

        @pl.when((x == 0) & row_next)
        def _():
            on_near_relay().wait_send()
            ln_relay().wait_send()

        @pl.when((x == 0) & row_last)
        def _():
            on_near_relay().wait_recv()
            on_far_relay().wait_recv()
            ln_relay().wait_recv()

        @pl.when(x > 0)
        def _():
            on_near().wait_recv()
            on_far().wait_recv()
            ln_copy().wait_recv()

    def a_copy(c):
        return pltpu.make_async_remote_copy(
            src_ref=own.at[:, columns(c)],
            dst_ref=other.at[:, columns(c)],
            send_sem=a_send,
            recv_sem=a_recv.at[c],
            device_id=(sp, 1 - tp),
            device_id_type=MESH,
        )

    def project(c):
        cs = columns(c)
        return dot(own[:, cs], wv[0, cs, :]) + dot(other[:, cs], wv[1, cs, :])

    def premerge(c, _):
        cs = columns(c)
        rows = slice(0, BACK)
        log3 = dot(lb[o_slot], spread(HEAD, HEADS, c * CHUNK_HEADS)) + jnp.where(sp >= 1, 0.0, MASKED)
        top = jnp.maximum(lse0[rows, cs], log3)
        w0, w3 = jnp.exp(lse0[rows, cs] - top), jnp.exp(log3 - top)
        o0[rows, cs] = w0 * o0[rows, cs] + w3 * ob[o_slot, :, cs].astype(F32)
        sum0[:, cs] = w0 + w3
        lse0[rows, cs] = top
        return 0

    scoped("premerge", premerge, 0)

    def merge(c, _):
        with jax.named_scope("wait_o1"):
            arrived(b1.at[pl.ds(0, LINE - 1), :, columns(c)], o1_recv.at[c])
            arrived(lb1.at[c, pl.ds(0, LINE - 1)], l1_recv.at[c])
        cs = columns(c)
        out12 = dot(perms[2], b1[:, :, cs].reshape(ROWS, WIDE))
        log12 = unpack(lb1, c, 0)
        for half in range(2):
            rows = slice(half * BACK, (half + 1) * BACK)
            top = jnp.maximum(lse0[rows, cs], log12[rows])
            old, new = jnp.exp(lse0[rows, cs] - top), jnp.exp(log12[rows] - top)
            weight = sum0[:, cs] * old + new if half == 0 else old + new
            own[rows, cs] = ((o0[rows, cs] * old + out12[rows] * new) / weight).astype(BF16)
        a_copy(c).start()

        @pl.when(c == 1)
        def _():
            a_copy(0).wait_recv()
            total[...] = project(0)

        @pl.when(c > 1)
        def _():
            a_copy(c - 1).wait_recv()
            total[...] += project(c - 1)

        return 0

    scoped("merge", merge, 0)

    with jax.named_scope("wait_a"):
        a_copy(CHUNKS - 1).wait_recv()
    with jax.named_scope("project"):
        out_ref[...] = (total[...] + project(CHUNKS - 1)).astype(BF16)

    with jax.named_scope("finish"):
        arrived(o2.at[pl.ds(0, PLANE - LINE)], o2_send)
        arrived(l2.at[:, pl.ds(0, LINE - 1)], l2_send)
        arrived(o1.at[pl.ds(0, LINE - 1)], o1_send)
        arrived(l1.at[:, pl.ds(0, LINE - 1)], l1_send)
        arrived(own, a_send)


def shards(queries, keys, values, w_out):
    sp_size = lax.axis_size("sp")
    inverse = ROPE_BASE ** (-jnp.arange(0, HEAD, 2, dtype=F32) / HEAD)
    n2, n1 = ROWS // PLANE, ROWS // LINE
    dma = pltpu.SemaphoreType.DMA
    vmem = pl.BlockSpec(memory_space=pltpu.VMEM)
    hbm = pl.BlockSpec(memory_space=pl.ANY)
    return pl.pallas_call(
        functools.partial(kernel, sp_size),
        out_shape=pltpu.VMEM((ROWS, COLS), BF16),
        in_specs=[vmem, hbm, hbm, hbm, hbm],
        out_specs=vmem,
        scratch_shapes=[
            pltpu.VMEM((3, ROWS, COLS), BF16),
            pltpu.VMEM((3, ROWS, COLS), BF16),
            pltpu.VMEM((3, ROWS, COLS), BF16),
            pltpu.VMEM((2, COLS, COLS), BF16),
            pltpu.VMEM((PLANE, 3, n2, COLS), BF16),
            pltpu.VMEM((PLANE + 8, 3, n2, COLS), BF16),
            pltpu.VMEM((LINE, 3, n1, COLS), BF16),
            pltpu.VMEM((LINE + 2, 3, n1, COLS), BF16),
            pltpu.VMEM((ROWS, COLS), BF16),
            pltpu.VMEM((ROWS, COLS), BF16),
            pltpu.VMEM((2, BACK, COLS), BF16),
            pltpu.VMEM((BACK, COLS), BF16),
            pltpu.VMEM((2, BACK, COLS), BF16),
            pltpu.VMEM((BACK, HEAD), BF16),
            pltpu.VMEM((2, BACK, HEAD), BF16),
            pltpu.VMEM((PLANE, n2, COLS), BF16),
            pltpu.VMEM((PLANE, n2, COLS), BF16),
            pltpu.VMEM((LINE, n1, COLS), BF16),
            pltpu.VMEM((LINE, n1, COLS), BF16),
            pltpu.VMEM((CHUNKS, LINE, n2, HEAD), BF16),
            pltpu.VMEM((CHUNKS, LINE, n2, HEAD), BF16),
            pltpu.VMEM((CHUNKS, LINE, n2, HEAD), BF16),
            pltpu.VMEM((CHUNKS, LINE, n2, HEAD), BF16),
            pltpu.VMEM((2, ROWS, WIDE), F32),
            pltpu.VMEM((2, ROWS, WIDE), F32),
            pltpu.VMEM((ROWS, COLS), F32),
            pltpu.VMEM((ROWS, COLS), F32),
            pltpu.VMEM((BACK, COLS), F32),
            pltpu.VMEM((ROWS, COLS), BF16),
            pltpu.VMEM((ROWS, COLS), BF16),
            pltpu.VMEM((ROWS, COLS), F32),
            pltpu.VMEM((3, BACK, 2 * BACK), F32),
            pltpu.VMEM((3, ROWS, ROWS), BF16),
            pltpu.VMEM((2, ROWS, LINE * HEAD), BF16),
            pltpu.VMEM((ROWS, HEAD), F32),
            pltpu.VMEM((ROWS, HEAD), F32),
            dma((3, 3)), dma((2,)),
            dma((2,)), dma((2, CHUNKS)), dma((2,)), dma((2, CHUNKS)),
            dma, dma((CHUNKS,)), dma, dma((CHUNKS,)),
            dma((9,)), dma((9,)),
            dma, dma((CHUNKS,)), dma, dma((CHUNKS,)), dma, dma((CHUNKS,)), dma, dma((CHUNKS,)),
            dma, dma((CHUNKS,)), pltpu.SemaphoreType.REGULAR, pltpu.SemaphoreType.REGULAR,
        ],
        name="attention",
        compiler_params=pltpu.CompilerParams(collective_id=0, has_side_effects=True),
    )(inverse[None, :], queries, keys, values, w_out)


def solution(mesh):
    return jax.shard_map(
        shards,
        mesh=mesh,
        in_specs=(P(None, "sp", "tp"), P(None, "sp", "tp"), P(None, "sp", "tp"), P(None, "tp")),
        out_specs=P("sp", "tp"),
        check_vma=False,
    )
```

```python
import functools

import jax
import jax.numpy as jnp
import numpy as np
from jax import lax
from jax.experimental import pallas as pl
from jax.experimental.pallas import tpu as pltpu
from jax.sharding import PartitionSpec as P

HEAD = 128
ROPE_BASE = 10000.0
MASKED = -1e30
ROWS = 256
COLS = 1024
HEADS = COLS // HEAD
BACK = 128
PLANE = 16
LINE = 4
CHUNKS = 4
WIDE = COLS // CHUNKS
CHUNK_HEADS = WIDE // HEAD
MESH = pl.DeviceIdType.MESH
BF16 = jnp.bfloat16
F32 = jnp.float32


def arrived(ref, sem):
    pltpu.make_async_copy(ref, ref, sem).wait()


def one_hot(condition):
    return jnp.where(condition, 1.0, 0.0).astype(BF16)


def scoped(name, body, carry, first=0, last=CHUNKS):
    def named(c, carry):
        with jax.named_scope(name):
            return body(c, carry)

    return lax.fori_loop(first, last, named, carry)


def dot(a, b):
    return jnp.dot(a, b, preferred_element_type=F32)


def dot_nt(a, b):
    return lax.dot_general(a, b, (((1,), (1,)), ((), ())), preferred_element_type=F32)


def kernel(
    sp_size,
    inverse_ref, q_hbm, k_hbm, v_hbm, w_hbm, out_ref,
    qv, kv, vv, wv, s2, r2, s1, r1, k0, q0, qn, on, ob, ln, lb, o2, b2, o1, b1, l2, lb2, l1, lb1,
    g1, log1, o0, lse0, sum0, own, other, total, band, perms, wanted, cos_full, sin_full,
    in_sem, w_sem, s2_send, s2_recv, s1_send, s1_recv, h2_send, h2_recv, h1_send, h1_recv,
    n0_send, n0_recv, o2_send, o2_recv, o1_send, o1_recv, l2_send, l2_recv, l1_send, l1_recv,
    a_send, a_recv, next_ready, row_ready,
):
    sp = lax.axis_index("sp")
    tp = lax.axis_index("tp")
    x = lax.rem(sp, LINE)
    y = lax.rem(sp // LINE, LINE)
    j = lax.rem(sp, PLANE)
    plane = sp - j

    def block(distance):
        return lax.rem(sp + distance + sp_size, sp_size)

    def peer(d):
        px = lax.rem(x + d // LINE, LINE)
        py = lax.rem(y + lax.rem(d, LINE), LINE)
        return py * LINE + px

    def mate(d):
        return lax.rem(x + d, LINE)

    def columns(c):
        return pl.ds(pl.multiple_of(c * WIDE, WIDE), WIDE)

    def load(g, i):
        src, dst = ((q_hbm, qv), (k_hbm, kv), (v_hbm, vv))[i]
        return pltpu.make_async_copy(src.at[g], dst.at[g], in_sem.at[g, i])

    load(0, 0).start()
    for g, i in ((2, 0), (2, 1), (2, 2), (1, 0), (1, 1), (1, 2)):
        load(g, i).start()
    w_copies = [
        pltpu.make_async_copy(w_hbm.at[pl.ds(pl.multiple_of(half * COLS, COLS), COLS)], wv.at[n], w_sem.at[n])
        for n, half in enumerate((tp, 1 - tp))
    ]

    barrier = pltpu.get_barrier_semaphore()

    def greet(d, _):
        pl.semaphore_signal(barrier, inc=1, device_id=(plane + peer(d), tp), device_id_type=MESH)
        return 0

    lax.fori_loop(1, PLANE, greet, 0)
    pl.semaphore_signal(barrier, inc=1, device_id=(sp, 1 - tp), device_id_type=MESH)

    has_next = sp + PLANE < sp_size
    has_last = sp >= PLANE
    row_next = sp + LINE < sp_size
    row_last = sp >= LINE
    edge_next = row_next & (y == LINE - 1)
    edge_last = row_last & (y == 0)

    @pl.when(has_next)
    def _():
        pl.semaphore_signal(barrier, inc=1, device_id=(block(PLANE), tp), device_id_type=MESH)

    @pl.when(edge_next)
    def _():
        pl.semaphore_signal(barrier, inc=1, device_id=(block(LINE), tp), device_id_type=MESH)

    row = lax.broadcasted_iota(jnp.int32, (ROWS, ROWS), 0)
    col = lax.broadcasted_iota(jnp.int32, (ROWS, ROWS), 1)
    n2 = ROWS // PLANE
    n1 = ROWS // LINE

    perms[0] = one_hot(col == PLANE * (row % n2) + row // n2)
    perms[1] = one_hot(col == LINE * (row % n1) + row // n1)

    half_row = lax.broadcasted_iota(jnp.int32, (ROWS // 2, HEAD), 0)
    feature = lax.broadcasted_iota(jnp.int32, (ROWS // 2, HEAD), 1)
    left = feature < HEAD // 2
    position = (sp * ROWS + half_row + jnp.where(left, 0, ROWS // 2)).astype(F32)
    inverse = inverse_ref[...]
    angles = position * jnp.concatenate([inverse, inverse], axis=1)
    for table, values, sign in ((cos_full, jnp.cos(angles), 1.0), (sin_full, jnp.sin(angles), -1.0)):
        swapped = pltpu.roll(values, HEAD // 2, 1)
        table[: ROWS // 2] = jnp.where(left, values * sign, swapped)
        table[ROWS // 2 :] = jnp.where(left, swapped * sign, values)

    def turned(piece):
        parts = []
        for h in range(piece.shape[1] // HEAD):
            m = piece[:, h * HEAD : (h + 1) * HEAD].astype(F32)
            parts.append(m * cos_full[...] + pltpu.roll(m, HEAD // 2, 1) * sin_full[...])
        return jnp.concatenate(parts, axis=1)

    def prepared(g, c):
        cs = columns(c)
        q = (turned(qv[g, :, cs]) * HEAD**-0.5).astype(BF16)
        k = turned(kv[g, :, cs]).astype(BF16)
        return q, k

    def remote(src, dst, i, device):
        return pltpu.make_async_remote_copy(
            src_ref=src,
            dst_ref=dst,
            send_sem=n0_send.at[i],
            recv_sem=n0_recv.at[i],
            device_id=(device, tp),
            device_id_type=MESH,
        )

    before, after = sp - x + mate(LINE - 1), sp - x + mate(1)

    def q0_copy():
        return remote(q0.at[pl.ds(0, BACK)], qn.at[0], 0, before)

    def q0_relay():
        return remote(qn.at[0], qn.at[1], 1, block(-LINE))

    near, far = pl.ds(0, COLS // 2), pl.ds(COLS // 2, COLS // 2)

    def on_near():
        return remote(on.at[:, near], ob.at[0, :, near], 2, after)

    def on_near_relay():
        return remote(ob.at[0, :, near], ob.at[1, :, near], 3, block(LINE))

    def on_far():
        return remote(on.at[:, far], ob.at[0, :, far], 6, after)

    def on_far_turn():
        return remote(on.at[:, far], ob.at[1, :, far], 7, block(LINE))

    def on_far_relay():
        return remote(ob.at[1, :, far], ob.at[1, :, far], 8, after)

    def ln_copy():
        return remote(ln, lb.at[0], 4, after)

    def ln_relay():
        return remote(lb.at[0], lb.at[1], 5, block(LINE))

    q_slot = jnp.where(x == LINE - 1, 1, 0)
    o_slot = jnp.where(x == 0, 1, 0)

    with jax.named_scope("load0"):
        load(0, 0).wait()
    for i in (1, 2):
        load(0, i).start()

    def q0_out(c, _):
        cs = columns(c)
        q0[:, cs] = (turned(qv[0, :, cs]) * HEAD**-0.5).astype(BF16)
        return 0

    def k0_out(c, _):
        cs = columns(c)
        k0[:, cs] = turned(kv[0, :, cs]).astype(BF16)
        return 0

    scoped("q0_out", q0_out, 0)
    with jax.named_scope("barrier"):
        expected = PLANE + jnp.where(has_last, 1, 0) + jnp.where(edge_last, 1, 0)
        pl.semaphore_wait(barrier, expected)

    @pl.when(has_last)
    def _():
        pl.semaphore_signal(next_ready, inc=1, device_id=(block(-PLANE), tp), device_id_type=MESH)

    @pl.when(edge_last)
    def _():
        pl.semaphore_signal(row_ready, inc=1, device_id=(block(-LINE), tp), device_id_type=MESH)

    q0_copy().start()

    def g2_copy(c, d, part):
        what = pl.ds(part, part + 1)
        return pltpu.make_async_remote_copy(
            src_ref=s2.at[peer(d), what, :, columns(c)],
            dst_ref=r2.at[8 + j, what, :, columns(c)],
            send_sem=s2_send.at[part],
            recv_sem=s2_recv.at[part, c],
            device_id=(plane + peer(d), tp),
            device_id_type=MESH,
        )

    def g2_out(c, _):
        cs = columns(c)
        q, k = prepared(2, c)
        order = perms[0]
        for i, m in enumerate((q, k, vv[2, :, cs])):
            s2[:, i, :, cs] = dot(order, m).astype(BF16).reshape(PLANE, n2, WIDE)
        r2[8 + j, :, :, cs] = s2[j, :, :, cs]
        lax.fori_loop(1, PLANE, lambda d, _: (g2_copy(c, d, 1).start(), 0)[1], 0)
        return 0

    def g2_queries(c, _):
        lax.fori_loop(1, PLANE, lambda d, _: (g2_copy(c, d, 0).start(), 0)[1], 0)
        return 0


    def g1_copy(c, d, part):
        what = pl.ds(part, part + 1)
        return pltpu.make_async_remote_copy(
            src_ref=s1.at[mate(d), what, :, columns(c)],
            dst_ref=r1.at[2 + x, what, :, columns(c)],
            send_sem=s1_send.at[part],
            recv_sem=s1_recv.at[part, c],
            device_id=(sp - x + mate(d), tp),
            device_id_type=MESH,
        )

    def g1_out(c, _):
        cs = columns(c)
        q, k = prepared(1, c)
        order = perms[1]
        for i, m in enumerate((q, k, vv[1, :, cs])):
            s1[:, i, :, cs] = dot(order, m).astype(BF16).reshape(LINE, n1, WIDE)
        r1[2 + x, :, :, cs] = s1[x, :, :, cs]
        lax.fori_loop(1, LINE, lambda d, _: (g1_copy(c, d, 1).start(), 0)[1], 0)
        return 0

    def g1_queries(c, _):
        lax.fori_loop(1, LINE, lambda d, _: (g1_copy(c, d, 0).start(), 0)[1], 0)
        return 0

    def send_out(c, _):
        g2_out(c, 0)

        @pl.when(c == 0)
        def _():
            for i in range(3):
                load(1, i).wait()

        g1_out(c, 0)
        return 0

    with jax.named_scope("load2"):
        for i in range(3):
            load(2, i).wait()
    scoped("send_out", send_out, 0)
    scoped("g2_queries", g2_queries, 0)

    @pl.when(jnp.logical_not(has_last))
    def _():
        r2[pl.ds(0, 8), pl.ds(1, 2)] = jnp.zeros((8, 2, ROWS // PLANE, COLS), BF16)

    @pl.when(jnp.logical_not(row_last))
    def _():
        r1[pl.ds(0, 2), pl.ds(1, 2)] = jnp.zeros((2, 2, ROWS // LINE, COLS), BF16)
        ob[1] = jnp.zeros((BACK, COLS), BF16)
        lb[1] = jnp.zeros((BACK, HEAD), BF16)

    @pl.when(jnp.logical_not(row_next))
    def _():
        qn[1] = jnp.zeros((BACK, COLS), BF16)

    q_index = lax.broadcasted_iota(jnp.int32, (BACK, 2 * BACK), 0)
    k_index = lax.broadcasted_iota(jnp.int32, (BACK, 2 * BACK), 1)
    inside = (k_index >= q_index) & (k_index <= q_index + BACK)
    base = jnp.where(inside, 0.0, MASKED)
    band[0] = base
    for g, reach in ((1, LINE), (2, PLANE)):
        opening = jnp.where(sp >= reach, 0.0, MASKED)
        band[g] = jnp.where(k_index < BACK, base + opening, base)

    perms[2] = one_hot(row == LINE * (col % n1) + col // n1)
    token = lax.broadcasted_iota(jnp.int32, (ROWS, LINE * HEAD), 0)
    lane1 = lax.broadcasted_iota(jnp.int32, (ROWS, LINE * HEAD), 1)
    for which, half in enumerate((x % 2, y % 2)):
        wanted[which] = one_hot(lane1 == (token % LINE) * HEAD + half * n1 + token // LINE)


    def h2_copy(c):
        return pltpu.make_async_remote_copy(
            src_ref=r2.at[pl.ds(16, 8), pl.ds(1, 2), :, columns(c)],
            dst_ref=r2.at[pl.ds(0, 8), pl.ds(1, 2), :, columns(c)],
            send_sem=h2_send,
            recv_sem=h2_recv.at[c],
            device_id=(block(PLANE), tp),
            device_id_type=MESH,
        )

    def h1_copy(c):
        return pltpu.make_async_remote_copy(
            src_ref=r1.at[pl.ds(4, 2), pl.ds(1, 2), :, columns(c)],
            dst_ref=r1.at[pl.ds(0, 2), pl.ds(1, 2), :, columns(c)],
            send_sem=h1_send,
            recv_sem=h1_recv.at[c],
            device_id=(block(LINE), tp),
            device_id_type=MESH,
        )

    def attend(q, k, v, bias):
        scores = dot_nt(q, k) + bias
        row_max = jnp.max(scores, axis=1, keepdims=True)
        probs = jnp.exp(scores - row_max)
        row_sum = jnp.sum(probs, axis=1, keepdims=True)
        result = dot(probs.astype(BF16), v) / row_sum
        return result, row_max + jnp.log(row_sum)

    lane = lax.broadcasted_iota(jnp.int32, (BACK, HEAD), 1)

    def g2_halo(c, _):
        arrived(r2.at[pl.ds(8, PLANE - 1), pl.ds(1, 2), :, columns(c)], s2_recv.at[1, c])

        @pl.when(has_next & (c == 0))
        def _():
            pl.semaphore_wait(next_ready, 1)

        @pl.when(has_next)
        def _():
            h2_copy(c).start()

        return 0

    def g1_halo(c, _):
        arrived(r1.at[pl.ds(2, LINE - 1), pl.ds(1, 2), :, columns(c)], s1_recv.at[1, c])

        @pl.when(edge_next & (c == 0))
        def _():
            pl.semaphore_wait(row_ready, 1)

        @pl.when(row_next)
        def _():
            h1_copy(c).start()

        return 0

    def rung(d):
        return lax.rem(y + d, LINE)

    def o2_copy(c, d):
        return pltpu.make_async_remote_copy(
            src_ref=o2.at[pl.ds(LINE * rung(d), LINE), :, columns(c)],
            dst_ref=b2.at[pl.ds(LINE * y, LINE), :, columns(c)],
            send_sem=o2_send,
            recv_sem=o2_recv.at[c],
            device_id=(plane + rung(d) * LINE + x, tp),
            device_id_type=MESH,
        )

    def l2_copy(c, d):
        return pltpu.make_async_remote_copy(
            src_ref=l2.at[c, rung(d)],
            dst_ref=lb2.at[c, y],
            send_sem=l2_send,
            recv_sem=l2_recv.at[c],
            device_id=(plane + rung(d) * LINE + x, tp),
            device_id_type=MESH,
        )

    def o1_copy(c, d):
        return pltpu.make_async_remote_copy(
            src_ref=o1.at[mate(d), :, columns(c)],
            dst_ref=b1.at[x, :, columns(c)],
            send_sem=o1_send,
            recv_sem=o1_recv.at[c],
            device_id=(sp - x + mate(d), tp),
            device_id_type=MESH,
        )

    def l1_copy(c, d):
        return pltpu.make_async_remote_copy(
            src_ref=l1.at[c, mate(d)],
            dst_ref=lb1.at[c, x],
            send_sem=l1_send,
            recv_sem=l1_recv.at[c],
            device_id=(sp - x + mate(d), tp),
            device_id_type=MESH,
        )

    def split_terms(lse, heads):
        high = lse.astype(BF16).astype(F32)
        rest = lse - high
        middle = rest.astype(BF16).astype(F32)
        low = rest - middle
        return (high + pltpu.roll(middle, heads, 1) + pltpu.roll(low, 2 * heads, 1)).astype(BF16)

    def place(lses, b, head, lse):
        lses[b] = jnp.where(lane == head, lse, lses[b])

    def pack(target, c, lses):
        slot = lax.broadcasted_iota(jnp.int32, (n2, HEAD), 0)
        chosen = one_hot(slot == lax.broadcasted_iota(jnp.int32, (n2, HEAD), 1))
        for b in range(2):
            tile = dot_nt(chosen, split_terms(lses[b], CHUNK_HEADS)).astype(BF16)
            target[c, 2 * b] = tile
            target[c, 2 * b + 1] = tile

    def unpack(tiles, c, which):
        lanes = jnp.concatenate([tiles[c, r] for r in range(LINE)], axis=1)
        return dot(dot_nt(wanted[which], lanes).astype(BF16), spread(n2, CHUNK_HEADS, 0))

    def g2_attend(c, _):
        with jax.named_scope("wait_h2"):

            @pl.when(has_last)
            def _():
                h2_copy(c).wait_recv()

        with jax.named_scope("wait_q2"):
            arrived(r2.at[pl.ds(8, PLANE - 1), pl.ds(0, 1), :, columns(c)], s2_recv.at[0, c])
        lses = list(empty)
        for h in range(CHUNK_HEADS):
            cs = pl.ds(pl.multiple_of(c * WIDE + h * HEAD, HEAD), HEAD)
            for b in range(2):
                q = r2[pl.ds(8 + 8 * b, 8), 0, :, cs].reshape(BACK, HEAD)
                k = r2[pl.ds(8 * b, 16), 1, :, cs].reshape(2 * BACK, HEAD)
                v = r2[pl.ds(8 * b, 16), 2, :, cs].reshape(2 * BACK, HEAD)
                result, lse = attend(q, k, v, band[2 if b == 0 else 0])
                o2[pl.ds(8 * b, 8), :, cs] = result.astype(BF16).reshape(8, n2, HEAD)
                place(lses, b, h, lse)
        pack(l2, c, lses)
        mine = pl.ds(LINE * y, LINE)
        b2[mine, :, columns(c)] = o2[mine, :, columns(c)]
        lb2[c, y] = l2[c, y]
        lax.fori_loop(1, LINE, lambda d, _: (o2_copy(c, d).start(), l2_copy(c, d).start(), 0)[2], 0)
        return 0

    def g1_attend(c, _):
        with jax.named_scope("wait_h1"):

            @pl.when(row_last)
            def _():
                h1_copy(c).wait_recv()

        with jax.named_scope("wait_q1"):
            arrived(r1.at[pl.ds(2, LINE - 1), pl.ds(0, 1), :, columns(c)], s1_recv.at[0, c])
        for h in range(CHUNK_HEADS):
            cs = pl.ds(pl.multiple_of(c * WIDE + h * HEAD, HEAD), HEAD)
            for b in range(2):
                q = r1[pl.ds(2 + 2 * b, 2), 0, :, cs].reshape(BACK, HEAD)
                k = r1[pl.ds(2 * b, 4), 1, :, cs].reshape(2 * BACK, HEAD)
                v = r1[pl.ds(2 * b, 4), 2, :, cs].reshape(2 * BACK, HEAD)
                result, lse = attend(q, k, v, band[1 if b == 0 else 0])
                rows, lanes = pl.ds(BACK * b, BACK), pl.ds(HEAD * h, HEAD)
                g1[lax.rem(c, 2), rows, lanes] = result
                log1[lax.rem(c, 2), rows, lanes] = jnp.broadcast_to(lse, (BACK, HEAD))
        return 0

    def join(c, _):
        with jax.named_scope("wait_o2"):
            arrived(b2.at[pl.ds(0, PLANE - LINE), :, columns(c)], o2_recv.at[c])
            arrived(lb2.at[c, pl.ds(0, LINE - 1)], l2_recv.at[c])
        cs = columns(c)
        out2 = dot(perms[2], b2[:, :, cs].reshape(ROWS, WIDE))
        log2 = unpack(lb2, c, 1)
        here = lax.rem(c, 2)
        top = jnp.maximum(log1[here], log2)
        w1, w2 = jnp.exp(log1[here] - top), jnp.exp(log2 - top)
        weight = w1 + w2
        o1[:, :, cs] = ((w1 * g1[here] + w2 * out2) / weight).astype(BF16).reshape(LINE, n1, WIDE)
        log12 = top + jnp.log(weight)
        lses = list(empty)
        for b in range(2):
            for h in range(CHUNK_HEADS):
                place(lses, b, h, log12[BACK * b : BACK * (b + 1), HEAD * h : HEAD * (h + 1)])
        pack(l1, c, lses)
        b1[x, :, cs] = o1[x, :, cs]
        lb1[c, x] = l1[c, x]
        lax.fori_loop(1, LINE, lambda d, _: (o1_copy(c, d).start(), l1_copy(c, d).start(), 0)[2], 0)
        return 0

    def spread(terms, heads, first):
        term = lax.broadcasted_iota(jnp.int32, (terms, WIDE), 0)
        feature = lax.broadcasted_iota(jnp.int32, (terms, WIDE), 1)
        return one_hot((term < 3 * heads) & (term % heads == first + feature // HEAD))

    def g0_attend(c, _):
        for h in range(CHUNK_HEADS):
            cs = pl.ds(pl.multiple_of(c * WIDE + h * HEAD, HEAD), HEAD)
            for b in range(2):
                q = q0[pl.ds(BACK * b, BACK), cs]
                k = k0[pl.ds(0, BACK * (b + 1)), cs]
                v = vv[0, pl.ds(0, BACK * (b + 1)), cs]
                result, lse = attend(q, k, v, band[0] if b else band[0, :, BACK:])
                o0[pl.ds(BACK * b, BACK), cs] = result
                lse0[pl.ds(BACK * b, BACK), cs] = jnp.broadcast_to(lse, (BACK, HEAD))
        return 0

    def n0_attend(c, carry):
        lses = list(carry)
        for h in range(CHUNK_HEADS):
            cs = pl.ds(pl.multiple_of(c * WIDE + h * HEAD, HEAD), HEAD)
            k = k0[pl.ds(BACK, BACK), cs]
            v = vv[0, pl.ds(BACK, BACK), cs]
            result, lse = attend(qn[q_slot, :, cs], k, v, band[0, :, :BACK])
            on[:, cs] = result.astype(BF16)
            place(lses, 0, c * CHUNK_HEADS + h, lse)
        return tuple(lses)

    empty = (jnp.zeros((BACK, HEAD), F32), jnp.zeros((BACK, HEAD), F32))

    for copy in w_copies:
        copy.start()
    load(0, 1).wait()
    load(0, 2).wait()
    scoped("k0_out", k0_out, 0)
    scoped("g0_attend", g0_attend, 0)
    with jax.named_scope("wait_q0"):
        q0_copy().wait_recv()

    @pl.when((x == LINE - 1) & row_last)
    def _():
        q0_relay().start()

    def step(c, _):
        with jax.named_scope("g2_halo"):
            g2_halo(c, 0)
        with jax.named_scope("g1_halo"):
            g1_halo(c, 0)

        @pl.when(c == 1)
        def _():
            with jax.named_scope("wait_q0r"):

                @pl.when((x == LINE - 1) & row_next)
                def _():
                    q0_relay().wait_recv()

            lses = scoped("n0_attend", n0_attend, empty[:1])
            ln[...] = split_terms(lses[0], HEADS)
            on_near().start()
            ln_copy().start()

            @pl.when(x < LINE - 1)
            def _():
                on_far().start()

            @pl.when((x == LINE - 1) & row_next)
            def _():
                on_far_turn().start()


        return 0

    lax.fori_loop(0, CHUNKS, step, 0)
    scoped("g1_queries", g1_queries, 0)

    def g2_step(c, _):
        @pl.when((c == 1) & (x == LINE - 1) & row_last)
        def _():
            with jax.named_scope("wait_far"):
                on_far_turn().wait_recv()
                on_far_relay().start()

        @pl.when((c == 2) & (x == 0))
        def _():
            with jax.named_scope("wait_on"):
                on_near().wait_recv()
                ln_copy().wait_recv()

                @pl.when(row_next)
                def _():
                    on_near_relay().start()
                    ln_relay().start()


        with jax.named_scope("g2_attend"):
            g2_attend(c, 0)
        return 0

    lax.fori_loop(0, CHUNKS, g2_step, 0)

    def last(c, _):
        @pl.when(c < CHUNKS)
        def _():
            with jax.named_scope("g1_attend"):
                g1_attend(c, 0)

        @pl.when(c > 0)
        def _():
            with jax.named_scope("join"):
                join(c - 1, 0)

        return 0

    lax.fori_loop(0, CHUNKS + 1, last, 0)

    with jax.named_scope("drain"):
        for part in range(2):
            what = pl.ds(part, part + 1)
            arrived(s2.at[pl.ds(0, PLANE - 1), what], s2_send.at[part])
            arrived(s1.at[pl.ds(0, LINE - 1), what], s1_send.at[part])

        @pl.when(has_next)
        def _():
            arrived(r2.at[pl.ds(16, 8), pl.ds(1, 2)], h2_send)

        @pl.when(row_next)
        def _():
            arrived(r1.at[pl.ds(4, 2), pl.ds(1, 2)], h1_send)

    for copy in w_copies:
        copy.wait()
    for copy in (q0_copy(), on_near(), ln_copy()):
        copy.wait_send()

    @pl.when((x == LINE - 1) & row_last)
    def _():
        q0_relay().wait_send()
        on_far_relay().wait_send()

    @pl.when((x == LINE - 1) & row_next)
    def _():
        on_far_turn().wait_send()

    @pl.when(x < LINE - 1)
    def _():
        on_far().wait_send()


    with jax.named_scope("wait_l"):

        @pl.when((x == 0) & row_next)
        def _():
            on_near_relay().wait_send()
            ln_relay().wait_send()

        @pl.when((x == 0) & row_last)
        def _():
            on_near_relay().wait_recv()
            on_far_relay().wait_recv()
            ln_relay().wait_recv()

        @pl.when(x > 0)
        def _():
            on_near().wait_recv()
            on_far().wait_recv()
            ln_copy().wait_recv()

    def a_copy(c):
        return pltpu.make_async_remote_copy(
            src_ref=own.at[:, columns(c)],
            dst_ref=other.at[:, columns(c)],
            send_sem=a_send,
            recv_sem=a_recv,
            device_id=(sp, 1 - tp),
            device_id_type=MESH,
        )

    def premerge(c, _):
        cs = columns(c)
        rows = slice(0, BACK)
        log3 = dot(lb[o_slot], spread(HEAD, HEADS, c * CHUNK_HEADS)) + jnp.where(sp >= 1, 0.0, MASKED)
        top = jnp.maximum(lse0[rows, cs], log3)
        w0, w3 = jnp.exp(lse0[rows, cs] - top), jnp.exp(log3 - top)
        o0[rows, cs] = w0 * o0[rows, cs] + w3 * ob[o_slot, :, cs].astype(F32)
        sum0[:, cs] = w0 + w3
        lse0[rows, cs] = top
        return 0

    scoped("premerge", premerge, 0)

    def merge(c, _):
        with jax.named_scope("wait_o1"):
            arrived(b1.at[pl.ds(0, LINE - 1), :, columns(c)], o1_recv.at[c])
            arrived(lb1.at[c, pl.ds(0, LINE - 1)], l1_recv.at[c])
        cs = columns(c)
        out12 = dot(perms[2], b1[:, :, cs].reshape(ROWS, WIDE))
        log12 = unpack(lb1, c, 0)
        for half in range(2):
            rows = slice(half * BACK, (half + 1) * BACK)
            top = jnp.maximum(lse0[rows, cs], log12[rows])
            old, new = jnp.exp(lse0[rows, cs] - top), jnp.exp(log12[rows] - top)
            weight = sum0[:, cs] * old + new if half == 0 else old + new
            own[rows, cs] = ((o0[rows, cs] * old + out12[rows] * new) / weight).astype(BF16)
        a_copy(c).start()

        return 0

    scoped("merge", merge, 0)

    with jax.named_scope("project"):
        for c in range(CHUNKS):
            cs = columns(c)
            total[:, cs] = dot(own[...], wv[0, :, cs])
    with jax.named_scope("wait_a"):
        arrived(other, a_recv)
    with jax.named_scope("project"):
        for c in range(CHUNKS):
            cs = columns(c)
            out_ref[:, cs] = (total[:, cs] + dot(other[...], wv[1, :, cs])).astype(BF16)

    with jax.named_scope("finish"):
        arrived(o2.at[pl.ds(0, PLANE - LINE)], o2_send)
        arrived(l2.at[:, pl.ds(0, LINE - 1)], l2_send)
        arrived(o1.at[pl.ds(0, LINE - 1)], o1_send)
        arrived(l1.at[:, pl.ds(0, LINE - 1)], l1_send)
        arrived(own, a_send)


def shards(queries, keys, values, w_out):
    sp_size = lax.axis_size("sp")
    inverse = np.float32(ROPE_BASE ** (-np.arange(0, HEAD, 2) / HEAD))
    n2, n1 = ROWS // PLANE, ROWS // LINE
    dma = pltpu.SemaphoreType.DMA
    vmem = pl.BlockSpec(memory_space=pltpu.VMEM)
    hbm = pl.BlockSpec(memory_space=pl.ANY)
    return pl.pallas_call(
        functools.partial(kernel, sp_size),
        out_shape=pltpu.VMEM((ROWS, COLS), BF16),
        in_specs=[vmem, hbm, hbm, hbm, hbm],
        out_specs=vmem,
        scratch_shapes=[
            pltpu.VMEM((3, ROWS, COLS), BF16),
            pltpu.VMEM((3, ROWS, COLS), BF16),
            pltpu.VMEM((3, ROWS, COLS), BF16),
            pltpu.VMEM((2, COLS, COLS), BF16),
            pltpu.VMEM((PLANE, 3, n2, COLS), BF16),
            pltpu.VMEM((PLANE + 8, 3, n2, COLS), BF16),
            pltpu.VMEM((LINE, 3, n1, COLS), BF16),
            pltpu.VMEM((LINE + 2, 3, n1, COLS), BF16),
            pltpu.VMEM((ROWS, COLS), BF16),
            pltpu.VMEM((ROWS, COLS), BF16),
            pltpu.VMEM((2, BACK, COLS), BF16),
            pltpu.VMEM((BACK, COLS), BF16),
            pltpu.VMEM((2, BACK, COLS), BF16),
            pltpu.VMEM((BACK, HEAD), BF16),
            pltpu.VMEM((2, BACK, HEAD), BF16),
            pltpu.VMEM((PLANE, n2, COLS), BF16),
            pltpu.VMEM((PLANE, n2, COLS), BF16),
            pltpu.VMEM((LINE, n1, COLS), BF16),
            pltpu.VMEM((LINE, n1, COLS), BF16),
            pltpu.VMEM((CHUNKS, LINE, n2, HEAD), BF16),
            pltpu.VMEM((CHUNKS, LINE, n2, HEAD), BF16),
            pltpu.VMEM((CHUNKS, LINE, n2, HEAD), BF16),
            pltpu.VMEM((CHUNKS, LINE, n2, HEAD), BF16),
            pltpu.VMEM((2, ROWS, WIDE), F32),
            pltpu.VMEM((2, ROWS, WIDE), F32),
            pltpu.VMEM((ROWS, COLS), F32),
            pltpu.VMEM((ROWS, COLS), F32),
            pltpu.VMEM((BACK, COLS), F32),
            pltpu.VMEM((ROWS, COLS), BF16),
            pltpu.VMEM((ROWS, COLS), BF16),
            pltpu.VMEM((ROWS, COLS), F32),
            pltpu.VMEM((3, BACK, 2 * BACK), F32),
            pltpu.VMEM((3, ROWS, ROWS), BF16),
            pltpu.VMEM((2, ROWS, LINE * HEAD), BF16),
            pltpu.VMEM((ROWS, HEAD), F32),
            pltpu.VMEM((ROWS, HEAD), F32),
            dma((3, 3)), dma((2,)),
            dma((2,)), dma((2, CHUNKS)), dma((2,)), dma((2, CHUNKS)),
            dma, dma((CHUNKS,)), dma, dma((CHUNKS,)),
            dma((9,)), dma((9,)),
            dma, dma((CHUNKS,)), dma, dma((CHUNKS,)), dma, dma((CHUNKS,)), dma, dma((CHUNKS,)),
            dma, dma, pltpu.SemaphoreType.REGULAR, pltpu.SemaphoreType.REGULAR,
        ],
        name="attention",
        compiler_params=pltpu.CompilerParams(collective_id=0, has_side_effects=True),
    )(jnp.asarray(inverse[None, :]), queries, keys, values, w_out)


def solution(mesh):
    return jax.shard_map(
        shards,
        mesh=mesh,
        in_specs=(P(None, "sp", "tp"), P(None, "sp", "tp"), P(None, "sp", "tp"), P(None, "tp")),
        out_specs=P("sp", "tp"),
        check_vma=False,
    )
```

```python
import functools

import jax
import jax.numpy as jnp
import numpy as np
from jax import lax
from jax.experimental import pallas as pl
from jax.experimental.pallas import tpu as pltpu
from jax.sharding import PartitionSpec as P

HEAD = 128
ROPE_BASE = 10000.0
MASKED = -1e30
ROWS = 256
COLS = 1024
HEADS = COLS // HEAD
BACK = 128
PLANE = 16
LINE = 4
CHUNKS = 4
WIDE = COLS // CHUNKS
CHUNK_HEADS = WIDE // HEAD
MESH = pl.DeviceIdType.MESH
BF16 = jnp.bfloat16
F32 = jnp.float32


def arrived(ref, sem):
    pltpu.make_async_copy(ref, ref, sem).wait()


def one_hot(condition):
    return jnp.where(condition, 1.0, 0.0).astype(BF16)


def scoped(name, body, carry, first=0, last=CHUNKS):
    def named(c, carry):
        with jax.named_scope(name):
            return body(c, carry)

    return lax.fori_loop(first, last, named, carry)


def dot(a, b):
    return jnp.dot(a, b, preferred_element_type=F32)


def dot_nt(a, b):
    return lax.dot_general(a, b, (((1,), (1,)), ((), ())), preferred_element_type=F32)


def kernel(
    sp_size,
    inverse_ref, q_hbm, k_hbm, v_hbm, w_hbm, out_ref,
    qv, kv, vv, wv, s2, r2, s1, r1, k0, q0, qn, on, ob, ln, lb, o2, b2, o1, b1, l2, lb2, l1, lb1,
    g1, log1, o0, lse0, sum0, own, other, total, band, perms, wanted, cos_full, sin_full,
    in_sem, w_sem, s2_send, s2_recv, s1_send, s1_recv, h2_send, h2_recv, h1_send, h1_recv,
    n0_send, n0_recv, o2_send, o2_recv, o1_send, o1_recv, l2_send, l2_recv, l1_send, l1_recv,
    a_send, a_recv, next_ready, row_ready,
):
    sp = lax.axis_index("sp")
    tp = lax.axis_index("tp")
    x = lax.rem(sp, LINE)
    y = lax.rem(sp // LINE, LINE)
    j = lax.rem(sp, PLANE)
    plane = sp - j

    def block(distance):
        return lax.rem(sp + distance + sp_size, sp_size)

    def peer(d):
        px = lax.rem(x + d // LINE, LINE)
        py = lax.rem(y + lax.rem(d, LINE), LINE)
        return py * LINE + px

    def mate(d):
        return lax.rem(x + d, LINE)

    def columns(c):
        return pl.ds(pl.multiple_of(c * WIDE, WIDE), WIDE)

    def load(g, i):
        src, dst = ((q_hbm, qv), (k_hbm, kv), (v_hbm, vv))[i]
        return pltpu.make_async_copy(src.at[g], dst.at[g], in_sem.at[g, i])

    load(0, 0).start()
    for g, i in ((2, 0), (2, 1), (2, 2), (1, 0), (1, 1), (1, 2)):
        load(g, i).start()
    w_copies = [
        pltpu.make_async_copy(w_hbm.at[pl.ds(pl.multiple_of(half * COLS, COLS), COLS)], wv.at[n], w_sem.at[n])
        for n, half in enumerate((tp, 1 - tp))
    ]

    barrier = pltpu.get_barrier_semaphore()

    def greet(d, _):
        pl.semaphore_signal(barrier, inc=1, device_id=(plane + peer(d), tp), device_id_type=MESH)
        return 0

    lax.fori_loop(1, PLANE, greet, 0)
    pl.semaphore_signal(barrier, inc=1, device_id=(sp, 1 - tp), device_id_type=MESH)

    has_next = sp + PLANE < sp_size
    has_last = sp >= PLANE
    row_next = sp + LINE < sp_size
    row_last = sp >= LINE
    edge_next = row_next & (y == LINE - 1)
    edge_last = row_last & (y == 0)

    @pl.when(has_next)
    def _():
        pl.semaphore_signal(barrier, inc=1, device_id=(block(PLANE), tp), device_id_type=MESH)

    @pl.when(edge_next)
    def _():
        pl.semaphore_signal(barrier, inc=1, device_id=(block(LINE), tp), device_id_type=MESH)

    row = lax.broadcasted_iota(jnp.int32, (ROWS, ROWS), 0)
    col = lax.broadcasted_iota(jnp.int32, (ROWS, ROWS), 1)
    n2 = ROWS // PLANE
    n1 = ROWS // LINE

    perms[0] = one_hot(col == PLANE * (row % n2) + row // n2)
    perms[1] = one_hot(col == LINE * (row % n1) + row // n1)

    half_row = lax.broadcasted_iota(jnp.int32, (ROWS // 2, HEAD), 0)
    feature = lax.broadcasted_iota(jnp.int32, (ROWS // 2, HEAD), 1)
    left = feature < HEAD // 2
    position = (sp * ROWS + half_row + jnp.where(left, 0, ROWS // 2)).astype(F32)
    inverse = inverse_ref[...]
    angles = position * jnp.concatenate([inverse, inverse], axis=1)
    for table, values, sign in ((cos_full, jnp.cos(angles), 1.0), (sin_full, jnp.sin(angles), -1.0)):
        swapped = pltpu.roll(values, HEAD // 2, 1)
        table[: ROWS // 2] = jnp.where(left, values * sign, swapped)
        table[ROWS // 2 :] = jnp.where(left, swapped * sign, values)

    def turned(piece):
        parts = []
        for h in range(piece.shape[1] // HEAD):
            m = piece[:, h * HEAD : (h + 1) * HEAD].astype(F32)
            parts.append(m * cos_full[...] + pltpu.roll(m, HEAD // 2, 1) * sin_full[...])
        return jnp.concatenate(parts, axis=1)

    def prepared(g, c):
        cs = columns(c)
        q = (turned(qv[g, :, cs]) * HEAD**-0.5).astype(BF16)
        k = turned(kv[g, :, cs]).astype(BF16)
        return q, k

    def remote(src, dst, i, device):
        return pltpu.make_async_remote_copy(
            src_ref=src,
            dst_ref=dst,
            send_sem=n0_send.at[i],
            recv_sem=n0_recv.at[i],
            device_id=(device, tp),
            device_id_type=MESH,
        )

    before, after = sp - x + mate(LINE - 1), sp - x + mate(1)

    def q0_copy():
        return remote(q0.at[pl.ds(0, BACK)], qn.at[0], 0, before)

    def q0_relay():
        return remote(qn.at[0], qn.at[1], 1, block(-LINE))

    near, far = pl.ds(0, 3 * COLS // 4), pl.ds(3 * COLS // 4, COLS // 4)

    def on_near():
        return remote(on.at[:, near], ob.at[0, :, near], 2, after)

    def on_near_relay():
        return remote(ob.at[0, :, near], ob.at[1, :, near], 3, block(LINE))

    def on_far():
        return remote(on.at[:, far], ob.at[0, :, far], 6, after)

    def on_far_turn():
        return remote(on.at[:, far], ob.at[1, :, far], 7, block(LINE))

    def on_far_relay():
        return remote(ob.at[1, :, far], ob.at[1, :, far], 8, after)

    def ln_copy():
        return remote(ln, lb.at[0], 4, after)

    def ln_relay():
        return remote(lb.at[0], lb.at[1], 5, block(LINE))

    q_slot = jnp.where(x == LINE - 1, 1, 0)
    o_slot = jnp.where(x == 0, 1, 0)

    with jax.named_scope("load0"):
        load(0, 0).wait()
    for i in (1, 2):
        load(0, i).start()

    def q0_out(c, _):
        cs = columns(c)
        q0[:, cs] = (turned(qv[0, :, cs]) * HEAD**-0.5).astype(BF16)
        return 0

    def k0_out(c, _):
        cs = columns(c)
        k0[:, cs] = turned(kv[0, :, cs]).astype(BF16)
        return 0

    scoped("q0_out", q0_out, 0)
    with jax.named_scope("barrier"):
        expected = PLANE + jnp.where(has_last, 1, 0) + jnp.where(edge_last, 1, 0)
        pl.semaphore_wait(barrier, expected)

    @pl.when(has_last)
    def _():
        pl.semaphore_signal(next_ready, inc=1, device_id=(block(-PLANE), tp), device_id_type=MESH)

    @pl.when(edge_last)
    def _():
        pl.semaphore_signal(row_ready, inc=1, device_id=(block(-LINE), tp), device_id_type=MESH)

    q0_copy().start()

    def g2_copy(c, d, part):
        what = pl.ds(part, part + 1)
        return pltpu.make_async_remote_copy(
            src_ref=s2.at[peer(d), what, :, columns(c)],
            dst_ref=r2.at[8 + j, what, :, columns(c)],
            send_sem=s2_send.at[part],
            recv_sem=s2_recv.at[part, c],
            device_id=(plane + peer(d), tp),
            device_id_type=MESH,
        )

    def g2_out(c, _):
        cs = columns(c)
        q, k = prepared(2, c)
        order = perms[0]
        for i, m in enumerate((q, k, vv[2, :, cs])):
            s2[:, i, :, cs] = dot(order, m).astype(BF16).reshape(PLANE, n2, WIDE)
        r2[8 + j, :, :, cs] = s2[j, :, :, cs]
        lax.fori_loop(1, PLANE, lambda d, _: (g2_copy(c, d, 1).start(), 0)[1], 0)
        return 0

    def g2_queries(c, _):
        lax.fori_loop(1, PLANE, lambda d, _: (g2_copy(c, d, 0).start(), 0)[1], 0)
        return 0


    def g1_copy(c, d, part):
        what = pl.ds(part, part + 1)
        return pltpu.make_async_remote_copy(
            src_ref=s1.at[mate(d), what, :, columns(c)],
            dst_ref=r1.at[2 + x, what, :, columns(c)],
            send_sem=s1_send.at[part],
            recv_sem=s1_recv.at[part, c],
            device_id=(sp - x + mate(d), tp),
            device_id_type=MESH,
        )

    def g1_out(c, _):
        cs = columns(c)
        q, k = prepared(1, c)
        order = perms[1]
        for i, m in enumerate((q, k, vv[1, :, cs])):
            s1[:, i, :, cs] = dot(order, m).astype(BF16).reshape(LINE, n1, WIDE)
        r1[2 + x, :, :, cs] = s1[x, :, :, cs]
        lax.fori_loop(1, LINE, lambda d, _: (g1_copy(c, d, 1).start(), 0)[1], 0)
        return 0

    def g1_queries(c, _):
        lax.fori_loop(1, LINE, lambda d, _: (g1_copy(c, d, 0).start(), 0)[1], 0)
        return 0

    def send_out(c, _):
        g2_out(c, 0)

        @pl.when(c == 0)
        def _():
            for i in range(3):
                load(1, i).wait()

        g1_out(c, 0)
        return 0

    with jax.named_scope("load2"):
        for i in range(3):
            load(2, i).wait()
    scoped("send_out", send_out, 0)
    scoped("g2_queries", g2_queries, 0)

    @pl.when(jnp.logical_not(has_last))
    def _():
        r2[pl.ds(0, 8), pl.ds(1, 2)] = jnp.zeros((8, 2, ROWS // PLANE, COLS), BF16)

    @pl.when(jnp.logical_not(row_last))
    def _():
        r1[pl.ds(0, 2), pl.ds(1, 2)] = jnp.zeros((2, 2, ROWS // LINE, COLS), BF16)
        ob[1] = jnp.zeros((BACK, COLS), BF16)
        lb[1] = jnp.zeros((BACK, HEAD), BF16)

    @pl.when(jnp.logical_not(row_next))
    def _():
        qn[1] = jnp.zeros((BACK, COLS), BF16)

    q_index = lax.broadcasted_iota(jnp.int32, (BACK, 2 * BACK), 0)
    k_index = lax.broadcasted_iota(jnp.int32, (BACK, 2 * BACK), 1)
    inside = (k_index >= q_index) & (k_index <= q_index + BACK)
    base = jnp.where(inside, 0.0, MASKED)
    band[0] = base
    for g, reach in ((1, LINE), (2, PLANE)):
        opening = jnp.where(sp >= reach, 0.0, MASKED)
        band[g] = jnp.where(k_index < BACK, base + opening, base)

    perms[2] = one_hot(row == LINE * (col % n1) + col // n1)
    token = lax.broadcasted_iota(jnp.int32, (ROWS, LINE * HEAD), 0)
    lane1 = lax.broadcasted_iota(jnp.int32, (ROWS, LINE * HEAD), 1)
    for which, half in enumerate((x % 2, y % 2)):
        wanted[which] = one_hot(lane1 == (token % LINE) * HEAD + half * n1 + token // LINE)


    def h2_copy(c):
        return pltpu.make_async_remote_copy(
            src_ref=r2.at[pl.ds(16, 8), pl.ds(1, 2), :, columns(c)],
            dst_ref=r2.at[pl.ds(0, 8), pl.ds(1, 2), :, columns(c)],
            send_sem=h2_send,
            recv_sem=h2_recv.at[c],
            device_id=(block(PLANE), tp),
            device_id_type=MESH,
        )

    def h1_copy(c):
        return pltpu.make_async_remote_copy(
            src_ref=r1.at[pl.ds(4, 2), pl.ds(1, 2), :, columns(c)],
            dst_ref=r1.at[pl.ds(0, 2), pl.ds(1, 2), :, columns(c)],
            send_sem=h1_send,
            recv_sem=h1_recv.at[c],
            device_id=(block(LINE), tp),
            device_id_type=MESH,
        )

    def attend(q, k, v, bias):
        scores = dot_nt(q, k) + bias
        row_max = jnp.max(scores, axis=1, keepdims=True)
        probs = jnp.exp(scores - row_max)
        row_sum = jnp.sum(probs, axis=1, keepdims=True)
        result = dot(probs.astype(BF16), v) / row_sum
        return result, row_max + jnp.log(row_sum)

    lane = lax.broadcasted_iota(jnp.int32, (BACK, HEAD), 1)

    def g2_halo(c, _):
        arrived(r2.at[pl.ds(8, PLANE - 1), pl.ds(1, 2), :, columns(c)], s2_recv.at[1, c])

        @pl.when(has_next & (c == 0))
        def _():
            pl.semaphore_wait(next_ready, 1)

        @pl.when(has_next)
        def _():
            h2_copy(c).start()

        return 0

    def g1_halo(c, _):
        arrived(r1.at[pl.ds(2, LINE - 1), pl.ds(1, 2), :, columns(c)], s1_recv.at[1, c])

        @pl.when(edge_next & (c == 0))
        def _():
            pl.semaphore_wait(row_ready, 1)

        @pl.when(row_next)
        def _():
            h1_copy(c).start()

        return 0

    def rung(d):
        return lax.rem(y + d, LINE)

    def o2_copy(c, d):
        return pltpu.make_async_remote_copy(
            src_ref=o2.at[pl.ds(LINE * rung(d), LINE), :, columns(c)],
            dst_ref=b2.at[pl.ds(LINE * y, LINE), :, columns(c)],
            send_sem=o2_send,
            recv_sem=o2_recv.at[c],
            device_id=(plane + rung(d) * LINE + x, tp),
            device_id_type=MESH,
        )

    def l2_copy(c, d):
        return pltpu.make_async_remote_copy(
            src_ref=l2.at[c, rung(d)],
            dst_ref=lb2.at[c, y],
            send_sem=l2_send,
            recv_sem=l2_recv.at[c],
            device_id=(plane + rung(d) * LINE + x, tp),
            device_id_type=MESH,
        )

    def o1_copy(c, d):
        return pltpu.make_async_remote_copy(
            src_ref=o1.at[mate(d), :, columns(c)],
            dst_ref=b1.at[x, :, columns(c)],
            send_sem=o1_send,
            recv_sem=o1_recv.at[c],
            device_id=(sp - x + mate(d), tp),
            device_id_type=MESH,
        )

    def l1_copy(c, d):
        return pltpu.make_async_remote_copy(
            src_ref=l1.at[c, mate(d)],
            dst_ref=lb1.at[c, x],
            send_sem=l1_send,
            recv_sem=l1_recv.at[c],
            device_id=(sp - x + mate(d), tp),
            device_id_type=MESH,
        )

    def split_terms(lse, heads):
        high = lse.astype(BF16).astype(F32)
        rest = lse - high
        middle = rest.astype(BF16).astype(F32)
        low = rest - middle
        return (high + pltpu.roll(middle, heads, 1) + pltpu.roll(low, 2 * heads, 1)).astype(BF16)

    def place(lses, b, head, lse):
        lses[b] = jnp.where(lane == head, lse, lses[b])

    def pack(target, c, lses):
        slot = lax.broadcasted_iota(jnp.int32, (n2, HEAD), 0)
        chosen = one_hot(slot == lax.broadcasted_iota(jnp.int32, (n2, HEAD), 1))
        for b in range(2):
            tile = dot_nt(chosen, split_terms(lses[b], CHUNK_HEADS)).astype(BF16)
            target[c, 2 * b] = tile
            target[c, 2 * b + 1] = tile

    def unpack(tiles, c, which):
        lanes = jnp.concatenate([tiles[c, r] for r in range(LINE)], axis=1)
        return dot(dot_nt(wanted[which], lanes).astype(BF16), spread(n2, CHUNK_HEADS, 0))

    def g2_attend(c, _):
        with jax.named_scope("wait_h2"):

            @pl.when(has_last)
            def _():
                h2_copy(c).wait_recv()

        with jax.named_scope("wait_q2"):
            arrived(r2.at[pl.ds(8, PLANE - 1), pl.ds(0, 1), :, columns(c)], s2_recv.at[0, c])
        lses = list(empty)
        for h in range(CHUNK_HEADS):
            cs = pl.ds(pl.multiple_of(c * WIDE + h * HEAD, HEAD), HEAD)
            for b in range(2):
                q = r2[pl.ds(8 + 8 * b, 8), 0, :, cs].reshape(BACK, HEAD)
                k = r2[pl.ds(8 * b, 16), 1, :, cs].reshape(2 * BACK, HEAD)
                v = r2[pl.ds(8 * b, 16), 2, :, cs].reshape(2 * BACK, HEAD)
                result, lse = attend(q, k, v, band[2 if b == 0 else 0])
                o2[pl.ds(8 * b, 8), :, cs] = result.astype(BF16).reshape(8, n2, HEAD)
                place(lses, b, h, lse)
        pack(l2, c, lses)
        mine = pl.ds(LINE * y, LINE)
        b2[mine, :, columns(c)] = o2[mine, :, columns(c)]
        lb2[c, y] = l2[c, y]
        lax.fori_loop(1, LINE, lambda d, _: (o2_copy(c, d).start(), l2_copy(c, d).start(), 0)[2], 0)
        return 0

    def g1_attend(c, _):
        with jax.named_scope("wait_h1"):

            @pl.when(row_last)
            def _():
                h1_copy(c).wait_recv()

        with jax.named_scope("wait_q1"):
            arrived(r1.at[pl.ds(2, LINE - 1), pl.ds(0, 1), :, columns(c)], s1_recv.at[0, c])
        for h in range(CHUNK_HEADS):
            cs = pl.ds(pl.multiple_of(c * WIDE + h * HEAD, HEAD), HEAD)
            for b in range(2):
                q = r1[pl.ds(2 + 2 * b, 2), 0, :, cs].reshape(BACK, HEAD)
                k = r1[pl.ds(2 * b, 4), 1, :, cs].reshape(2 * BACK, HEAD)
                v = r1[pl.ds(2 * b, 4), 2, :, cs].reshape(2 * BACK, HEAD)
                result, lse = attend(q, k, v, band[1 if b == 0 else 0])
                rows, lanes = pl.ds(BACK * b, BACK), pl.ds(HEAD * h, HEAD)
                g1[lax.rem(c, 2), rows, lanes] = result
                log1[lax.rem(c, 2), rows, lanes] = jnp.broadcast_to(lse, (BACK, HEAD))
        return 0

    def join(c, _):
        with jax.named_scope("wait_o2"):
            arrived(b2.at[pl.ds(0, PLANE - LINE), :, columns(c)], o2_recv.at[c])
            arrived(lb2.at[c, pl.ds(0, LINE - 1)], l2_recv.at[c])
        cs = columns(c)
        out2 = dot(perms[2], b2[:, :, cs].reshape(ROWS, WIDE))
        log2 = unpack(lb2, c, 1)
        here = lax.rem(c, 2)
        top = jnp.maximum(log1[here], log2)
        w1, w2 = jnp.exp(log1[here] - top), jnp.exp(log2 - top)
        weight = w1 + w2
        o1[:, :, cs] = ((w1 * g1[here] + w2 * out2) / weight).astype(BF16).reshape(LINE, n1, WIDE)
        log12 = top + jnp.log(weight)
        lses = list(empty)
        for b in range(2):
            for h in range(CHUNK_HEADS):
                place(lses, b, h, log12[BACK * b : BACK * (b + 1), HEAD * h : HEAD * (h + 1)])
        pack(l1, c, lses)
        b1[x, :, cs] = o1[x, :, cs]
        lb1[c, x] = l1[c, x]
        lax.fori_loop(1, LINE, lambda d, _: (o1_copy(c, d).start(), l1_copy(c, d).start(), 0)[2], 0)
        return 0

    def spread(terms, heads, first):
        term = lax.broadcasted_iota(jnp.int32, (terms, WIDE), 0)
        feature = lax.broadcasted_iota(jnp.int32, (terms, WIDE), 1)
        return one_hot((term < 3 * heads) & (term % heads == first + feature // HEAD))

    def g0_attend(c, _):
        for h in range(CHUNK_HEADS):
            cs = pl.ds(pl.multiple_of(c * WIDE + h * HEAD, HEAD), HEAD)
            for b in range(2):
                q = q0[pl.ds(BACK * b, BACK), cs]
                k = k0[pl.ds(0, BACK * (b + 1)), cs]
                v = vv[0, pl.ds(0, BACK * (b + 1)), cs]
                result, lse = attend(q, k, v, band[0] if b else band[0, :, BACK:])
                o0[pl.ds(BACK * b, BACK), cs] = result
                lse0[pl.ds(BACK * b, BACK), cs] = jnp.broadcast_to(lse, (BACK, HEAD))
        return 0

    def n0_attend(c, carry):
        lses = list(carry)
        for h in range(CHUNK_HEADS):
            cs = pl.ds(pl.multiple_of(c * WIDE + h * HEAD, HEAD), HEAD)
            k = k0[pl.ds(BACK, BACK), cs]
            v = vv[0, pl.ds(BACK, BACK), cs]
            result, lse = attend(qn[q_slot, :, cs], k, v, band[0, :, :BACK])
            on[:, cs] = result.astype(BF16)
            place(lses, 0, c * CHUNK_HEADS + h, lse)
        return tuple(lses)

    empty = (jnp.zeros((BACK, HEAD), F32), jnp.zeros((BACK, HEAD), F32))

    for copy in w_copies:
        copy.start()
    load(0, 1).wait()
    load(0, 2).wait()
    scoped("k0_out", k0_out, 0)
    scoped("g0_attend", g0_attend, 0)
    with jax.named_scope("wait_q0"):
        q0_copy().wait_recv()

    @pl.when((x == LINE - 1) & row_last)
    def _():
        q0_relay().start()

    def step(c, _):
        with jax.named_scope("g2_halo"):
            g2_halo(c, 0)
        with jax.named_scope("g1_halo"):
            g1_halo(c, 0)

        @pl.when(c == 1)
        def _():
            with jax.named_scope("wait_q0r"):

                @pl.when((x == LINE - 1) & row_next)
                def _():
                    q0_relay().wait_recv()

            lses = scoped("n0_attend", n0_attend, empty[:1])
            ln[...] = split_terms(lses[0], HEADS)
            on_near().start()
            ln_copy().start()

            @pl.when(x < LINE - 1)
            def _():
                on_far().start()

            @pl.when((x == LINE - 1) & row_next)
            def _():
                on_far_turn().start()


        return 0

    lax.fori_loop(0, CHUNKS, step, 0)
    scoped("g1_queries", g1_queries, 0)

    def g2_step(c, _):
        @pl.when((c == 1) & (x == LINE - 1) & row_last)
        def _():
            with jax.named_scope("wait_far"):
                on_far_turn().wait_recv()
                on_far_relay().start()

        @pl.when((c == 2) & (x == 0))
        def _():
            with jax.named_scope("wait_on"):
                on_near().wait_recv()
                ln_copy().wait_recv()

                @pl.when(row_next)
                def _():
                    on_near_relay().start()
                    ln_relay().start()


        with jax.named_scope("g2_attend"):
            g2_attend(c, 0)
        return 0

    lax.fori_loop(0, CHUNKS, g2_step, 0)

    def last(c, _):
        @pl.when(c < CHUNKS)
        def _():
            with jax.named_scope("g1_attend"):
                g1_attend(c, 0)

        @pl.when(c > 0)
        def _():
            with jax.named_scope("join"):
                join(c - 1, 0)

        return 0

    lax.fori_loop(0, CHUNKS + 1, last, 0)

    with jax.named_scope("drain"):
        for part in range(2):
            what = pl.ds(part, part + 1)
            arrived(s2.at[pl.ds(0, PLANE - 1), what], s2_send.at[part])
            arrived(s1.at[pl.ds(0, LINE - 1), what], s1_send.at[part])

        @pl.when(has_next)
        def _():
            arrived(r2.at[pl.ds(16, 8), pl.ds(1, 2)], h2_send)

        @pl.when(row_next)
        def _():
            arrived(r1.at[pl.ds(4, 2), pl.ds(1, 2)], h1_send)

    for copy in w_copies:
        copy.wait()
    for copy in (q0_copy(), on_near(), ln_copy()):
        copy.wait_send()

    @pl.when((x == LINE - 1) & row_last)
    def _():
        q0_relay().wait_send()
        on_far_relay().wait_send()

    @pl.when((x == LINE - 1) & row_next)
    def _():
        on_far_turn().wait_send()

    @pl.when(x < LINE - 1)
    def _():
        on_far().wait_send()


    with jax.named_scope("wait_l"):

        @pl.when((x == 0) & row_next)
        def _():
            on_near_relay().wait_send()
            ln_relay().wait_send()

        @pl.when((x == 0) & row_last)
        def _():
            on_near_relay().wait_recv()
            on_far_relay().wait_recv()
            ln_relay().wait_recv()

        @pl.when(x > 0)
        def _():
            on_near().wait_recv()
            on_far().wait_recv()
            ln_copy().wait_recv()

    def a_copy(c):
        return pltpu.make_async_remote_copy(
            src_ref=own.at[:, columns(c)],
            dst_ref=other.at[:, columns(c)],
            send_sem=a_send,
            recv_sem=a_recv,
            device_id=(sp, 1 - tp),
            device_id_type=MESH,
        )

    def premerge(c, _):
        cs = columns(c)
        rows = slice(0, BACK)
        log3 = dot(lb[o_slot], spread(HEAD, HEADS, c * CHUNK_HEADS)) + jnp.where(sp >= 1, 0.0, MASKED)
        top = jnp.maximum(lse0[rows, cs], log3)
        w0, w3 = jnp.exp(lse0[rows, cs] - top), jnp.exp(log3 - top)
        o0[rows, cs] = w0 * o0[rows, cs] + w3 * ob[o_slot, :, cs].astype(F32)
        sum0[:, cs] = w0 + w3
        lse0[rows, cs] = top
        return 0

    scoped("premerge", premerge, 0)

    def merge(c, _):
        with jax.named_scope("wait_o1"):
            arrived(b1.at[pl.ds(0, LINE - 1), :, columns(c)], o1_recv.at[c])
            arrived(lb1.at[c, pl.ds(0, LINE - 1)], l1_recv.at[c])
        cs = columns(c)
        out12 = dot(perms[2], b1[:, :, cs].reshape(ROWS, WIDE))
        log12 = unpack(lb1, c, 0)
        for half in range(2):
            rows = slice(half * BACK, (half + 1) * BACK)
            top = jnp.maximum(lse0[rows, cs], log12[rows])
            old, new = jnp.exp(lse0[rows, cs] - top), jnp.exp(log12[rows] - top)
            weight = sum0[:, cs] * old + new if half == 0 else old + new
            own[rows, cs] = ((o0[rows, cs] * old + out12[rows] * new) / weight).astype(BF16)
        a_copy(c).start()

        return 0

    def merges(k, _):
        merge(2 * k, 0)
        merge(2 * k + 1, 0)
        return 0

    scoped("merge", merges, 0, 0, CHUNKS // 2)

    with jax.named_scope("project"):
        for c in range(CHUNKS):
            cs = columns(c)
            total[:, cs] = dot(own[...], wv[0, :, cs])
    with jax.named_scope("wait_a"):
        arrived(other, a_recv)
    with jax.named_scope("project"):
        for c in range(CHUNKS):
            cs = columns(c)
            out_ref[:, cs] = (total[:, cs] + dot(other[...], wv[1, :, cs])).astype(BF16)

    with jax.named_scope("finish"):
        arrived(o2.at[pl.ds(0, PLANE - LINE)], o2_send)
        arrived(l2.at[:, pl.ds(0, LINE - 1)], l2_send)
        arrived(o1.at[pl.ds(0, LINE - 1)], o1_send)
        arrived(l1.at[:, pl.ds(0, LINE - 1)], l1_send)
        arrived(own, a_send)


def shards(queries, keys, values, w_out):
    sp_size = lax.axis_size("sp")
    inverse = np.float32(ROPE_BASE ** (-np.arange(0, HEAD, 2) / HEAD))
    n2, n1 = ROWS // PLANE, ROWS // LINE
    dma = pltpu.SemaphoreType.DMA
    vmem = pl.BlockSpec(memory_space=pltpu.VMEM)
    hbm = pl.BlockSpec(memory_space=pl.ANY)
    return pl.pallas_call(
        functools.partial(kernel, sp_size),
        out_shape=pltpu.VMEM((ROWS, COLS), BF16),
        in_specs=[vmem, hbm, hbm, hbm, hbm],
        out_specs=vmem,
        scratch_shapes=[
            pltpu.VMEM((3, ROWS, COLS), BF16),
            pltpu.VMEM((3, ROWS, COLS), BF16),
            pltpu.VMEM((3, ROWS, COLS), BF16),
            pltpu.VMEM((2, COLS, COLS), BF16),
            pltpu.VMEM((PLANE, 3, n2, COLS), BF16),
            pltpu.VMEM((PLANE + 8, 3, n2, COLS), BF16),
            pltpu.VMEM((LINE, 3, n1, COLS), BF16),
            pltpu.VMEM((LINE + 2, 3, n1, COLS), BF16),
            pltpu.VMEM((ROWS, COLS), BF16),
            pltpu.VMEM((ROWS, COLS), BF16),
            pltpu.VMEM((2, BACK, COLS), BF16),
            pltpu.VMEM((BACK, COLS), BF16),
            pltpu.VMEM((2, BACK, COLS), BF16),
            pltpu.VMEM((BACK, HEAD), BF16),
            pltpu.VMEM((2, BACK, HEAD), BF16),
            pltpu.VMEM((PLANE, n2, COLS), BF16),
            pltpu.VMEM((PLANE, n2, COLS), BF16),
            pltpu.VMEM((LINE, n1, COLS), BF16),
            pltpu.VMEM((LINE, n1, COLS), BF16),
            pltpu.VMEM((CHUNKS, LINE, n2, HEAD), BF16),
            pltpu.VMEM((CHUNKS, LINE, n2, HEAD), BF16),
            pltpu.VMEM((CHUNKS, LINE, n2, HEAD), BF16),
            pltpu.VMEM((CHUNKS, LINE, n2, HEAD), BF16),
            pltpu.VMEM((2, ROWS, WIDE), F32),
            pltpu.VMEM((2, ROWS, WIDE), F32),
            pltpu.VMEM((ROWS, COLS), F32),
            pltpu.VMEM((ROWS, COLS), F32),
            pltpu.VMEM((BACK, COLS), F32),
            pltpu.VMEM((ROWS, COLS), BF16),
            pltpu.VMEM((ROWS, COLS), BF16),
            pltpu.VMEM((ROWS, COLS), F32),
            pltpu.VMEM((3, BACK, 2 * BACK), F32),
            pltpu.VMEM((3, ROWS, ROWS), BF16),
            pltpu.VMEM((2, ROWS, LINE * HEAD), BF16),
            pltpu.VMEM((ROWS, HEAD), F32),
            pltpu.VMEM((ROWS, HEAD), F32),
            dma((3, 3)), dma((2,)),
            dma((2,)), dma((2, CHUNKS)), dma((2,)), dma((2, CHUNKS)),
            dma, dma((CHUNKS,)), dma, dma((CHUNKS,)),
            dma((9,)), dma((9,)),
            dma, dma((CHUNKS,)), dma, dma((CHUNKS,)), dma, dma((CHUNKS,)), dma, dma((CHUNKS,)),
            dma, dma, pltpu.SemaphoreType.REGULAR, pltpu.SemaphoreType.REGULAR,
        ],
        name="attention",
        compiler_params=pltpu.CompilerParams(collective_id=0, has_side_effects=True),
    )(jnp.asarray(inverse[None, :]), queries, keys, values, w_out)


def solution(mesh):
    return jax.shard_map(
        shards,
        mesh=mesh,
        in_specs=(P(None, "sp", "tp"), P(None, "sp", "tp"), P(None, "sp", "tp"), P(None, "tp")),
        out_specs=P("sp", "tp"),
        check_vma=False,
    )
```

```python
import functools

import jax
import jax.numpy as jnp
import numpy as np
from jax import lax
from jax.experimental import pallas as pl
from jax.experimental.pallas import tpu as pltpu
from jax.sharding import PartitionSpec as P

HEAD = 128
ROPE_BASE = 10000.0
MASKED = -1e30
ROWS = 256
COLS = 1024
HEADS = COLS // HEAD
BACK = 128
PLANE = 16
LINE = 4
CHUNKS = 4
WIDE = COLS // CHUNKS
CHUNK_HEADS = WIDE // HEAD
MESH = pl.DeviceIdType.MESH
BF16 = jnp.bfloat16
F32 = jnp.float32


def arrived(ref, sem):
    pltpu.make_async_copy(ref, ref, sem).wait()


def one_hot(condition):
    return jnp.where(condition, 1.0, 0.0).astype(BF16)


def scoped(name, body, carry, first=0, last=CHUNKS):
    def named(c, carry):
        with jax.named_scope(name):
            return body(c, carry)

    return lax.fori_loop(first, last, named, carry)


def dot(a, b):
    return jnp.dot(a, b, preferred_element_type=F32)


def dot_nt(a, b):
    return lax.dot_general(a, b, (((1,), (1,)), ((), ())), preferred_element_type=F32)


def kernel(
    sp_size,
    inverse_ref, q_hbm, k_hbm, v_hbm, w_hbm, out_ref,
    qv, kv, vv, wv, s2, r2, s1, r1, k0, q0, qn, on, ob, ln, lb, o2, b2, o1, b1, l2, lb2, l1, lb1,
    g1, log1, o0, lse0, sum0, own, other, total, band, perms, wanted, cos_full, sin_full,
    in_sem, w_sem, s2_send, s2_recv, s1_send, s1_recv, h2_send, h2_recv, h1_send, h1_recv,
    n0_send, n0_recv, o2_send, o2_recv, o1_send, o1_recv, l2_send, l2_recv, l1_send, l1_recv,
    a_send, a_recv, next_ready, row_ready,
):
    sp = lax.axis_index("sp")
    tp = lax.axis_index("tp")
    x = lax.rem(sp, LINE)
    y = lax.rem(sp // LINE, LINE)
    j = lax.rem(sp, PLANE)
    plane = sp - j

    def block(distance):
        return lax.rem(sp + distance + sp_size, sp_size)

    def peer(d):
        px = lax.rem(x + d // LINE, LINE)
        py = lax.rem(y + lax.rem(d, LINE), LINE)
        return py * LINE + px

    def mate(d):
        return lax.rem(x + d, LINE)

    def columns(c):
        return pl.ds(pl.multiple_of(c * WIDE, WIDE), WIDE)

    def load(g, i):
        src, dst = ((q_hbm, qv), (k_hbm, kv), (v_hbm, vv))[i]
        return pltpu.make_async_copy(src.at[g], dst.at[g], in_sem.at[g, i])

    load(0, 0).start()
    for g, i in ((2, 0), (2, 1), (2, 2), (1, 0), (1, 1), (1, 2)):
        load(g, i).start()
    w_copies = [
        pltpu.make_async_copy(w_hbm.at[pl.ds(pl.multiple_of(half * COLS, COLS), COLS)], wv.at[n], w_sem.at[n])
        for n, half in enumerate((tp, 1 - tp))
    ]

    barrier = pltpu.get_barrier_semaphore()

    def greet(d, _):
        pl.semaphore_signal(barrier, inc=1, device_id=(plane + peer(d), tp), device_id_type=MESH)
        return 0

    lax.fori_loop(1, PLANE, greet, 0)
    pl.semaphore_signal(barrier, inc=1, device_id=(sp, 1 - tp), device_id_type=MESH)

    has_next = sp + PLANE < sp_size
    has_last = sp >= PLANE
    row_next = sp + LINE < sp_size
    row_last = sp >= LINE
    edge_next = row_next & (y == LINE - 1)
    edge_last = row_last & (y == 0)

    @pl.when(has_next)
    def _():
        pl.semaphore_signal(barrier, inc=1, device_id=(block(PLANE), tp), device_id_type=MESH)

    @pl.when(edge_next)
    def _():
        pl.semaphore_signal(barrier, inc=1, device_id=(block(LINE), tp), device_id_type=MESH)

    row = lax.broadcasted_iota(jnp.int32, (ROWS, ROWS), 0)
    col = lax.broadcasted_iota(jnp.int32, (ROWS, ROWS), 1)
    n2 = ROWS // PLANE
    n1 = ROWS // LINE

    perms[0] = one_hot(col == PLANE * (row % n2) + row // n2)
    perms[1] = one_hot(col == LINE * (row % n1) + row // n1)

    half_row = lax.broadcasted_iota(jnp.int32, (ROWS // 2, HEAD), 0)
    feature = lax.broadcasted_iota(jnp.int32, (ROWS // 2, HEAD), 1)
    left = feature < HEAD // 2
    position = (sp * ROWS + half_row + jnp.where(left, 0, ROWS // 2)).astype(F32)
    inverse = inverse_ref[...]
    angles = position * jnp.concatenate([inverse, inverse], axis=1)
    for table, values, sign in ((cos_full, jnp.cos(angles), 1.0), (sin_full, jnp.sin(angles), -1.0)):
        swapped = pltpu.roll(values, HEAD // 2, 1)
        table[: ROWS // 2] = jnp.where(left, values * sign, swapped)
        table[ROWS // 2 :] = jnp.where(left, swapped * sign, values)

    def turned(piece):
        parts = []
        for h in range(piece.shape[1] // HEAD):
            m = piece[:, h * HEAD : (h + 1) * HEAD].astype(F32)
            parts.append(m * cos_full[...] + pltpu.roll(m, HEAD // 2, 1) * sin_full[...])
        return jnp.concatenate(parts, axis=1)

    def prepared(g, c):
        cs = columns(c)
        q = (turned(qv[g, :, cs]) * HEAD**-0.5).astype(BF16)
        k = turned(kv[g, :, cs]).astype(BF16)
        return q, k

    def remote(src, dst, i, device):
        return pltpu.make_async_remote_copy(
            src_ref=src,
            dst_ref=dst,
            send_sem=n0_send.at[i],
            recv_sem=n0_recv.at[i],
            device_id=(device, tp),
            device_id_type=MESH,
        )

    before, after = sp - x + mate(LINE - 1), sp - x + mate(1)

    def q0_copy():
        return remote(q0.at[pl.ds(0, BACK)], qn.at[0], 0, before)

    def q0_relay():
        return remote(qn.at[0], qn.at[1], 1, block(-LINE))

    near, far = pl.ds(0, 3 * COLS // 4), pl.ds(3 * COLS // 4, COLS // 4)

    def on_near():
        return remote(on.at[:, near], ob.at[0, :, near], 2, after)

    def on_near_relay():
        return remote(ob.at[0, :, near], ob.at[1, :, near], 3, block(LINE))

    def on_far():
        return remote(on.at[:, far], ob.at[0, :, far], 6, after)

    def on_far_turn():
        return remote(on.at[:, far], ob.at[1, :, far], 7, block(LINE))

    def on_far_relay():
        return remote(ob.at[1, :, far], ob.at[1, :, far], 8, after)

    def ln_copy():
        return remote(ln, lb.at[0], 4, after)

    def ln_relay():
        return remote(lb.at[0], lb.at[1], 5, block(LINE))

    q_slot = jnp.where(x == LINE - 1, 1, 0)
    o_slot = jnp.where(x == 0, 1, 0)

    with jax.named_scope("load0"):
        load(0, 0).wait()
    for i in (1, 2):
        load(0, i).start()

    def q0_out(c, _):
        cs = columns(c)
        q0[:, cs] = (turned(qv[0, :, cs]) * HEAD**-0.5).astype(BF16)
        return 0

    def k0_out(c, _):
        cs = columns(c)
        k0[:, cs] = turned(kv[0, :, cs]).astype(BF16)
        return 0

    scoped("q0_out", q0_out, 0)
    with jax.named_scope("barrier"):
        expected = PLANE + jnp.where(has_last, 1, 0) + jnp.where(edge_last, 1, 0)
        pl.semaphore_wait(barrier, expected)

    @pl.when(has_last)
    def _():
        pl.semaphore_signal(next_ready, inc=1, device_id=(block(-PLANE), tp), device_id_type=MESH)

    @pl.when(edge_last)
    def _():
        pl.semaphore_signal(row_ready, inc=1, device_id=(block(-LINE), tp), device_id_type=MESH)

    q0_copy().start()

    def g2_copy(c, d, part):
        what = pl.ds(part, part + 1)
        return pltpu.make_async_remote_copy(
            src_ref=s2.at[peer(d), what, :, columns(c)],
            dst_ref=r2.at[8 + j, what, :, columns(c)],
            send_sem=s2_send.at[part],
            recv_sem=s2_recv.at[part, c],
            device_id=(plane + peer(d), tp),
            device_id_type=MESH,
        )

    def g2_out(c, _):
        cs = columns(c)
        q, k = prepared(2, c)
        order = perms[0]
        for i, m in enumerate((q, k, vv[2, :, cs])):
            s2[:, i, :, cs] = dot(order, m).astype(BF16).reshape(PLANE, n2, WIDE)
        r2[8 + j, :, :, cs] = s2[j, :, :, cs]
        lax.fori_loop(1, PLANE, lambda d, _: (g2_copy(c, d, 1).start(), 0)[1], 0)
        return 0

    def g2_queries(c, _):
        lax.fori_loop(1, PLANE, lambda d, _: (g2_copy(c, d, 0).start(), 0)[1], 0)
        return 0


    def g1_copy(c, d, part):
        what = pl.ds(part, part + 1)
        return pltpu.make_async_remote_copy(
            src_ref=s1.at[mate(d), what, :, columns(c)],
            dst_ref=r1.at[2 + x, what, :, columns(c)],
            send_sem=s1_send.at[part],
            recv_sem=s1_recv.at[part, c],
            device_id=(sp - x + mate(d), tp),
            device_id_type=MESH,
        )

    def g1_out(c, _):
        cs = columns(c)
        q, k = prepared(1, c)
        order = perms[1]
        for i, m in enumerate((q, k, vv[1, :, cs])):
            s1[:, i, :, cs] = dot(order, m).astype(BF16).reshape(LINE, n1, WIDE)
        r1[2 + x, :, :, cs] = s1[x, :, :, cs]
        lax.fori_loop(1, LINE, lambda d, _: (g1_copy(c, d, 1).start(), 0)[1], 0)
        return 0

    def g1_queries(c, _):
        lax.fori_loop(1, LINE, lambda d, _: (g1_copy(c, d, 0).start(), 0)[1], 0)
        return 0

    def send_out(c, _):
        g2_out(c, 0)

        @pl.when(c == 0)
        def _():
            for i in range(3):
                load(1, i).wait()

        g1_out(c, 0)
        return 0

    with jax.named_scope("load2"):
        for i in range(3):
            load(2, i).wait()
    scoped("send_out", send_out, 0)
    scoped("g2_queries", g2_queries, 0)

    @pl.when(jnp.logical_not(has_last))
    def _():
        r2[pl.ds(0, 8), pl.ds(1, 2)] = jnp.zeros((8, 2, ROWS // PLANE, COLS), BF16)

    @pl.when(jnp.logical_not(row_last))
    def _():
        r1[pl.ds(0, 2), pl.ds(1, 2)] = jnp.zeros((2, 2, ROWS // LINE, COLS), BF16)
        ob[1] = jnp.zeros((BACK, COLS), BF16)
        lb[1] = jnp.zeros((BACK, HEAD), BF16)

    @pl.when(jnp.logical_not(row_next))
    def _():
        qn[1] = jnp.zeros((BACK, COLS), BF16)

    q_index = lax.broadcasted_iota(jnp.int32, (BACK, 2 * BACK), 0)
    k_index = lax.broadcasted_iota(jnp.int32, (BACK, 2 * BACK), 1)
    inside = (k_index >= q_index) & (k_index <= q_index + BACK)
    base = jnp.where(inside, 0.0, MASKED)
    band[0] = base
    for g, reach in ((1, LINE), (2, PLANE)):
        opening = jnp.where(sp >= reach, 0.0, MASKED)
        band[g] = jnp.where(k_index < BACK, base + opening, base)

    perms[2] = one_hot(row == LINE * (col % n1) + col // n1)
    token = lax.broadcasted_iota(jnp.int32, (ROWS, LINE * HEAD), 0)
    lane1 = lax.broadcasted_iota(jnp.int32, (ROWS, LINE * HEAD), 1)
    for which, half in enumerate((x % 2, y % 2)):
        wanted[which] = one_hot(lane1 == (token % LINE) * HEAD + half * n1 + token // LINE)


    def h2_copy(c):
        return pltpu.make_async_remote_copy(
            src_ref=r2.at[pl.ds(16, 8), pl.ds(1, 2), :, columns(c)],
            dst_ref=r2.at[pl.ds(0, 8), pl.ds(1, 2), :, columns(c)],
            send_sem=h2_send,
            recv_sem=h2_recv.at[c],
            device_id=(block(PLANE), tp),
            device_id_type=MESH,
        )

    def h1_copy(c):
        return pltpu.make_async_remote_copy(
            src_ref=r1.at[pl.ds(4, 2), pl.ds(1, 2), :, columns(c)],
            dst_ref=r1.at[pl.ds(0, 2), pl.ds(1, 2), :, columns(c)],
            send_sem=h1_send,
            recv_sem=h1_recv.at[c],
            device_id=(block(LINE), tp),
            device_id_type=MESH,
        )

    def attend(q, k, v, bias):
        scores = dot_nt(q, k) + bias
        row_max = jnp.max(scores, axis=1, keepdims=True)
        probs = jnp.exp(scores - row_max)
        row_sum = jnp.sum(probs, axis=1, keepdims=True)
        result = dot(probs.astype(BF16), v) / row_sum
        return result, row_max + jnp.log(row_sum)

    lane = lax.broadcasted_iota(jnp.int32, (BACK, HEAD), 1)

    def g2_halo(c, _):
        arrived(r2.at[pl.ds(8, PLANE - 1), pl.ds(1, 2), :, columns(c)], s2_recv.at[1, c])

        @pl.when(has_next & (c == 0))
        def _():
            pl.semaphore_wait(next_ready, 1)

        @pl.when(has_next)
        def _():
            h2_copy(c).start()

        return 0

    def g1_halo(c, _):
        arrived(r1.at[pl.ds(2, LINE - 1), pl.ds(1, 2), :, columns(c)], s1_recv.at[1, c])

        @pl.when(edge_next & (c == 0))
        def _():
            pl.semaphore_wait(row_ready, 1)

        @pl.when(row_next)
        def _():
            h1_copy(c).start()

        return 0

    def rung(d):
        return lax.rem(y + d, LINE)

    def o2_copy(c, d):
        return pltpu.make_async_remote_copy(
            src_ref=o2.at[pl.ds(LINE * rung(d), LINE), :, columns(c)],
            dst_ref=b2.at[pl.ds(LINE * y, LINE), :, columns(c)],
            send_sem=o2_send,
            recv_sem=o2_recv.at[c],
            device_id=(plane + rung(d) * LINE + x, tp),
            device_id_type=MESH,
        )

    def l2_copy(c, d):
        return pltpu.make_async_remote_copy(
            src_ref=l2.at[c, rung(d)],
            dst_ref=lb2.at[c, y],
            send_sem=l2_send,
            recv_sem=l2_recv.at[c],
            device_id=(plane + rung(d) * LINE + x, tp),
            device_id_type=MESH,
        )

    def o1_copy(c, d):
        return pltpu.make_async_remote_copy(
            src_ref=o1.at[mate(d), :, columns(c)],
            dst_ref=b1.at[x, :, columns(c)],
            send_sem=o1_send,
            recv_sem=o1_recv.at[c],
            device_id=(sp - x + mate(d), tp),
            device_id_type=MESH,
        )

    def l1_copy(c, d):
        return pltpu.make_async_remote_copy(
            src_ref=l1.at[c, mate(d)],
            dst_ref=lb1.at[c, x],
            send_sem=l1_send,
            recv_sem=l1_recv.at[c],
            device_id=(sp - x + mate(d), tp),
            device_id_type=MESH,
        )

    def split_terms(lse, heads):
        high = lse.astype(BF16).astype(F32)
        rest = lse - high
        middle = rest.astype(BF16).astype(F32)
        low = rest - middle
        return (high + pltpu.roll(middle, heads, 1) + pltpu.roll(low, 2 * heads, 1)).astype(BF16)

    def place(lses, b, head, lse):
        lses[b] = jnp.where(lane == head, lse, lses[b])

    def pack(target, c, lses):
        slot = lax.broadcasted_iota(jnp.int32, (n2, HEAD), 0)
        chosen = one_hot(slot == lax.broadcasted_iota(jnp.int32, (n2, HEAD), 1))
        for b in range(2):
            tile = dot_nt(chosen, split_terms(lses[b], CHUNK_HEADS)).astype(BF16)
            target[c, 2 * b] = tile
            target[c, 2 * b + 1] = tile

    def unpack(tiles, c, which):
        lanes = jnp.concatenate([tiles[c, r] for r in range(LINE)], axis=1)
        return dot(dot_nt(wanted[which], lanes).astype(BF16), spread(n2, CHUNK_HEADS, 0))

    def g2_attend(c, _):
        with jax.named_scope("wait_h2"):

            @pl.when(has_last)
            def _():
                h2_copy(c).wait_recv()

        with jax.named_scope("wait_q2"):
            arrived(r2.at[pl.ds(8, PLANE - 1), pl.ds(0, 1), :, columns(c)], s2_recv.at[0, c])
        lses = list(empty)
        for h in range(CHUNK_HEADS):
            cs = pl.ds(pl.multiple_of(c * WIDE + h * HEAD, HEAD), HEAD)
            for b in range(2):
                q = r2[pl.ds(8 + 8 * b, 8), 0, :, cs].reshape(BACK, HEAD)
                k = r2[pl.ds(8 * b, 16), 1, :, cs].reshape(2 * BACK, HEAD)
                v = r2[pl.ds(8 * b, 16), 2, :, cs].reshape(2 * BACK, HEAD)
                result, lse = attend(q, k, v, band[2 if b == 0 else 0])
                o2[pl.ds(8 * b, 8), :, cs] = result.astype(BF16).reshape(8, n2, HEAD)
                place(lses, b, h, lse)
        pack(l2, c, lses)
        mine = pl.ds(LINE * y, LINE)
        b2[mine, :, columns(c)] = o2[mine, :, columns(c)]
        lb2[c, y] = l2[c, y]
        lax.fori_loop(1, LINE, lambda d, _: (o2_copy(c, d).start(), l2_copy(c, d).start(), 0)[2], 0)
        return 0

    def g1_attend(c, _):
        with jax.named_scope("wait_h1"):

            @pl.when(row_last)
            def _():
                h1_copy(c).wait_recv()

        with jax.named_scope("wait_q1"):
            arrived(r1.at[pl.ds(2, LINE - 1), pl.ds(0, 1), :, columns(c)], s1_recv.at[0, c])
        for h in range(CHUNK_HEADS):
            cs = pl.ds(pl.multiple_of(c * WIDE + h * HEAD, HEAD), HEAD)
            for b in range(2):
                q = r1[pl.ds(2 + 2 * b, 2), 0, :, cs].reshape(BACK, HEAD)
                k = r1[pl.ds(2 * b, 4), 1, :, cs].reshape(2 * BACK, HEAD)
                v = r1[pl.ds(2 * b, 4), 2, :, cs].reshape(2 * BACK, HEAD)
                result, lse = attend(q, k, v, band[1 if b == 0 else 0])
                rows, lanes = pl.ds(BACK * b, BACK), pl.ds(HEAD * h, HEAD)
                g1[lax.rem(c, 2), rows, lanes] = result
                log1[lax.rem(c, 2), rows, lanes] = jnp.broadcast_to(lse, (BACK, HEAD))
        return 0

    def join(c, _):
        with jax.named_scope("wait_o2"):
            arrived(b2.at[pl.ds(0, PLANE - LINE), :, columns(c)], o2_recv.at[c])
            arrived(lb2.at[c, pl.ds(0, LINE - 1)], l2_recv.at[c])
        cs = columns(c)
        out2 = dot(perms[2], b2[:, :, cs].reshape(ROWS, WIDE))
        log2 = unpack(lb2, c, 1)
        here = lax.rem(c, 2)
        top = jnp.maximum(log1[here], log2)
        w1, w2 = jnp.exp(log1[here] - top), jnp.exp(log2 - top)
        weight = w1 + w2
        o1[:, :, cs] = ((w1 * g1[here] + w2 * out2) / weight).astype(BF16).reshape(LINE, n1, WIDE)
        log12 = top + jnp.log(weight)
        lses = list(empty)
        for b in range(2):
            for h in range(CHUNK_HEADS):
                place(lses, b, h, log12[BACK * b : BACK * (b + 1), HEAD * h : HEAD * (h + 1)])
        pack(l1, c, lses)
        b1[x, :, cs] = o1[x, :, cs]
        lb1[c, x] = l1[c, x]
        lax.fori_loop(1, LINE, lambda d, _: (o1_copy(c, d).start(), l1_copy(c, d).start(), 0)[2], 0)
        return 0

    def spread(terms, heads, first):
        term = lax.broadcasted_iota(jnp.int32, (terms, WIDE), 0)
        feature = lax.broadcasted_iota(jnp.int32, (terms, WIDE), 1)
        return one_hot((term < 3 * heads) & (term % heads == first + feature // HEAD))

    def g0_attend(c, _):
        for h in range(CHUNK_HEADS):
            cs = pl.ds(pl.multiple_of(c * WIDE + h * HEAD, HEAD), HEAD)
            for b in range(2):
                q = q0[pl.ds(BACK * b, BACK), cs]
                k = k0[pl.ds(0, BACK * (b + 1)), cs]
                v = vv[0, pl.ds(0, BACK * (b + 1)), cs]
                result, lse = attend(q, k, v, band[0] if b else band[0, :, BACK:])
                o0[pl.ds(BACK * b, BACK), cs] = result
                lse0[pl.ds(BACK * b, BACK), cs] = jnp.broadcast_to(lse, (BACK, HEAD))
        return 0

    def n0_attend(c, carry):
        lses = list(carry)
        for h in range(CHUNK_HEADS):
            cs = pl.ds(pl.multiple_of(c * WIDE + h * HEAD, HEAD), HEAD)
            k = k0[pl.ds(BACK, BACK), cs]
            v = vv[0, pl.ds(BACK, BACK), cs]
            result, lse = attend(qn[q_slot, :, cs], k, v, band[0, :, :BACK])
            on[:, cs] = result.astype(BF16)
            place(lses, 0, c * CHUNK_HEADS + h, lse)
        return tuple(lses)

    empty = (jnp.zeros((BACK, HEAD), F32), jnp.zeros((BACK, HEAD), F32))

    for copy in w_copies:
        copy.start()
    with jax.named_scope("wait_q0"):
        q0_copy().wait_recv()

    @pl.when((x == LINE - 1) & row_last)
    def _():
        q0_relay().start()

    load(0, 1).wait()
    load(0, 2).wait()
    scoped("k0_out", k0_out, 0)
    scoped("g0_attend", g0_attend, 0)
    def step(c, _):
        with jax.named_scope("g2_halo"):
            g2_halo(c, 0)
        with jax.named_scope("g1_halo"):
            g1_halo(c, 0)

        @pl.when(c == 1)
        def _():
            with jax.named_scope("wait_q0r"):

                @pl.when((x == LINE - 1) & row_next)
                def _():
                    q0_relay().wait_recv()

            lses = scoped("n0_attend", n0_attend, empty[:1])
            ln[...] = split_terms(lses[0], HEADS)
            on_near().start()
            ln_copy().start()

            @pl.when(x < LINE - 1)
            def _():
                on_far().start()

            @pl.when((x == LINE - 1) & row_next)
            def _():
                on_far_turn().start()


        return 0

    lax.fori_loop(0, CHUNKS, step, 0)
    scoped("g1_queries", g1_queries, 0)

    def g2_step(c, _):
        @pl.when((c == 1) & (x == LINE - 1) & row_last)
        def _():
            with jax.named_scope("wait_far"):
                on_far_turn().wait_recv()
                on_far_relay().start()

        @pl.when((c == 2) & (x == 0))
        def _():
            with jax.named_scope("wait_on"):
                on_near().wait_recv()
                ln_copy().wait_recv()

                @pl.when(row_next)
                def _():
                    on_near_relay().start()
                    ln_relay().start()


        with jax.named_scope("g2_attend"):
            g2_attend(c, 0)
        return 0

    lax.fori_loop(0, CHUNKS, g2_step, 0)

    def last(c, _):
        @pl.when(c < CHUNKS)
        def _():
            with jax.named_scope("g1_attend"):
                g1_attend(c, 0)

        @pl.when(c > 0)
        def _():
            with jax.named_scope("join"):
                join(c - 1, 0)

        return 0

    lax.fori_loop(0, CHUNKS + 1, last, 0)

    with jax.named_scope("drain"):
        for part in range(2):
            what = pl.ds(part, part + 1)
            arrived(s2.at[pl.ds(0, PLANE - 1), what], s2_send.at[part])
            arrived(s1.at[pl.ds(0, LINE - 1), what], s1_send.at[part])

        @pl.when(has_next)
        def _():
            arrived(r2.at[pl.ds(16, 8), pl.ds(1, 2)], h2_send)

        @pl.when(row_next)
        def _():
            arrived(r1.at[pl.ds(4, 2), pl.ds(1, 2)], h1_send)

    for copy in w_copies:
        copy.wait()
    for copy in (q0_copy(), on_near(), ln_copy()):
        copy.wait_send()

    @pl.when((x == LINE - 1) & row_last)
    def _():
        q0_relay().wait_send()
        on_far_relay().wait_send()

    @pl.when((x == LINE - 1) & row_next)
    def _():
        on_far_turn().wait_send()

    @pl.when(x < LINE - 1)
    def _():
        on_far().wait_send()


    with jax.named_scope("wait_l"):

        @pl.when((x == 0) & row_next)
        def _():
            on_near_relay().wait_send()
            ln_relay().wait_send()

        @pl.when((x == 0) & row_last)
        def _():
            on_near_relay().wait_recv()
            on_far_relay().wait_recv()
            ln_relay().wait_recv()

        @pl.when(x > 0)
        def _():
            on_near().wait_recv()
            on_far().wait_recv()
            ln_copy().wait_recv()

    def a_copy(c):
        return pltpu.make_async_remote_copy(
            src_ref=own.at[:, columns(c)],
            dst_ref=other.at[:, columns(c)],
            send_sem=a_send,
            recv_sem=a_recv,
            device_id=(sp, 1 - tp),
            device_id_type=MESH,
        )

    def premerge(c, _):
        cs = columns(c)
        rows = slice(0, BACK)
        log3 = dot(lb[o_slot], spread(HEAD, HEADS, c * CHUNK_HEADS)) + jnp.where(sp >= 1, 0.0, MASKED)
        top = jnp.maximum(lse0[rows, cs], log3)
        w0, w3 = jnp.exp(lse0[rows, cs] - top), jnp.exp(log3 - top)
        o0[rows, cs] = w0 * o0[rows, cs] + w3 * ob[o_slot, :, cs].astype(F32)
        sum0[:, cs] = w0 + w3
        lse0[rows, cs] = top
        return 0

    scoped("premerge", premerge, 0)

    def merge(c, _):
        with jax.named_scope("wait_o1"):
            arrived(b1.at[pl.ds(0, LINE - 1), :, columns(c)], o1_recv.at[c])
            arrived(lb1.at[c, pl.ds(0, LINE - 1)], l1_recv.at[c])
        cs = columns(c)
        out12 = dot(perms[2], b1[:, :, cs].reshape(ROWS, WIDE))
        log12 = unpack(lb1, c, 0)
        for half in range(2):
            rows = slice(half * BACK, (half + 1) * BACK)
            top = jnp.maximum(lse0[rows, cs], log12[rows])
            old, new = jnp.exp(lse0[rows, cs] - top), jnp.exp(log12[rows] - top)
            weight = sum0[:, cs] * old + new if half == 0 else old + new
            own[rows, cs] = ((o0[rows, cs] * old + out12[rows] * new) / weight).astype(BF16)
        a_copy(c).start()

        return 0

    def merges(k, _):
        merge(2 * k, 0)
        merge(2 * k + 1, 0)
        return 0

    scoped("merge", merges, 0, 0, CHUNKS // 2)

    with jax.named_scope("project"):
        for c in range(CHUNKS):
            cs = columns(c)
            total[:, cs] = dot(own[...], wv[0, :, cs])
    with jax.named_scope("wait_a"):
        arrived(other, a_recv)
    with jax.named_scope("project"):
        for c in range(CHUNKS):
            cs = columns(c)
            out_ref[:, cs] = (total[:, cs] + dot(other[...], wv[1, :, cs])).astype(BF16)

    with jax.named_scope("finish"):
        arrived(o2.at[pl.ds(0, PLANE - LINE)], o2_send)
        arrived(l2.at[:, pl.ds(0, LINE - 1)], l2_send)
        arrived(o1.at[pl.ds(0, LINE - 1)], o1_send)
        arrived(l1.at[:, pl.ds(0, LINE - 1)], l1_send)
        arrived(own, a_send)


def shards(queries, keys, values, w_out):
    sp_size = lax.axis_size("sp")
    inverse = np.float32(ROPE_BASE ** (-np.arange(0, HEAD, 2) / HEAD))
    n2, n1 = ROWS // PLANE, ROWS // LINE
    dma = pltpu.SemaphoreType.DMA
    vmem = pl.BlockSpec(memory_space=pltpu.VMEM)
    hbm = pl.BlockSpec(memory_space=pl.ANY)
    return pl.pallas_call(
        functools.partial(kernel, sp_size),
        out_shape=pltpu.VMEM((ROWS, COLS), BF16),
        in_specs=[vmem, hbm, hbm, hbm, hbm],
        out_specs=vmem,
        scratch_shapes=[
            pltpu.VMEM((3, ROWS, COLS), BF16),
            pltpu.VMEM((3, ROWS, COLS), BF16),
            pltpu.VMEM((3, ROWS, COLS), BF16),
            pltpu.VMEM((2, COLS, COLS), BF16),
            pltpu.VMEM((PLANE, 3, n2, COLS), BF16),
            pltpu.VMEM((PLANE + 8, 3, n2, COLS), BF16),
            pltpu.VMEM((LINE, 3, n1, COLS), BF16),
            pltpu.VMEM((LINE + 2, 3, n1, COLS), BF16),
            pltpu.VMEM((ROWS, COLS), BF16),
            pltpu.VMEM((ROWS, COLS), BF16),
            pltpu.VMEM((2, BACK, COLS), BF16),
            pltpu.VMEM((BACK, COLS), BF16),
            pltpu.VMEM((2, BACK, COLS), BF16),
            pltpu.VMEM((BACK, HEAD), BF16),
            pltpu.VMEM((2, BACK, HEAD), BF16),
            pltpu.VMEM((PLANE, n2, COLS), BF16),
            pltpu.VMEM((PLANE, n2, COLS), BF16),
            pltpu.VMEM((LINE, n1, COLS), BF16),
            pltpu.VMEM((LINE, n1, COLS), BF16),
            pltpu.VMEM((CHUNKS, LINE, n2, HEAD), BF16),
            pltpu.VMEM((CHUNKS, LINE, n2, HEAD), BF16),
            pltpu.VMEM((CHUNKS, LINE, n2, HEAD), BF16),
            pltpu.VMEM((CHUNKS, LINE, n2, HEAD), BF16),
            pltpu.VMEM((2, ROWS, WIDE), F32),
            pltpu.VMEM((2, ROWS, WIDE), F32),
            pltpu.VMEM((ROWS, COLS), F32),
            pltpu.VMEM((ROWS, COLS), F32),
            pltpu.VMEM((BACK, COLS), F32),
            pltpu.VMEM((ROWS, COLS), BF16),
            pltpu.VMEM((ROWS, COLS), BF16),
            pltpu.VMEM((ROWS, COLS), F32),
            pltpu.VMEM((3, BACK, 2 * BACK), F32),
            pltpu.VMEM((3, ROWS, ROWS), BF16),
            pltpu.VMEM((2, ROWS, LINE * HEAD), BF16),
            pltpu.VMEM((ROWS, HEAD), F32),
            pltpu.VMEM((ROWS, HEAD), F32),
            dma((3, 3)), dma((2,)),
            dma((2,)), dma((2, CHUNKS)), dma((2,)), dma((2, CHUNKS)),
            dma, dma((CHUNKS,)), dma, dma((CHUNKS,)),
            dma((9,)), dma((9,)),
            dma, dma((CHUNKS,)), dma, dma((CHUNKS,)), dma, dma((CHUNKS,)), dma, dma((CHUNKS,)),
            dma, dma, pltpu.SemaphoreType.REGULAR, pltpu.SemaphoreType.REGULAR,
        ],
        name="attention",
        compiler_params=pltpu.CompilerParams(collective_id=0, has_side_effects=True),
    )(jnp.asarray(inverse[None, :]), queries, keys, values, w_out)


def solution(mesh):
    return jax.shard_map(
        shards,
        mesh=mesh,
        in_specs=(P(None, "sp", "tp"), P(None, "sp", "tp"), P(None, "sp", "tp"), P(None, "tp")),
        out_specs=P("sp", "tp"),
        check_vma=False,
    )
```
